32 devices in a mesh: sp: 8 (over z, x), tp: 4 (over y, core).
Axes of the slice: x: 2, y: 2, z: 4, core: 2. Of those that a mesh axis runs over, the one named last changes fastest.
Arguments:
- block_input: bfloat16 [2048, 2048], P('sp'), may hold values from -8 to 8
- queries: bfloat16 [2048, 1024], P('sp', 'tp'), may hold values from -6 to 6
- keys: bfloat16 [2048, 1024], P('sp', 'tp'), may hold values from -6 to 6
- w_value: bfloat16 [2048, 2048], P(None, 'tp'), may hold values from -0.125 to 0.125
- log_decay: float32 [2048, 1024], P('sp', 'tp'), as said below
- d_out: bfloat16 [2048, 2048], P('sp', 'tp'), may hold values from -0.125 to 0.125
Outputs:
- d_queries: bfloat16 [2048, 1024], P('sp', 'tp')
- d_keys: bfloat16 [2048, 1024], P('sp', 'tp')
- d_log_decay: float32 [2048, 1024], P('sp', 'tp')
- d_w_value: float32 [2048, 2048], P('sp', 'tp')
- row_norms: float32 [2048], P('sp')
The draws below stay inside these ranges and needn't reach their ends.
Inputs may be any that keep to these rules, and one draw needn't show every extreme that they name: log_decay is negative; key channels differ in rate, and rates change along the sequence.
All inputs are finite; a program needn't handle non-finite values.
Results may differ from the reference program's by a relative error of at most 0.015.
Values sent between devices are 32-bit elements; how exact they have to be, the bound alone decides.
A program may use at most 64 MiB of HBM per device.

```python
import math
import jax
import jax.numpy as jnp
from jax import lax

D = 2048
HEADS = 8
DK = 128
DV = 256
TOK_DEV = 256
TOKENS = 2048


def draw_log_decay(key, part):
    rate_key, noise_key, span_key = jax.random.split(jax.random.fold_in(key, 11), 3)
    rates = jnp.exp(jax.random.uniform(rate_key, (HEADS * DK,), jnp.float32, math.log(0.08), math.log(2.1))) / TOKENS
    span_factor = jnp.exp(jax.random.uniform(span_key, (TOKENS // TOK_DEV, 1, HEADS * DK), jnp.float32, -1.5, 1.5))
    span_factor = jnp.broadcast_to(span_factor, (TOKENS // TOK_DEV, TOK_DEV, HEADS * DK)).reshape(TOKENS, HEADS * DK)
    noise = jnp.clip(0.5 * jax.random.normal(noise_key, (TOKENS, HEADS * DK), jnp.float32), -1.5, 1.5)
    return (-rates[None, :] * span_factor * jnp.exp(noise)).astype(jnp.float32)


def strengthened(values, key, source, target, shards_of, factor):
    def block_of(position):
        return (jnp.arange(values.shape[position]) // (values.shape[position] // shards_of)).reshape((-1,) + (1,) * (values.ndim - 1 - position))

    near = jax.random.permutation(key, shards_of)[block_of(target)]
    other_side = (block_of(target) + shards_of // 2) % shards_of
    return jnp.where((block_of(source) == near) | (block_of(source) == other_side), factor * values, values)


def levels(own_key, extent, shards, least, top_value):
    loudness, own = 1.0, jax.random.fold_in(own_key, 6)
    for dim, blocks in shards:
        draws = jnp.exp(jax.random.uniform(jax.random.fold_in(own, dim), (blocks,), jnp.float32, least / len(shards), top_value / len(shards)))
        loudness = loudness * jnp.repeat(draws, extent[dim] // blocks).reshape([-1 if axis == dim else 1 for axis in range(len(extent))])
    return loudness


def normal_values(own_key, dims, deviation, limit, cuts=(), kind=jnp.bfloat16):
    values = deviation * jax.random.normal(own_key, dims, jnp.float32)
    if cuts:
        values = values * levels(own_key, dims, cuts, -0.22, 0.18)
    return jnp.clip(values, -limit, limit).astype(kind)


def gaussian_with(stream_key, shape, spread, bound, cuts, heavy, held_as=jnp.bfloat16):
    values = spread * jax.random.normal(stream_key, shape, jnp.float32)
    if cuts:
        values = values * levels(stream_key, shape, cuts, -0.22, 0.18)
    return jnp.clip(strengthened(values, jax.random.fold_in(stream_key, 3), *heavy), -bound, bound).astype(held_as)


def setup_inputs(seed: int = 0) -> dict:
    key_list = jax.random.split(jax.random.key(seed), 7)
    block_input = gaussian_with(key_list[0], (TOKENS, D), 1.0, 8.0, ((0, 8),), (0, 1, 8, 2.0))
    queries = normal_values(key_list[1], (TOKENS, HEADS * DK), 1.0, 6.0, ((0, 8), (1, 4)))
    keys = normal_values(key_list[2], (TOKENS, HEADS * DK), 1.0, 6.0, ((0, 8), (1, 4)))
    w_value = normal_values(key_list[3], (D, HEADS * DV), D ** -0.5, 0.125, ((1, 4),))
    log_decay = draw_log_decay(jax.random.fold_in(key_list[6], 71), 0)
    d_out = normal_values(key_list[5], (TOKENS, HEADS * DV), (TOKENS ** -0.5), 0.125, ((0, 8), (1, 4)))
    return dict(block_input=block_input, queries=queries, keys=keys, w_value=w_value, log_decay=log_decay, d_out=d_out)


def split_heads(array, block_len, width):
    length = array.shape[0]
    return array.reshape(length // block_len, block_len, -1, width).transpose(2, 0, 1, 3)


def merge_heads(array):
    return array.transpose(1, 2, 0, 3).reshape(array.shape[1] * array.shape[2], -1)


def product(form, left, right):
    return jnp.einsum(form, left.astype(jnp.float32), right.astype(jnp.float32), precision=lax.Precision.HIGHEST)


def reference(block_input, queries, keys, w_value, log_decay, d_out):
    q_scale = DK ** -0.5
    values = jnp.dot(block_input, w_value, preferred_element_type=jnp.float32).astype(jnp.bfloat16)
    block_len = 32
    q_heads = split_heads(queries, block_len, DK).astype(jnp.float32) * q_scale
    k_heads = split_heads(keys, block_len, DK).astype(jnp.float32)
    v_heads = split_heads(values, block_len, DV)
    g_heads = split_heads(log_decay, block_len, DK).astype(jnp.float32)
    o_grad = split_heads(d_out, block_len, DV)
    cumlog = jnp.cumsum(g_heads, axis=2)
    last_log = cumlog[:, :, -1:, :]
    k_tail = jnp.exp(last_log - cumlog)
    q_grown = (q_heads * jnp.exp(cumlog)).astype(jnp.bfloat16)
    k_shrunk = (k_heads * jnp.exp(-cumlog)).astype(jnp.bfloat16)
    k_tailed = (k_heads * k_tail).astype(jnp.bfloat16)
    causal = jnp.tril(jnp.ones((block_len, block_len), jnp.float32))
    out_dots = (product('hbcv,hbsv->hbcs', o_grad, v_heads) * causal).astype(jnp.bfloat16)
    key_dots = (product('hbcd,hbsd->hbcs', q_grown, k_shrunk) * causal).astype(jnp.bfloat16)
    increments = product('hbcd,hbcv->hbdv', k_tailed, v_heads)
    backwards = product('hbcd,hbcv->hbdv', q_grown, o_grad)
    block_decay = jnp.exp(last_log[:, :, 0, :])

    def leading(array):
        return jnp.moveaxis(array, 1, 0)

    def forward_step(carried, inputs):
        decay_block, grown = inputs
        return decay_block[:, :, None] * carried + grown, carried

    zero_state = jnp.zeros((HEADS, DK, DV), jnp.float32)
    _, entering = lax.scan(forward_step, zero_state, (leading(block_decay), leading(increments)))

    def backward_step(adjoint, inputs):
        decay_block, grown = inputs
        return grown + decay_block[:, :, None] * adjoint, adjoint

    _, from_right = lax.scan(backward_step, zero_state, (leading(block_decay), leading(backwards)), reverse=True)
    entering = jnp.moveaxis(entering, 0, 1)
    from_right = jnp.moveaxis(from_right, 0, 1)
    q_adjoint = jnp.exp(cumlog) * (product('hbcv,hbdv->hbcd', o_grad, entering) + product('hbcs,hbsd->hbcd', out_dots, k_shrunk))
    k_grad = jnp.exp(-cumlog) * product('hbcs,hbcd->hbsd', out_dots, q_grown) + k_tail * product('hbsv,hbdv->hbsd', v_heads, from_right)
    v_grad = product('hbcs,hbcv->hbsv', key_dots, o_grad) + product('hbsd,hbdv->hbsv', k_tailed, from_right)
    decay_terms = merge_heads(q_heads * q_adjoint - k_heads * k_grad)
    d_log_decay = jnp.flip(jnp.cumsum(jnp.flip(decay_terms, 0), 0), 0)
    value_grad = merge_heads(v_grad).astype(jnp.bfloat16)
    d_w_value = lax.dot_general(block_input, value_grad, (((0,), (0,)), ((), ())), preferred_element_type=jnp.float32)
    row_norms = jnp.sum(d_w_value * d_w_value, axis=1)
    return (merge_heads(q_adjoint * q_scale).astype(jnp.bfloat16), merge_heads(k_grad).astype(jnp.bfloat16), d_log_decay, d_w_value, row_norms)
```

```python
import functools

import jax
import jax.numpy as jnp
from jax import lax
from jax.experimental import pallas as pl
from jax.experimental.pallas import tpu as pltpu
from jax.sharding import PartitionSpec as P

DK = 128
DV = 256
BLOCK = 32
F32 = jnp.float32
BF16 = jnp.bfloat16
MESH = pl.DeviceIdType.MESH


def nn(left, right):
    return lax.dot_general(left, right, (((1,), (0,)), ((), ())), preferred_element_type=F32)


def nt(left, right):
    return lax.dot_general(left, right, (((1,), (1,)), ((), ())), preferred_element_type=F32)


def tn(left, right):
    return lax.dot_general(left, right, (((0,), (0,)), ((), ())), preferred_element_type=F32)


def pieces(value, count):
    parts = []
    for _ in range(count):
        part = value.astype(BF16)
        parts.append(part)
        value = value - part.astype(F32)
    return parts


def ring_place(z, x, nz, nx):
    r = nz - 1 - z
    across = jnp.where(r % 2 == 0, x - 1, nx - 1 - x)
    return jnp.where(x == 0, z, nz + r * (nx - 1) + across)


def ring_member(p, nz, nx):
    u = jnp.maximum(p - nz, 0)
    r = u // (nx - 1)
    w = u % (nx - 1)
    x = jnp.where(r % 2 == 0, 1 + w, nx - 1 - w)
    return jnp.where(p < nz, p * nx, (nz - 1 - r) * nx + x)


def is_cube(n, nx, ntp):
    return nx == 2 and n == 4 * nx and ntp == 2 * nx


def kernel(
    n, nx, ntp,
    x_hbm, q_hbm, k_hbm, w_hbm, g_hbm, o_hbm,
    dq_ref, dk_ref, dg_ref, dw_ref, rn_ref,
    x_ref, q_ref, k_ref, w_ref, g_ref, o_ref, in_sem,
    c_buf, span_buf, v_buf, qg_buf, kt_buf, ks_buf, y_buf, kp_buf, vp_buf, st_buf, xt_buf, vg_buf,
    a_out, a_in, z_out, z_in, z_acc, c_out, c_in, h_out, h_in, b_out, b_in, fr_buf,
    norm_out, norm_in,
    a_send, a_recv, z_send, z_recv, c_send, c_recv, h_send, h_recv, b_send, b_recv, n_send, n_recv,
    *late,
):
    cube = is_cube(n, nx, ntp)
    if cube:
        (xs_out, xr_in, xr_buf, vx_out, vx_in, vgp_buf, sx_out, sx_in, acc_buf, sm_out, sm_in,
         xs_send, xr_recv, v_send, v_recv, sx_send, sx_recv, sm_send, sm_recv) = late
    else:
        first, part, ring, r_send, r_recv = late
    nz = n // nx
    me = lax.axis_index("sp")
    mine = lax.axis_index("tp")
    z, x = me // nx, me % nx
    tokens, heads = q_ref.shape[0], q_ref.shape[1] // DK
    blocks = tokens // BLOCK
    dvx = DV // nx
    scale = DK ** (-0.5)
    loads = [
        pltpu.make_async_copy(source, target, in_sem.at[i])
        for i, (source, target) in enumerate(
            [(g_hbm, g_ref), (q_hbm, q_ref), (o_hbm, o_ref), (k_hbm, k_ref), (x_hbm, x_ref), (w_hbm, w_ref)]
        )
    ]
    for load in loads:
        load.start()
    barrier = pltpu.get_barrier_semaphore()
    for off in range(1, nx):
        pl.semaphore_signal(
            barrier, inc=1, device_id={"sp": z * nx + (x + off) % nx}, device_id_type=MESH)
    for off in range(1, nz):
        pl.semaphore_signal(
            barrier, inc=1, device_id={"sp": (z + off) % nz * nx + x}, device_id_type=MESH)
    for off in range(1, ntp):
        pl.semaphore_signal(barrier, inc=1, device_id={"tp": (mine + off) % ntp}, device_id_type=MESH)

    row = lax.broadcasted_iota(jnp.int32, (tokens, tokens), 0)
    col = lax.broadcasted_iota(jnp.int32, (tokens, tokens), 1)
    below = col <= row
    inside = below & (col // BLOCK == row // BLOCK)
    tri = jnp.where(below, 1.0, 0.0).astype(BF16)
    tri_in = jnp.where(inside, 1.0, 0.0).astype(BF16)
    upper = jnp.where(col >= row, 1.0, 0.0).astype(BF16)
    last_in = jnp.where(col // BLOCK == row // BLOCK, 1.0, 0.0).astype(BF16)

    def hd(h):
        return slice(h * DK, (h + 1) * DK)

    def hv(h):
        return slice(h * DV, (h + 1) * DV)

    loads[0].wait()
    g_parts = pieces(g_ref[...], 3)
    span_buf[...] = sum(nn(tri, part_) for part_ in g_parts)
    c_buf[...] = sum(nn(tri_in, part_) for part_ in g_parts)
    total = span_buf[tokens - 1 : tokens, :]
    decay = jnp.exp(total)

    def scatter_copy(d, m, h):
        return pltpu.make_async_remote_copy(
            src_ref=a_out.at[d, m, h], dst_ref=a_in.at[d, x, h],
            send_sem=a_send.at[d, m, h], recv_sem=a_recv.at[d, x, h],
            device_id={"sp": z * nx + m}, device_id_type=MESH)

    def scatter_wait(d, h):
        for m in range(nx):
            @pl.when(m != x)
            def _():
                pltpu.make_async_remote_copy(
                    src_ref=a_out.at[d, m, h], dst_ref=a_in.at[d, m, h],
                    send_sem=a_send.at[d, m, h], recv_sem=a_recv.at[d, m, h],
                    device_id={"sp": z * nx + m}, device_id_type=MESH).wait_recv()

    def give(d, h, totals):
        for m in range(nx):
            a_out[d, m, h, :dvx, :] = totals[m * dvx : (m + 1) * dvx]
            a_out[d, m, h, dvx:, :] = jnp.broadcast_to(decay[:, hd(h)], (8, DK))
        for m in range(nx):
            @pl.when(m != x)
            def _():
                scatter_copy(d, m, h).start()

            @pl.when(m == x)
            def _():
                a_in[d, m, h] = a_out[d, m, h]

    loads[1].wait()
    q_all = q_ref[...].astype(F32) * scale
    q_span = (q_all * jnp.exp(span_buf[...])).astype(BF16)
    loads[2].wait()
    for h in range(heads):
        adjoint = tn(o_ref[:, hv(h)], q_span[:, hd(h)])
        if h == 0:
            pl.semaphore_wait(barrier, nx - 1 + nz - 1 + ntp - 1)
        give(1, h, adjoint)

    loads[4].wait()
    depth = x_ref.shape[1]
    for at in range(0, depth, 256):
        xt_buf[at : at + 256, :] = x_ref[:, at : at + 256].T

    own = dw_ref.shape[0]
    cols = dw_ref.shape[1]
    wide = min(cols, 128)
    chunks = cols // wide
    half_r = own // 2
    near, mirror = z + 1 - 2 * (z % 2), nz - 1 - z
    core_mate, row_mate = mine + 1 - 2 * (mine % 2), (mine + 2) % 4

    def gather_with(mode):
        return near if mode == 0 else mirror

    def scatter_with(mode):
        return mirror if mode == 0 else near

    def block_rows(slab, xx, base=0, size=None):
        return pl.ds(pl.multiple_of((slab * nx + xx) * own + base, half_r), own if size is None else size)

    def x_copy(mode):
        return pltpu.make_async_remote_copy(
            src_ref=xs_out.at[mode], dst_ref=xr_in.at[mode, mine],
            send_sem=xs_send.at[mode, 0], recv_sem=xr_recv.at[mode, mine],
            device_id={"sp": gather_with(mode) * nx + x}, device_id_type=MESH)

    def x_pass(mode, which, block, mate):
        return pltpu.make_async_remote_copy(
            src_ref=xr_in.at[mode, block], dst_ref=xr_in.at[mode, block],
            send_sem=xs_send.at[mode, which], recv_sem=xr_recv.at[mode, block],
            device_id={"tp": mate}, device_id_type=MESH)

    def x_send(mode):
        slab = gather_with(mode)
        other = nz - 1 - slab if mode == 0 else slab + 1 - 2 * (slab % 2)
        slab = jnp.where(mine < nx, other, slab)
        xs_out[mode] = xt_buf[block_rows(slab, mine % nx), :].astype(F32)
        x_copy(mode).start()

    def x_relay(mode):
        x_copy(mode).wait_recv()
        x_pass(mode, 1, mine, core_mate).start()
        x_pass(mode, 2, mine, row_mate).start()

    def x_forward(mode):
        x_pass(mode, 2, row_mate, row_mate).wait_recv()
        x_pass(mode, 3, row_mate, core_mate).start()

    def x_take(mode):
        x_pass(mode, 1, core_mate, core_mate).wait_recv()
        far_mate = (core_mate + 2) % 4
        x_pass(mode, 3, far_mate, core_mate).wait_recv()
        for j in range(2 * nx):
            xr_buf[mode, j] = xr_in[mode, j].astype(BF16)

    if cube:
        @pl.when(z < nz - 1)
        def _():
            x_send(0)

    loads[3].wait()
    loads[5].wait()
    k_all = k_ref[...].astype(F32)
    k_far = jnp.exp(total - span_buf[...])
    k_span = (k_all * k_far).astype(BF16)
    for h in range(heads):
        v_buf[:, hv(h)] = nn(x_ref[...], w_ref[:, hv(h)]).astype(BF16)
        give(0, h, tn(v_buf[:, hv(h)], k_span[:, hd(h)]))

    def order(d):
        return range(nx) if d == 0 else range(nx - 1, -1, -1)

    def plane_copy(dz):
        return pltpu.make_async_remote_copy(
            src_ref=z_out, dst_ref=z_in.at[z],
            send_sem=z_send.at[dz], recv_sem=z_recv.at[z],
            device_id={"sp": (z + dz) * nx + x}, device_id_type=MESH)

    def composite(d, h, rows_):
        acc, dec = None, None
        for m in order(d):
            local, rate = a_in[d, m, h, rows_, :], a_in[d, m, h, dvx : dvx + 1, :]
            acc = local if acc is None else local + rate * acc
            dec = rate if dec is None else rate * dec
        return acc, dec

    def forward_start():
        for h in range(heads):
            scatter_wait(0, h)
            acc, dec = composite(0, h, slice(0, dvx))
            z_out[h, :dvx, :] = acc
            z_out[h, dvx:, :] = jnp.broadcast_to(dec, (8, DK))
        for dz in range(1, nz):
            @pl.when(z + dz < nz)
            def _():
                plane_copy(dz).start()

    @pl.when(z < nz - 2)
    def _():
        forward_start()

    if cube:
        @pl.when(z < nz - 2)
        def _():
            x_relay(0)

    half_v = dvx // 4

    def chain_copy(c):
        return pltpu.make_async_remote_copy(
            src_ref=h_out.at[c], dst_ref=h_in.at[c],
            send_sem=h_send.at[c], recv_sem=h_recv.at[c],
            device_id={"sp": (z - 1) * nx + x}, device_id_type=MESH)

    def piece_copy(m, c):
        return pltpu.make_async_remote_copy(
            src_ref=b_out.at[m, c], dst_ref=b_in.at[x, c],
            send_sem=b_send.at[m, c], recv_sem=b_recv.at[x, c],
            device_id={"sp": z * nx + m}, device_id_type=MESH)

    for c in range(4 * heads):
        h, rows_ = c // 4, slice(c % 4 * half_v, (c % 4 + 1) * half_v)
        if c % 4 == 0:
            scatter_wait(1, h)
        acc, dec = composite(1, h, rows_)

        @pl.when(z == nz - 1)
        def _():
            h_in[c] = jnp.zeros((half_v, DK), F32)

        @pl.when(z < nz - 1)
        def _():
            chain_copy(c).wait_recv()

        enter = h_in[c]

        @pl.when(z > 0)
        def _():
            h_out[c] = acc + dec * enter
            chain_copy(c).start()

        for m in order(1):
            b_out[m, c] = enter
            enter = a_in[1, m, h, rows_, :] + a_in[1, m, h, dvx : dvx + 1, :] * enter
        for m in range(nx):
            @pl.when(m != x)
            def _():
                piece_copy(m, c).start()

            @pl.when(m == x)
            def _():
                b_in[m, c] = b_out[m, c]

    @pl.when(z == nz - 2)
    def _():
        forward_start()

    @pl.when(z == nz - 1)
    def _():
        if cube:
            x_send(0)
        for h in range(heads):
            scatter_wait(0, h)

    cum = c_buf[...]
    block_end = sum(nn(last_in, part_) for part_ in g_parts)
    k_tail = jnp.exp(block_end - cum)
    grow = jnp.exp(cum)
    qg_buf[...] = (q_all * grow).astype(BF16)
    ks_buf[...] = (k_all * jnp.exp(-cum)).astype(BF16)
    kt_buf[...] = (k_all * k_tail).astype(BF16)
    st_buf[...] = jnp.zeros_like(st_buf)

    def adjoint_step(step, carry):
        rows = pl.ds(pl.multiple_of((blocks - 1 - step) * BLOCK, BLOCK), BLOCK)
        for h in range(heads):
            keep = jnp.exp(c_buf[rows, hd(h)][BLOCK - 1 :])
            adjoint = st_buf[1, h]
            narrow = adjoint.astype(BF16)
            kp_buf[rows, hd(h)] = nn(v_buf[rows, hv(h)], narrow)
            vp_buf[rows, hv(h)] = nt(kt_buf[rows, hd(h)], narrow)
            st_buf[1, h] = keep * adjoint + tn(o_ref[rows, hv(h)], qg_buf[rows, hd(h)])
        return carry

    def state_step(step, carry):
        rows = pl.ds(pl.multiple_of(step * BLOCK, BLOCK), BLOCK)
        for h in range(heads):
            keep = jnp.exp(c_buf[rows, hd(h)][BLOCK - 1 :])
            state = st_buf[0, h]
            y_buf[rows, hd(h)] = nn(o_ref[rows, hv(h)], state.astype(BF16))
            st_buf[0, h] = keep * state + tn(v_buf[rows, hv(h)], kt_buf[rows, hd(h)])
        return carry

    lax.fori_loop(0, blocks, adjoint_step, 0)

    for h in range(heads):
        dots = jnp.where(inside, nt(qg_buf[:, hd(h)], ks_buf[:, hd(h)]), 0.0).astype(BF16)
        vp_buf[:, hv(h)] += tn(dots, o_ref[:, hv(h)])

    def member_copy(m):
        return pltpu.make_async_remote_copy(
            src_ref=c_out.at[m], dst_ref=c_in.at[x],
            send_sem=c_send.at[m], recv_sem=c_recv.at[x],
            device_id={"sp": z * nx + m}, device_id_type=MESH)

    def forward_spread():
        z_acc[...] = jnp.zeros_like(z_acc)
        for zp in range(nz):
            @pl.when(zp < z)
            def _():
                pltpu.make_async_remote_copy(
                    src_ref=z_out, dst_ref=z_in.at[zp],
                    send_sem=z_send.at[0], recv_sem=z_recv.at[zp],
                    device_id={"sp": zp * nx + x}, device_id_type=MESH).wait_recv()
                for h in range(heads):
                    z_acc[h] = z_in[zp, h, :dvx, :] + z_in[zp, h, dvx : dvx + 1, :] * z_acc[h]
        for h in range(heads):
            acc = z_acc[h]
            for m in order(0):
                c_out[m, h] = acc
                acc = a_in[0, m, h, :dvx, :] + a_in[0, m, h, dvx : dvx + 1, :] * acc
        for m in range(nx):
            @pl.when(m != x)
            def _():
                member_copy(m).start()

            @pl.when(m == x)
            def _():
                c_in[m] = c_out[m]

    modes = [0] * chunks

    def near_copy(c):
        return pltpu.make_async_remote_copy(
            src_ref=vx_out.at[c], dst_ref=vx_in.at[c],
            send_sem=v_send.at[c], recv_sem=v_recv.at[c],
            device_id={"sp": gather_with(modes[c]) * nx + x}, device_id_type=MESH)

    def side_copy(c, s, u):
        return pltpu.make_async_remote_copy(
            src_ref=sx_out.at[c, s, u], dst_ref=sx_in.at[c, s, u],
            send_sem=sx_send.at[c, s, u], recv_sem=sx_recv.at[c, s, u],
            device_id={"sp": z * nx + 1 - x}, device_id_type=MESH)

    def far_copy(c, u):
        return pltpu.make_async_remote_copy(
            src_ref=sm_out.at[c, u], dst_ref=sm_in.at[c, u],
            send_sem=sm_send.at[c, u], recv_sem=sm_recv.at[c, u],
            device_id={"sp": scatter_with(modes[c]) * nx + x}, device_id_type=MESH)

    def piece(c, s, xx):
        at = slice(c * wide, (c + 1) * wide)
        slab = scatter_with(modes[c]) if s == 0 else z
        return nn(xt_buf[block_rows(slab, xx), :], vg_buf[:, at]) + nn(
            xr_buf[modes[c], s * nx + xx], vgp_buf[:, at])

    def take_near(c):
        near_copy(c).wait_recv()
        vgp_buf[:, c * wide : (c + 1) * wide] = vx_in[c].astype(BF16)

    def side_send(c, s):
        value = piece(c, s, 1 - x)
        for u in range(2):
            sx_out[c, s, u] = value[u * half_r : (u + 1) * half_r]
            side_copy(c, s, u).start()

    def keep(c, s):
        value = piece(c, s, x)
        for u in range(2):
            acc_buf[c, s, u] = value[u * half_r : (u + 1) * half_r]

    def far_send(c):
        for u in range(2):
            side_copy(c, 0, u).wait_recv()
            sm_out[c, u] = acc_buf[c, 0, u] + sx_in[c, 0, u]
            far_copy(c, u).start()

    for h in range(heads):
        for m in range(nx):
            for c in range(4 * h, 4 * (h + 1)):
                @pl.when(m != x)
                def _():
                    pltpu.make_async_remote_copy(
                        src_ref=b_out.at[m, c], dst_ref=b_in.at[m, c],
                        send_sem=b_send.at[m, c], recv_sem=b_recv.at[m, c],
                        device_id={"sp": z * nx + m}, device_id_type=MESH).wait_recv()
                at = m * dvx + c % 4 * half_v
                fr_buf[h, at : at + half_v, :] = b_in[m, c]
        narrow = fr_buf[h].astype(BF16)
        vg_buf[:, hv(h)] = (vp_buf[:, hv(h)] + nt(k_span[:, hd(h)], narrow)).astype(BF16)
        if cube:
            for c in range(h * DV // wide, (h + 1) * DV // wide):
                vx_out[c] = vg_buf[:, c * wide : (c + 1) * wide].astype(F32)
                near_copy(c).start()

    half_c = cols // 2
    p = ring_place(z, x, nz, nx)
    ahead = ring_member((p + 1) % n, nz, nx)
    behind = ring_member((p + n - 1) % n, nz, nx)

    def share(d, u, owner):
        rows_ = pl.ds(pl.multiple_of(owner * own + u * half_r, half_r), half_r)
        return nn(xt_buf[rows_, :], vg_buf[:, d * half_c : (d + 1) * half_c])

    def ring_copy(step, d, u, src):
        return pltpu.make_async_remote_copy(
            src_ref=src, dst_ref=ring.at[step, d, u],
            send_sem=r_send.at[step, d, u], recv_sem=r_recv.at[step, d, u],
            device_id={"sp": ahead if d == 0 else behind}, device_id_type=MESH)

    def owner_at(step, d):
        return ring_member((p + n - step - 1) % n if d == 0 else (p + step + 1) % n, nz, nx)

    if not cube:
        for u in range(2):
            for d in range(2):
                first[d, u] = share(d, u, owner_at(0, d))
                ring_copy(0, d, u, first.at[d, u]).start()

    else:
        @pl.when(z >= nz - 2)
        def _():
            x_relay(0)

        @pl.when(z < nz - 2)
        def _():
            x_forward(0)
            forward_spread()

    lax.fori_loop(0, blocks, state_step, 0)
    for h in range(heads):
        dots = jnp.where(inside, nt(o_ref[:, hv(h)], v_buf[:, hv(h)]), 0.0).astype(BF16)
        y_buf[:, hd(h)] += nn(dots, ks_buf[:, hd(h)])
        k_grad = (
            k_tail[:, hd(h)] * kp_buf[:, hd(h)]
            + jnp.exp(-cum[:, hd(h)]) * tn(dots, qg_buf[:, hd(h)])
            + k_far[:, hd(h)] * nn(v_buf[:, hv(h)], fr_buf[h].astype(BF16))
        )
        kp_buf[:, hd(h)] = k_grad
        dk_ref[:, hd(h)] = k_grad.astype(BF16)

    def query_side(first_head=0, last_head=heads):
        for m in range(nx):
            if first_head:
                break

            @pl.when(m != x)
            def _():
                pltpu.make_async_remote_copy(
                    src_ref=c_out.at[m], dst_ref=c_in.at[m],
                    send_sem=c_send.at[m], recv_sem=c_recv.at[m],
                    device_id={"sp": z * nx + m}, device_id_type=MESH).wait_recv()
        for h in range(first_head, last_head):
            state_in = jnp.concatenate([c_in[m, h] for m in range(nx)], axis=0)
            q_side = q_ref[:, hd(h)].astype(F32) * scale
            k_side = k_ref[:, hd(h)].astype(F32)
            q_grad = jnp.exp(c_buf[:, hd(h)]) * y_buf[:, hd(h)] + jnp.exp(span_buf[:, hd(h)]) * nn(
                o_ref[:, hv(h)], state_in.astype(BF16)
            )
            dq_ref[:, hd(h)] = (q_grad * scale).astype(BF16)
            terms = q_side * q_grad - k_side * kp_buf[:, hd(h)]
            far = jnp.exp(span_buf[tokens - 1 : tokens, hd(h)])
            span_end = st_buf[0, h] + far * state_in
            carry = jnp.sum(fr_buf[h] * span_end, axis=0, keepdims=True)
            dg_ref[:, hd(h)] = sum(nn(upper, part_) for part_ in pieces(terms, 3)) + carry

    def ring_step(step, carry):
        for d in range(2):
            for u in range(2):
                part[d, u] = share(d, u, owner_at(step, d))
        for u in range(2):
            for d in range(2):
                ring_copy(step - 1, d, u, first.at[d, u]).wait_recv()
                ring[step - 1, d, u] += part[d, u]
                ring_copy(step, d, u, ring.at[step - 1, d, u]).start()

        @pl.when(step == 2)
        def _():
            forward_spread()

        @pl.when(step == 4)
        def _():
            query_side()

        return carry

    if not cube:
        lax.fori_loop(1, n - 1, ring_step, 0)

        for d in range(2):
            for u in range(2):
                part[d, u] = share(d, u, me)
        for u in range(2):
            squares = 0.0
            for d in range(2):
                ring_copy(n - 2, d, u, first.at[d, u]).wait_recv()
                done = ring[n - 2, d, u] + part[d, u]
                dw_ref[u * half_r : (u + 1) * half_r, d * half_c : (d + 1) * half_c] = done
                for at in range(0, half_c, 128):
                    squares = squares + done[:, at : at + 128] * done[:, at : at + 128]
            norm_out[u] = jnp.broadcast_to(jnp.sum(squares.T, axis=0, keepdims=True), (8, half_r))
    else:
        @pl.when(z >= nz - 2)
        def _():
            x_forward(0)
            forward_spread()

        x_take(0)
        take_near(0)
        side_send(0, 0)
        keep(0, 0)
        side_send(0, 1)
        keep(0, 1)
        for c in range(1, chunks):
            take_near(c)
            side_send(c, 0)
            keep(c, 0)
            far_send(c - 1)
            side_send(c, 1)
            keep(c, 1)
            if c == chunks - 2:
                query_side(0, 1)
        far_send(chunks - 1)
        query_side(1, heads)
        squares = [0.0, 0.0]
        for c in range(chunks):
            for u in range(2):
                side_copy(c, 1, u).wait_recv()
                far_copy(c, u).wait_recv()
                done = acc_buf[c, 1, u] + sx_in[c, 1, u] + sm_in[c, u]
                dw_ref[u * half_r : (u + 1) * half_r, c * wide : (c + 1) * wide] = done
                squares[u] = squares[u] + done * done
        for u in range(2):
            norm_out[u] = jnp.broadcast_to(jnp.sum(squares[u].T, axis=0, keepdims=True), (8, half_r))

    def norm_copy(off):
        return pltpu.make_async_remote_copy(
            src_ref=norm_out, dst_ref=norm_in.at[off],
            send_sem=n_send.at[off], recv_sem=n_recv.at[off],
            device_id={"tp": (mine + off) % ntp}, device_id_type=MESH)

    for off in range(1, ntp):
        norm_copy(off).start()

    for m in range(nx):
        @pl.when(m != x)
        def _():
            for h in range(heads):
                for d in range(2):
                    scatter_copy(d, m, h).wait_send()
            for c in range(4 * heads):
                piece_copy(m, c).wait_send()
            member_copy(m).wait_send()
    for dz in range(1, nz):
        @pl.when(z + dz < nz)
        def _():
            plane_copy(dz).wait_send()

    @pl.when(z > 0)
    def _():
        for c in range(4 * heads):
            chain_copy(c).wait_send()

    if not cube:
        def sent(step, carry):
            for u in range(2):
                for d in range(2):
                    ring_copy(step, d, u, first.at[d, u]).wait_send()
            return carry

        lax.fori_loop(0, n - 1, sent, 0)
    else:
        x_copy(0).wait_send()
        x_pass(0, 1, mine, core_mate).wait_send()
        x_pass(0, 2, mine, row_mate).wait_send()
        x_pass(0, 3, row_mate, core_mate).wait_send()
        for c in range(chunks):
            near_copy(c).wait_send()
            for u in range(2):
                side_copy(c, 0, u).wait_send()
                side_copy(c, 1, u).wait_send()
                far_copy(c, u).wait_send()

    norms = norm_out[...]
    for off in range(1, ntp):
        norm_copy(off).wait()
        norms = norms + norm_in[off]
    rn_ref[...] = norms


def finish(*refs):
    sems = refs[10]
    writes = [pltpu.make_async_copy(refs[i], refs[5 + i], sems.at[i]) for i in range(4)]
    for write in writes:
        write.start()
    refs[9][...] = refs[4][:, :1]
    for write in writes:
        write.wait()


def on_device(n, nx, ntp, block_input, queries, keys, w_value, log_decay, d_out):
    tokens, wide = queries.shape
    heads = wide // DK
    cols = w_value.shape[1]
    depth = block_input.shape[1]
    own = depth // n
    nz = n // nx
    dvx = DV // nx
    vm = pltpu.VMEM
    dma = pltpu.SemaphoreType.DMA
    wide_c = min(cols, 128)
    chunks, half = cols // wide_c, own // 2
    late = [
        vm((2, 2, half, cols // 2), F32),
        vm((2, 2, half, cols // 2), F32),
        vm((n - 1, 2, 2, half, cols // 2), F32),
        dma((n - 1, 2, 2)),
        dma((n - 1, 2, 2)),
    ]
    if is_cube(n, nx, ntp):
        late = [
            vm((2, own, tokens), F32),
            vm((2, ntp, own, tokens), F32),
            vm((2, ntp, own, tokens), BF16),
            vm((chunks, tokens, wide_c), F32),
            vm((chunks, tokens, wide_c), F32),
            vm((tokens, cols), BF16),
            vm((chunks, 2, 2, half, wide_c), F32),
            vm((chunks, 2, 2, half, wide_c), F32),
            vm((chunks, 2, 2, half, wide_c), F32),
            vm((chunks, 2, half, wide_c), F32),
            vm((chunks, 2, half, wide_c), F32),
            dma((2, 4)),
            dma((2, ntp)),
            dma((chunks,)),
            dma((chunks,)),
            dma((chunks, 2, 2)),
            dma((chunks, 2, 2)),
            dma((chunks, 2)),
            dma((chunks, 2)),
        ]
    out = pl.pallas_call(
        functools.partial(kernel, n, nx, ntp),
        out_shape=(
            vm((tokens, wide), BF16),
            vm((tokens, wide), BF16),
            vm((tokens, wide), F32),
            vm((own, cols), F32),
            vm((2, 8, own // 2), F32),
        ),
        in_specs=[pl.BlockSpec(memory_space=pltpu.HBM)] * 6,
        out_specs=(pl.BlockSpec(memory_space=vm),) * 5,
        scratch_shapes=[
            vm(block_input.shape, BF16),
            vm(queries.shape, BF16),
            vm(keys.shape, BF16),
            vm(w_value.shape, BF16),
            vm(log_decay.shape, F32),
            vm(d_out.shape, BF16),
            dma((6,)),
            vm((tokens, wide), F32),
            vm((tokens, wide), F32),
            vm((tokens, cols), BF16),
            vm((tokens, wide), BF16),
            vm((tokens, wide), BF16),
            vm((tokens, wide), BF16),
            vm((tokens, wide), F32),
            vm((tokens, wide), F32),
            vm((tokens, cols), F32),
            vm((2, heads, DV, DK), F32),
            vm((depth, tokens), BF16),
            vm((tokens, cols), BF16),
            vm((2, nx, heads, dvx + 8, DK), F32),
            vm((2, nx, heads, dvx + 8, DK), F32),
            vm((heads, dvx + 8, DK), F32),
            vm((nz, heads, dvx + 8, DK), F32),
            vm((heads, dvx, DK), F32),
            vm((nx, heads, dvx, DK), F32),
            vm((nx, heads, dvx, DK), F32),
            vm((4 * heads, dvx // 4, DK), F32),
            vm((4 * heads, dvx // 4, DK), F32),
            vm((nx, 4 * heads, dvx // 4, DK), F32),
            vm((nx, 4 * heads, dvx // 4, DK), F32),
            vm((heads, DV, DK), F32),
            vm((2, 8, own // 2), F32),
            vm((ntp, 2, 8, own // 2), F32),
            dma((2, nx, heads)),
            dma((2, nx, heads)),
            dma((nz,)),
            dma((nz,)),
            dma((nx,)),
            dma((nx,)),
            dma((4 * heads,)),
            dma((4 * heads,)),
            dma((nx, 4 * heads)),
            dma((nx, 4 * heads)),
            dma((ntp,)),
            dma((ntp,)),
            *late,
        ],
        compiler_params=pltpu.CompilerParams(
            collective_id=0, has_side_effects=True, vmem_limit_bytes=62 * 1024 * 1024
        ),
    )(block_input, queries, keys, w_value, log_decay, d_out)
    final = pl.pallas_call(
        finish,
        out_shape=tuple(jax.ShapeDtypeStruct(a.shape, a.dtype) for a in out[:4])
        + (jax.ShapeDtypeStruct((2, 1, own // 2), F32),),
        in_specs=[pl.BlockSpec(memory_space=vm)] * 5,
        out_specs=(pl.BlockSpec(memory_space=pltpu.HBM),) * 4 + (pl.BlockSpec(memory_space=vm),),
        scratch_shapes=[dma((4,))],
        compiler_params=pltpu.CompilerParams(vmem_limit_bytes=1024 * 1024),
    )(*out)
    return (*final[:4], final[4].reshape(-1))


def solution(mesh):
    n, ntp = mesh.shape["sp"], mesh.shape["tp"]
    nx = 1 << ((n.bit_length() - 1) // 2)
    placed = (
        P("sp", None),
        P("sp", "tp"),
        P("sp", "tp"),
        P(None, "tp"),
        P("sp", "tp"),
        P("sp", "tp"),
    )
    return jax.shard_map(
        functools.partial(on_device, n, nx, ntp),
        mesh=mesh,
        in_specs=placed,
        out_specs=(P("sp", "tp"), P("sp", "tp"), P("sp", "tp"), P("sp", "tp"), P("sp")),
        check_vma=False,
    )
```

```python
import functools

import jax
import jax.numpy as jnp
from jax import lax
from jax.experimental import pallas as pl
from jax.experimental.pallas import tpu as pltpu
from jax.sharding import PartitionSpec as P

DK = 128
DV = 256
BLOCK = 32
F32 = jnp.float32
BF16 = jnp.bfloat16
MESH = pl.DeviceIdType.MESH


def nn(left, right):
    return lax.dot_general(left, right, (((1,), (0,)), ((), ())), preferred_element_type=F32)


def nt(left, right):
    return lax.dot_general(left, right, (((1,), (1,)), ((), ())), preferred_element_type=F32)


def tn(left, right):
    return lax.dot_general(left, right, (((0,), (0,)), ((), ())), preferred_element_type=F32)


def pieces(value, count):
    parts = []
    for _ in range(count):
        part = value.astype(BF16)
        parts.append(part)
        value = value - part.astype(F32)
    return parts


def ring_place(z, x, nz, nx):
    r = nz - 1 - z
    across = jnp.where(r % 2 == 0, x - 1, nx - 1 - x)
    return jnp.where(x == 0, z, nz + r * (nx - 1) + across)


def ring_member(p, nz, nx):
    u = jnp.maximum(p - nz, 0)
    r = u // (nx - 1)
    w = u % (nx - 1)
    x = jnp.where(r % 2 == 0, 1 + w, nx - 1 - w)
    return jnp.where(p < nz, p * nx, (nz - 1 - r) * nx + x)


def is_cube(n, nx, ntp):
    return nx == 2 and n == 4 * nx and ntp == 2 * nx


def kernel(
    n, nx, ntp,
    x_hbm, q_hbm, k_hbm, w_hbm, g_hbm, o_hbm,
    dq_ref, dk_ref, dg_ref, dw_ref, rn_ref,
    x_ref, q_ref, k_ref, w_ref, g_ref, o_ref, in_sem,
    c_buf, span_buf, v_buf, qg_buf, kt_buf, ks_buf, y_buf, kp_buf, vp_buf, st_buf, xt_buf, vg_buf,
    a_out, a_in, z_out, z_in, z_acc, c_out, c_in, h_out, h_in, b_out, b_in, fr_buf,
    norm_out, norm_in,
    a_send, a_recv, e_recv, z_send, z_recv, c_send, c_recv, h_send, h_recv, b_send, b_recv, n_send, n_recv,
    tail_buf, *late,
):
    cube = is_cube(n, nx, ntp)
    if cube:
        (xs_out, xr_in, xr_buf, vx_out, vx_in, vgp_buf, sx_out, sx_in, acc_buf, sm_out, sm_in,
         xs_send, xr_recv, v_send, v_recv, sx_send, sx_recv, sm_send, sm_recv) = late
    else:
        first, part, ring, r_send, r_recv = late
    nz = n // nx
    me = lax.axis_index("sp")
    mine = lax.axis_index("tp")
    z, x = me // nx, me % nx
    tokens, heads = q_ref.shape[0], q_ref.shape[1] // DK
    blocks = tokens // BLOCK
    dvx = DV // nx
    scale = DK ** (-0.5)
    loads = [
        pltpu.make_async_copy(source, target, in_sem.at[i])
        for i, (source, target) in enumerate(
            [(g_hbm, g_ref), (q_hbm, q_ref), (o_hbm, o_ref), (k_hbm, k_ref), (x_hbm, x_ref), (w_hbm, w_ref)]
        )
    ]
    for load in loads:
        load.start()
    barrier = pltpu.get_barrier_semaphore()
    for off in range(1, nx):
        pl.semaphore_signal(
            barrier, inc=1, device_id={"sp": z * nx + (x + off) % nx}, device_id_type=MESH)
    for off in range(1, nz):
        pl.semaphore_signal(
            barrier, inc=1, device_id={"sp": (z + off) % nz * nx + x}, device_id_type=MESH)
    for off in range(1, ntp):
        pl.semaphore_signal(barrier, inc=1, device_id={"tp": (mine + off) % ntp}, device_id_type=MESH)

    row = lax.broadcasted_iota(jnp.int32, (tokens, tokens), 0)
    col = lax.broadcasted_iota(jnp.int32, (tokens, tokens), 1)
    below = col <= row
    inside = below & (col // BLOCK == row // BLOCK)
    tri = jnp.where(below, 1.0, 0.0).astype(BF16)
    tri_in = jnp.where(inside, 1.0, 0.0).astype(BF16)
    upper = jnp.where(col >= row, 1.0, 0.0).astype(BF16)
    last_in = jnp.where(col // BLOCK == row // BLOCK, 1.0, 0.0).astype(BF16)

    def hd(h):
        return slice(h * DK, (h + 1) * DK)

    def hv(h):
        return slice(h * DV, (h + 1) * DV)

    loads[0].wait()
    g_parts = pieces(g_ref[...], 3)
    span_buf[...] = sum(nn(tri, part_) for part_ in g_parts)
    c_buf[...] = sum(nn(tri_in, part_) for part_ in g_parts)
    total = span_buf[tokens - 1 : tokens, :]
    decay = jnp.exp(total)

    quarter = dvx // 4

    def part_rows(part):
        return slice(8 + part * quarter if part else 0, 8 + (part + 1) * quarter)

    def slot(to, frm):
        return (frm + nx - 1 - to) % nx

    def first_part(m, h, part):
        return pltpu.make_async_remote_copy(
            src_ref=a_out.at[1, m, h, part_rows(part), :], dst_ref=a_in.at[1, x, h, part_rows(part), :],
            send_sem=a_send.at[1, m], recv_sem=e_recv.at[slot(m, x), h * 4 + part],
            device_id={"sp": z * nx + m}, device_id_type=MESH)

    def first_wait(h, part):
        for m in range(nx):
            @pl.when(m != x)
            def _():
                pltpu.make_async_remote_copy(
                    src_ref=a_out.at[1, m, h, part_rows(part), :], dst_ref=a_in.at[1, m, h, part_rows(part), :],
                    send_sem=a_send.at[1, m], recv_sem=e_recv.at[slot(x, m), h * 4 + part],
                    device_id={"sp": z * nx + m}, device_id_type=MESH).wait_recv()

    def scatter_copy(d, m):
        return pltpu.make_async_remote_copy(
            src_ref=a_out.at[d, m], dst_ref=a_in.at[d, x],
            send_sem=a_send.at[d, m], recv_sem=a_recv.at[slot(m, x)],
            device_id={"sp": z * nx + m}, device_id_type=MESH)

    def scatter_wait(d):
        for m in range(nx):
            @pl.when(m != x)
            def _():
                pltpu.make_async_remote_copy(
                    src_ref=a_out.at[d, m], dst_ref=a_in.at[d, m],
                    send_sem=a_send.at[d, m], recv_sem=a_recv.at[slot(x, m)],
                    device_id={"sp": z * nx + m}, device_id_type=MESH).wait_recv()

    def give(d, h, totals):
        for m in range(nx):
            a_out[d, m, h, :8, :] = jnp.broadcast_to(decay[:, hd(h)], (8, DK))
            a_out[d, m, h, 8:, :] = totals[m * dvx : (m + 1) * dvx]
        for m in range(nx):
            @pl.when(m != x)
            def _():
                if d == 1:
                    for part in range(4):
                        first_part(m, h, part).start()
                elif h == heads - 1:
                    scatter_copy(d, m).start()

            @pl.when(m == x)
            def _():
                a_in[d, m, h] = a_out[d, m, h]

    loads[1].wait()
    q_all = q_ref[...].astype(F32) * scale
    q_span = (q_all * jnp.exp(span_buf[...])).astype(BF16)
    loads[2].wait()
    for h in range(heads):
        adjoint = tn(o_ref[:, hv(h)], q_span[:, hd(h)])
        if h == 0:
            pl.semaphore_wait(barrier, nx - 1 + nz - 1 + ntp - 1)
        give(1, h, adjoint)

    loads[4].wait()
    depth = x_ref.shape[1]
    for at in range(0, depth, 256):
        xt_buf[at : at + 256, :] = x_ref[:, at : at + 256].T

    own = dw_ref.shape[0]
    cols = dw_ref.shape[1]
    wide = min(cols, 128)
    chunks = cols // wide
    half_r = own // 2
    near, mirror = z + 1 - 2 * (z % 2), nz - 1 - z
    core_mate, row_mate = mine + 1 - 2 * (mine % 2), (mine + 2) % 4

    def block_rows(slab, xx, base=0, size=None):
        return pl.ds(pl.multiple_of((slab * nx + xx) * own + base, half_r), own if size is None else size)

    def x_copy(p):
        return pltpu.make_async_remote_copy(
            src_ref=xs_out.at[p], dst_ref=xr_in.at[mine, p],
            send_sem=xs_send.at[0], recv_sem=xr_recv.at[mine, p],
            device_id={"sp": near * nx + x}, device_id_type=MESH)

    def x_pass(which, block, p, mate):
        return pltpu.make_async_remote_copy(
            src_ref=xr_in.at[block, p], dst_ref=xr_in.at[block, p],
            send_sem=xs_send.at[which], recv_sem=xr_recv.at[block, p],
            device_id={"tp": mate}, device_id_type=MESH)

    def x_send(p):
        slab = jnp.where(mine < nx, nz - 1 - near, near)
        xs_out[p] = xt_buf[block_rows(slab, mine % nx, p * half_r, half_r), :].astype(F32)
        x_copy(p).start()

    def x_relay(p):
        x_copy(p).wait_recv()
        x_pass(2, mine, p, row_mate).start()
        x_pass(1, mine, p, core_mate).start()

    def x_forward():
        for p in range(2):
            x_pass(2, row_mate, p, row_mate).wait_recv()
            x_pass(3, row_mate, p, core_mate).start()

    def x_take():
        far_mate = (core_mate + 2) % 4
        for p in range(2):
            x_pass(1, core_mate, p, core_mate).wait_recv()
            x_pass(3, far_mate, p, core_mate).wait_recv()
        for j in range(2 * nx):
            for p in range(2):
                xr_buf[j, p * half_r : (p + 1) * half_r] = xr_in[j, p].astype(BF16)

    if cube:
        x_send(0)

        @pl.when(z < nz - 1)
        def _():
            x_send(1)

    loads[3].wait()
    loads[5].wait()
    k_all = k_ref[...].astype(F32)
    k_far = jnp.exp(total - span_buf[...])
    k_span = (k_all * k_far).astype(BF16)
    for h in range(heads):
        v_buf[:, hv(h)] = nn(x_ref[...], w_ref[:, hv(h)]).astype(BF16)
        give(0, h, tn(v_buf[:, hv(h)], k_span[:, hd(h)]))

    def order(d):
        return range(nx) if d == 0 else range(nx - 1, -1, -1)

    def plane_copy(dz):
        return pltpu.make_async_remote_copy(
            src_ref=z_out, dst_ref=z_in.at[z],
            send_sem=z_send.at[dz], recv_sem=z_recv.at[z],
            device_id={"sp": (z + dz) * nx + x}, device_id_type=MESH)

    def composite(d, h, rows_):
        acc, dec = None, None
        for m in order(d):
            local, rate = a_in[d, m, h, rows_, :], a_in[d, m, h, 0:1, :]
            acc = local if acc is None else local + rate * acc
            dec = rate if dec is None else rate * dec
        return acc, dec

    def forward_start():
        scatter_wait(0)
        for h in range(heads):
            acc, dec = composite(0, h, slice(8, 8 + dvx))
            z_out[h, :dvx, :] = acc
            z_out[h, dvx:, :] = jnp.broadcast_to(dec, (8, DK))
        for dz in range(1, nz):
            @pl.when(z + dz < nz)
            def _():
                plane_copy(dz).start()

    def local_side():
        cum = c_buf[...]
        block_end = sum(nn(last_in, part_) for part_ in g_parts)
        k_tail = jnp.exp(block_end - cum)
        tail_buf[...] = k_tail
        grow = jnp.exp(cum)
        qg_buf[...] = (q_all * grow).astype(BF16)
        ks_buf[...] = (k_all * jnp.exp(-cum)).astype(BF16)
        kt_buf[...] = (k_all * k_tail).astype(BF16)
        st_buf[...] = jnp.zeros_like(st_buf)

        def adjoint_step(step, carry):
            rows = pl.ds(pl.multiple_of((blocks - 1 - step) * BLOCK, BLOCK), BLOCK)
            for h in range(heads):
                keep = jnp.exp(c_buf[rows, hd(h)][BLOCK - 1 :])
                adjoint = st_buf[1, h]
                narrow = adjoint.astype(BF16)
                kp_buf[rows, hd(h)] = nn(v_buf[rows, hv(h)], narrow)
                vp_buf[rows, hv(h)] = nt(kt_buf[rows, hd(h)], narrow)
                st_buf[1, h] = keep * adjoint + tn(o_ref[rows, hv(h)], qg_buf[rows, hd(h)])
            return carry

        lax.fori_loop(0, blocks, adjoint_step, 0)

        for h in range(heads):
            dots = jnp.where(inside, nt(qg_buf[:, hd(h)], ks_buf[:, hd(h)]), 0.0).astype(BF16)
            vp_buf[:, hv(h)] += tn(dots, o_ref[:, hv(h)])

    @pl.when(z < nz - 1)
    def _():
        local_side()

    @pl.when(z < nz - 2)
    def _():
        forward_start()

    if cube:
        @pl.when(z < nz - 1)
        def _():
            x_relay(0)

        @pl.when(z < nz - 2)
        def _():
            x_relay(1)

    half_v = dvx // 4

    def chain_copy(c):
        return pltpu.make_async_remote_copy(
            src_ref=h_out.at[c], dst_ref=h_in.at[c],
            send_sem=h_send, recv_sem=h_recv.at[c],
            device_id={"sp": (z - 1) * nx + x}, device_id_type=MESH)

    def piece_copy(m, c):
        return pltpu.make_async_remote_copy(
            src_ref=b_out.at[m, c], dst_ref=b_in.at[x, c],
            send_sem=b_send.at[m], recv_sem=b_recv.at[slot(m, x), c],
            device_id={"sp": z * nx + m}, device_id_type=MESH)

    for c in range(4 * heads):
        h, rows_ = c // 4, slice(8 + c % 4 * half_v, 8 + (c % 4 + 1) * half_v)
        first_wait(h, c % 4)
        acc, dec = composite(1, h, rows_)

        @pl.when(z == nz - 1)
        def _():
            h_in[c] = jnp.zeros((half_v, DK), F32)

        @pl.when(z < nz - 1)
        def _():
            chain_copy(c).wait_recv()

        enter = h_in[c]

        @pl.when(z > 0)
        def _():
            h_out[c] = acc + dec * enter
            chain_copy(c).start()

        for m in order(1):
            b_out[m, c] = enter
            enter = a_in[1, m, h, rows_, :] + a_in[1, m, h, 0:1, :] * enter
        for m in range(nx):
            @pl.when(m != x)
            def _():
                piece_copy(m, c).start()

            @pl.when(m == x)
            def _():
                b_in[m, c] = b_out[m, c]

    @pl.when(z == nz - 1)
    def _():
        if cube:
            x_send(1)
        local_side()


    def state_step(step, carry):
        rows = pl.ds(pl.multiple_of(step * BLOCK, BLOCK), BLOCK)
        for h in range(heads):
            keep = jnp.exp(c_buf[rows, hd(h)][BLOCK - 1 :])
            state = st_buf[0, h]
            y_buf[rows, hd(h)] = nn(o_ref[rows, hv(h)], state.astype(BF16))
            st_buf[0, h] = keep * state + tn(v_buf[rows, hv(h)], kt_buf[rows, hd(h)])
        return carry

    def member_copy(m):
        return pltpu.make_async_remote_copy(
            src_ref=c_out.at[m], dst_ref=c_in.at[x],
            send_sem=c_send.at[m], recv_sem=c_recv.at[x],
            device_id={"sp": z * nx + m}, device_id_type=MESH)

    def forward_spread():
        z_acc[...] = jnp.zeros_like(z_acc)
        for zp in range(nz):
            @pl.when(zp < z)
            def _():
                pltpu.make_async_remote_copy(
                    src_ref=z_out, dst_ref=z_in.at[zp],
                    send_sem=z_send.at[0], recv_sem=z_recv.at[zp],
                    device_id={"sp": zp * nx + x}, device_id_type=MESH).wait_recv()
                for h in range(heads):
                    z_acc[h] = z_in[zp, h, :dvx, :] + z_in[zp, h, dvx : dvx + 1, :] * z_acc[h]
        for h in range(heads):
            acc = z_acc[h]
            for m in order(0):
                c_out[m, h] = acc
                acc = a_in[0, m, h, 8:, :] + a_in[0, m, h, 0:1, :] * acc
        for m in range(nx):
            @pl.when(m != x)
            def _():
                member_copy(m).start()

            @pl.when(m == x)
            def _():
                c_in[m] = c_out[m]

    def near_copy(c):
        return pltpu.make_async_remote_copy(
            src_ref=vx_out.at[c], dst_ref=vx_in.at[c],
            send_sem=v_send, recv_sem=v_recv.at[c],
            device_id={"sp": near * nx + x}, device_id_type=MESH)

    def side_copy(c, s, u):
        return pltpu.make_async_remote_copy(
            src_ref=sx_out.at[c, s, u], dst_ref=sx_in.at[c, s, u],
            send_sem=sx_send, recv_sem=sx_recv.at[c, s, u],
            device_id={"sp": z * nx + 1 - x}, device_id_type=MESH)

    def far_copy(c, u):
        return pltpu.make_async_remote_copy(
            src_ref=sm_out.at[c, u], dst_ref=sm_in.at[c, u],
            send_sem=sm_send, recv_sem=sm_recv.at[c, u],
            device_id={"sp": mirror * nx + x}, device_id_type=MESH)

    def piece(c, s, xx):
        at = slice(c * wide, (c + 1) * wide)
        slab = mirror if s == 0 else z
        return nn(xt_buf[block_rows(slab, xx), :], vg_buf[:, at]) + nn(
            xr_buf[s * nx + xx], vgp_buf[:, at])

    def take_near(c):
        near_copy(c).wait_recv()
        vgp_buf[:, c * wide : (c + 1) * wide] = vx_in[c].astype(BF16)

    def side_send(c, s):
        value = piece(c, s, 1 - x)
        for u in range(2):
            sx_out[c, s, u] = value[u * half_r : (u + 1) * half_r]
            side_copy(c, s, u).start()

    def keep(c, s):
        value = piece(c, s, x)
        for u in range(2):
            acc_buf[c, s, u] = value[u * half_r : (u + 1) * half_r]

    def far_send(c):
        for u in range(2):
            side_copy(c, 0, u).wait_recv()
            sm_out[c, u] = acc_buf[c, 0, u] + sx_in[c, 0, u]
            far_copy(c, u).start()

    for h in range(heads):
        for m in range(nx):
            for c in range(4 * h, 4 * (h + 1)):
                @pl.when(m != x)
                def _():
                    pltpu.make_async_remote_copy(
                        src_ref=b_out.at[m, c], dst_ref=b_in.at[m, c],
                        send_sem=b_send.at[m], recv_sem=b_recv.at[slot(x, m), c],
                        device_id={"sp": z * nx + m}, device_id_type=MESH).wait_recv()
                at = m * dvx + c % 4 * half_v
                fr_buf[h, at : at + half_v, :] = b_in[m, c]
        narrow = fr_buf[h].astype(BF16)
        vg_buf[:, hv(h)] = (vp_buf[:, hv(h)] + nt(k_span[:, hd(h)], narrow)).astype(BF16)
        if cube:
            for c in range(h * DV // wide, (h + 1) * DV // wide):
                vx_out[c] = vg_buf[:, c * wide : (c + 1) * wide].astype(F32)
                near_copy(c).start()

    half_c = cols // 2
    p = ring_place(z, x, nz, nx)
    ahead = ring_member((p + 1) % n, nz, nx)
    behind = ring_member((p + n - 1) % n, nz, nx)

    def share(d, u, owner):
        rows_ = pl.ds(pl.multiple_of(owner * own + u * half_r, half_r), half_r)
        return nn(xt_buf[rows_, :], vg_buf[:, d * half_c : (d + 1) * half_c])

    def ring_copy(step, d, u, src):
        return pltpu.make_async_remote_copy(
            src_ref=src, dst_ref=ring.at[step, d, u],
            send_sem=r_send.at[step, d, u], recv_sem=r_recv.at[step, d, u],
            device_id={"sp": ahead if d == 0 else behind}, device_id_type=MESH)

    def owner_at(step, d):
        return ring_member((p + n - step - 1) % n if d == 0 else (p + step + 1) % n, nz, nx)

    if not cube:
        for u in range(2):
            for d in range(2):
                first[d, u] = share(d, u, owner_at(0, d))
                ring_copy(0, d, u, first.at[d, u]).start()

    @pl.when(z == nz - 2)
    def _():
        forward_start()

    @pl.when(z == nz - 1)
    def _():
        scatter_wait(0)

    if cube:
        @pl.when(z == nz - 1)
        def _():
            x_relay(0)

        @pl.when(z >= nz - 2)
        def _():
            x_relay(1)

        @pl.when(z < nz - 2)
        def _():
            x_forward()
            forward_spread()

    lax.fori_loop(0, blocks, state_step, 0)
    for h in range(heads):
        dots = jnp.where(inside, nt(o_ref[:, hv(h)], v_buf[:, hv(h)]), 0.0).astype(BF16)
        y_buf[:, hd(h)] += nn(dots, ks_buf[:, hd(h)])
        k_grad = (
            tail_buf[:, hd(h)] * kp_buf[:, hd(h)]
            + jnp.exp(-c_buf[:, hd(h)]) * tn(dots, qg_buf[:, hd(h)])
            + k_far[:, hd(h)] * nn(v_buf[:, hv(h)], fr_buf[h].astype(BF16))
        )
        kp_buf[:, hd(h)] = k_grad
        dk_ref[:, hd(h)] = k_grad.astype(BF16)

    def query_side(first_head=0, last_head=heads):
        for m in range(nx):
            if first_head:
                break

            @pl.when(m != x)
            def _():
                pltpu.make_async_remote_copy(
                    src_ref=c_out.at[m], dst_ref=c_in.at[m],
                    send_sem=c_send.at[m], recv_sem=c_recv.at[m],
                    device_id={"sp": z * nx + m}, device_id_type=MESH).wait_recv()
        for h in range(first_head, last_head):
            state_in = jnp.concatenate([c_in[m, h] for m in range(nx)], axis=0)
            q_side = q_ref[:, hd(h)].astype(F32) * scale
            k_side = k_ref[:, hd(h)].astype(F32)
            q_grad = jnp.exp(c_buf[:, hd(h)]) * y_buf[:, hd(h)] + jnp.exp(span_buf[:, hd(h)]) * nn(
                o_ref[:, hv(h)], state_in.astype(BF16)
            )
            dq_ref[:, hd(h)] = (q_grad * scale).astype(BF16)
            terms = q_side * q_grad - k_side * kp_buf[:, hd(h)]
            far = jnp.exp(span_buf[tokens - 1 : tokens, hd(h)])
            span_end = st_buf[0, h] + far * state_in
            carry = jnp.sum(fr_buf[h] * span_end, axis=0, keepdims=True)
            dg_ref[:, hd(h)] = sum(nn(upper, part_) for part_ in pieces(terms, 3)) + carry

    def ring_step(step, carry):
        for d in range(2):
            for u in range(2):
                part[d, u] = share(d, u, owner_at(step, d))
        for u in range(2):
            for d in range(2):
                ring_copy(step - 1, d, u, first.at[d, u]).wait_recv()
                ring[step - 1, d, u] += part[d, u]
                ring_copy(step, d, u, ring.at[step - 1, d, u]).start()

        @pl.when(step == 2)
        def _():
            forward_spread()

        @pl.when(step == 4)
        def _():
            query_side()

        return carry

    if not cube:
        lax.fori_loop(1, n - 1, ring_step, 0)

        for d in range(2):
            for u in range(2):
                part[d, u] = share(d, u, me)
        for u in range(2):
            squares = 0.0
            for d in range(2):
                ring_copy(n - 2, d, u, first.at[d, u]).wait_recv()
                done = ring[n - 2, d, u] + part[d, u]
                dw_ref[u * half_r : (u + 1) * half_r, d * half_c : (d + 1) * half_c] = done
                for at in range(0, half_c, 128):
                    squares = squares + done[:, at : at + 128] * done[:, at : at + 128]
            norm_out[u] = jnp.broadcast_to(jnp.sum(squares.T, axis=0, keepdims=True), (8, half_r))
    else:
        @pl.when(z >= nz - 2)
        def _():
            x_forward()

        x_take()
        take_near(0)
        side_send(0, 0)
        keep(0, 0)
        for c in range(1, chunks):
            take_near(c)
            side_send(c, 0)
            side_send(c - 1, 1)
            keep(c, 0)
            far_send(c - 1)
            keep(c - 1, 1)
            if c == 2:
                @pl.when(z >= nz - 2)
                def _():
                    forward_spread()
        side_send(chunks - 1, 1)
        query_side(0, 1)
        far_send(chunks - 1)
        keep(chunks - 1, 1)
        query_side(1, heads)
        squares = [0.0, 0.0]
        for c in range(chunks):
            for u in range(2):
                side_copy(c, 1, u).wait_recv()
                far_copy(c, u).wait_recv()
                done = acc_buf[c, 1, u] + sx_in[c, 1, u] + sm_in[c, u]
                dw_ref[u * half_r : (u + 1) * half_r, c * wide : (c + 1) * wide] = done
                squares[u] = squares[u] + done * done
        for u in range(2):
            norm_out[u] = jnp.broadcast_to(jnp.sum(squares[u].T, axis=0, keepdims=True), (8, half_r))

    def norm_copy(off):
        return pltpu.make_async_remote_copy(
            src_ref=norm_out, dst_ref=norm_in.at[off],
            send_sem=n_send.at[off], recv_sem=n_recv.at[off],
            device_id={"tp": (mine + off) % ntp}, device_id_type=MESH)

    for off in range(1, ntp):
        norm_copy(off).start()

    for m in range(nx):
        @pl.when(m != x)
        def _():
            for d in range(2):
                pltpu.make_async_remote_copy(
                    src_ref=a_out.at[d, m], dst_ref=a_in.at[d, x],
                    send_sem=a_send.at[d, m], recv_sem=a_recv.at[slot(m, x)],
                    device_id={"sp": z * nx + m}, device_id_type=MESH).wait_send()
            pltpu.make_async_remote_copy(
                src_ref=b_out.at[m], dst_ref=b_in.at[x],
                send_sem=b_send.at[m], recv_sem=b_recv.at[slot(m, x), 0],
                device_id={"sp": z * nx + m}, device_id_type=MESH).wait_send()
            member_copy(m).wait_send()
    for dz in range(1, nz):
        @pl.when(z + dz < nz)
        def _():
            plane_copy(dz).wait_send()

    @pl.when(z > 0)
    def _():
        pltpu.make_async_remote_copy(
            src_ref=h_out, dst_ref=h_in,
            send_sem=h_send, recv_sem=h_recv.at[0],
            device_id={"sp": (z - 1) * nx + x}, device_id_type=MESH).wait_send()

    if not cube:
        def sent(step, carry):
            for u in range(2):
                for d in range(2):
                    ring_copy(step, d, u, first.at[d, u]).wait_send()
            return carry

        lax.fori_loop(0, n - 1, sent, 0)
    else:
        def all_sent(ref, sem):
            pltpu.make_async_remote_copy(
                src_ref=ref, dst_ref=ref, send_sem=sem, recv_sem=v_recv.at[0],
                device_id={"sp": near * nx + x}, device_id_type=MESH).wait_send()

        all_sent(xs_out, xs_send.at[0])
        all_sent(xr_in.at[mine], xs_send.at[1])
        all_sent(xr_in.at[mine], xs_send.at[2])
        all_sent(xr_in.at[row_mate], xs_send.at[3])
        all_sent(vx_out, v_send)
        all_sent(sx_out, sx_send)
        all_sent(sm_out, sm_send)

    norms = norm_out[...]
    for off in range(1, ntp):
        norm_copy(off).wait()
        norms = norms + norm_in[off]
    rn_ref[...] = norms


def finish(*refs):
    sems = refs[10]
    writes = [pltpu.make_async_copy(refs[i], refs[5 + i], sems.at[i]) for i in range(4)]
    for write in writes:
        write.start()
    refs[9][...] = refs[4][:, :1]
    for write in writes:
        write.wait()


def on_device(n, nx, ntp, block_input, queries, keys, w_value, log_decay, d_out):
    tokens, wide = queries.shape
    heads = wide // DK
    cols = w_value.shape[1]
    depth = block_input.shape[1]
    own = depth // n
    nz = n // nx
    dvx = DV // nx
    vm = pltpu.VMEM
    dma = pltpu.SemaphoreType.DMA
    wide_c = min(cols, 128)
    chunks, half = cols // wide_c, own // 2
    late = [
        vm((2, 2, half, cols // 2), F32),
        vm((2, 2, half, cols // 2), F32),
        vm((n - 1, 2, 2, half, cols // 2), F32),
        dma((n - 1, 2, 2)),
        dma((n - 1, 2, 2)),
    ]
    if is_cube(n, nx, ntp):
        late = [
            vm((2, half, tokens), F32),
            vm((ntp, 2, half, tokens), F32),
            vm((ntp, own, tokens), BF16),
            vm((chunks, tokens, wide_c), F32),
            vm((chunks, tokens, wide_c), F32),
            vm((tokens, cols), BF16),
            vm((chunks, 2, 2, half, wide_c), F32),
            vm((chunks, 2, 2, half, wide_c), F32),
            vm((chunks, 2, 2, half, wide_c), F32),
            vm((chunks, 2, half, wide_c), F32),
            vm((chunks, 2, half, wide_c), F32),
            dma((4,)),
            dma((ntp, 2)),
            dma,
            dma((chunks,)),
            dma,
            dma((chunks, 2, 2)),
            dma,
            dma((chunks, 2)),
        ]
    out = pl.pallas_call(
        functools.partial(kernel, n, nx, ntp),
        out_shape=(
            vm((tokens, wide), BF16),
            vm((tokens, wide), BF16),
            vm((tokens, wide), F32),
            vm((own, cols), F32),
            vm((2, 8, own // 2), F32),
        ),
        in_specs=[pl.BlockSpec(memory_space=pltpu.HBM)] * 6,
        out_specs=(pl.BlockSpec(memory_space=vm),) * 5,
        scratch_shapes=[
            vm(block_input.shape, BF16),
            vm(queries.shape, BF16),
            vm(keys.shape, BF16),
            vm(w_value.shape, BF16),
            vm(log_decay.shape, F32),
            vm(d_out.shape, BF16),
            dma((6,)),
            vm((tokens, wide), F32),
            vm((tokens, wide), F32),
            vm((tokens, cols), BF16),
            vm((tokens, wide), BF16),
            vm((tokens, wide), BF16),
            vm((tokens, wide), BF16),
            vm((tokens, wide), F32),
            vm((tokens, wide), F32),
            vm((tokens, cols), F32),
            vm((2, heads, DV, DK), F32),
            vm((depth, tokens), BF16),
            vm((tokens, cols), BF16),
            vm((2, nx, heads, dvx + 8, DK), F32),
            vm((2, nx, heads, dvx + 8, DK), F32),
            vm((heads, dvx + 8, DK), F32),
            vm((nz, heads, dvx + 8, DK), F32),
            vm((heads, dvx, DK), F32),
            vm((nx, heads, dvx, DK), F32),
            vm((nx, heads, dvx, DK), F32),
            vm((4 * heads, dvx // 4, DK), F32),
            vm((4 * heads, dvx // 4, DK), F32),
            vm((nx, 4 * heads, dvx // 4, DK), F32),
            vm((nx, 4 * heads, dvx // 4, DK), F32),
            vm((heads, DV, DK), F32),
            vm((2, 8, own // 2), F32),
            vm((ntp, 2, 8, own // 2), F32),
            dma((2, nx)),
            dma((nx - 1,)),
            dma((nx - 1, 4 * heads)),
            dma((nz,)),
            dma((nz,)),
            dma((nx,)),
            dma((nx,)),
            dma,
            dma((4 * heads,)),
            dma((nx,)),
            dma((nx - 1, 4 * heads)),
            dma((ntp,)),
            dma((ntp,)),
            vm((tokens, wide), F32),
            *late,
        ],
        compiler_params=pltpu.CompilerParams(
            collective_id=0, has_side_effects=True, vmem_limit_bytes=62 * 1024 * 1024
        ),
    )(block_input, queries, keys, w_value, log_decay, d_out)
    final = pl.pallas_call(
        finish,
        out_shape=tuple(jax.ShapeDtypeStruct(a.shape, a.dtype) for a in out[:4])
        + (jax.ShapeDtypeStruct((2, 1, own // 2), F32),),
        in_specs=[pl.BlockSpec(memory_space=vm)] * 5,
        out_specs=(pl.BlockSpec(memory_space=pltpu.HBM),) * 4 + (pl.BlockSpec(memory_space=vm),),
        scratch_shapes=[dma((4,))],
        compiler_params=pltpu.CompilerParams(vmem_limit_bytes=1024 * 1024),
    )(*out)
    return (*final[:4], final[4].reshape(-1))


def solution(mesh):
    n, ntp = mesh.shape["sp"], mesh.shape["tp"]
    nx = 1 << ((n.bit_length() - 1) // 2)
    placed = (
        P("sp", None),
        P("sp", "tp"),
        P("sp", "tp"),
        P(None, "tp"),
        P("sp", "tp"),
        P("sp", "tp"),
    )
    return jax.shard_map(
        functools.partial(on_device, n, nx, ntp),
        mesh=mesh,
        in_specs=placed,
        out_specs=(P("sp", "tp"), P("sp", "tp"), P("sp", "tp"), P("sp", "tp"), P("sp")),
        check_vma=False,
    )
```

```python
import functools

import jax
import jax.numpy as jnp
from jax import lax
from jax.experimental import pallas as pl
from jax.experimental.pallas import tpu as pltpu
from jax.sharding import PartitionSpec as P

DK = 128
DV = 256
BLOCK = 32
F32 = jnp.float32
BF16 = jnp.bfloat16
MESH = pl.DeviceIdType.MESH


def nn(left, right):
    return lax.dot_general(left, right, (((1,), (0,)), ((), ())), preferred_element_type=F32)


def nt(left, right):
    return lax.dot_general(left, right, (((1,), (1,)), ((), ())), preferred_element_type=F32)


def tn(left, right):
    return lax.dot_general(left, right, (((0,), (0,)), ((), ())), preferred_element_type=F32)


def pieces(value, count):
    parts = []
    for _ in range(count):
        part = value.astype(BF16)
        parts.append(part)
        value = value - part.astype(F32)
    return parts


def ring_place(z, x, nz, nx):
    r = nz - 1 - z
    across = jnp.where(r % 2 == 0, x - 1, nx - 1 - x)
    return jnp.where(x == 0, z, nz + r * (nx - 1) + across)


def ring_member(p, nz, nx):
    u = jnp.maximum(p - nz, 0)
    r = u // (nx - 1)
    w = u % (nx - 1)
    x = jnp.where(r % 2 == 0, 1 + w, nx - 1 - w)
    return jnp.where(p < nz, p * nx, (nz - 1 - r) * nx + x)


def is_cube(n, nx, ntp):
    return nx == 2 and n == 4 * nx and ntp == 2 * nx


def kernel(
    n, nx, ntp,
    x_hbm, q_hbm, k_hbm, w_hbm, g_hbm, o_hbm,
    dq_ref, dk_ref, dg_ref, dw_ref, rn_ref,
    x_ref, q_ref, k_ref, w_ref, g_ref, o_ref, in_sem,
    c_buf, span_buf, v_buf, qg_buf, kt_buf, ks_buf, y_buf, kp_buf, vp_buf, st_buf, xt_buf, vg_buf,
    a_out, a_in, z_out, z_in, z_acc, c_out, c_in, h_out, h_in, b_out, b_in, fr_buf,
    norm_out, norm_in,
    a_send, a_recv, e_recv, z_send, z_recv, c_send, c_recv, h_send, h_recv, b_send, b_recv, n_send, n_recv,
    tail_buf, *late,
):
    cube = is_cube(n, nx, ntp) and dw_ref.shape[1] == 2 * DV
    if cube:
        (xs_out, xr_in, xr_buf, vx_out, vx_in, vgp_buf, sx_out, sx_in, acc_buf, sm_out, sm_in,
         xs_send, xr_recv, v_send, v_recv, sx_send, sx_recv, sm_send, sm_recv) = late
    else:
        first, part, ring, r_send, r_recv = late
    nz = n // nx
    me = lax.axis_index("sp")
    mine = lax.axis_index("tp")
    z, x = me // nx, me % nx
    tokens, heads = q_ref.shape[0], q_ref.shape[1] // DK
    blocks = tokens // BLOCK
    dvx = DV // nx
    scale = DK ** (-0.5)
    loads = [
        pltpu.make_async_copy(source, target, in_sem.at[i])
        for i, (source, target) in enumerate(
            [(g_hbm, g_ref), (q_hbm, q_ref), (o_hbm, o_ref), (k_hbm, k_ref), (x_hbm, x_ref), (w_hbm, w_ref)]
        )
    ]
    for load in loads:
        load.start()
    barrier = pltpu.get_barrier_semaphore()
    for off in range(1, nx):
        pl.semaphore_signal(
            barrier, inc=1, device_id={"sp": z * nx + (x + off) % nx}, device_id_type=MESH)
    for off in range(1, nz):
        pl.semaphore_signal(
            barrier, inc=1, device_id={"sp": (z + off) % nz * nx + x}, device_id_type=MESH)
    for off in range(1, ntp):
        pl.semaphore_signal(barrier, inc=1, device_id={"tp": (mine + off) % ntp}, device_id_type=MESH)

    row = lax.broadcasted_iota(jnp.int32, (tokens, tokens), 0)
    col = lax.broadcasted_iota(jnp.int32, (tokens, tokens), 1)
    tri = jnp.where(col <= row, 1.0, 0.0).astype(BF16)

    def inside():
        return (col <= row) & (col // BLOCK == row // BLOCK)

    def hd(h):
        return slice(h * DK, (h + 1) * DK)

    def hv(h):
        return slice(h * DV, (h + 1) * DV)

    loads[0].wait()
    g_parts = pieces(g_ref[...], 3)
    span_buf[...] = sum(nn(tri, part_) for part_ in g_parts)
    total = span_buf[tokens - 1 : tokens, :]
    decay = jnp.exp(total)

    quarter = dvx // 4

    def part_rows(part):
        return slice(8 + part * quarter if part else 0, 8 + (part + 1) * quarter)

    def slot(to, frm):
        return (frm + nx - 1 - to) % nx

    def first_part(m, h, part):
        return pltpu.make_async_remote_copy(
            src_ref=a_out.at[1, m, h, part_rows(part), :], dst_ref=a_in.at[1, x, h, part_rows(part), :],
            send_sem=a_send.at[1, m], recv_sem=e_recv.at[slot(m, x), h * 4 + part],
            device_id={"sp": z * nx + m}, device_id_type=MESH)

    def first_wait(h, part):
        for m in range(nx):
            @pl.when(m != x)
            def _():
                pltpu.make_async_remote_copy(
                    src_ref=a_out.at[1, m, h, part_rows(part), :], dst_ref=a_in.at[1, m, h, part_rows(part), :],
                    send_sem=a_send.at[1, m], recv_sem=e_recv.at[slot(x, m), h * 4 + part],
                    device_id={"sp": z * nx + m}, device_id_type=MESH).wait_recv()

    def scatter_copy(d, m):
        return pltpu.make_async_remote_copy(
            src_ref=a_out.at[d, m], dst_ref=a_in.at[d, x],
            send_sem=a_send.at[d, m], recv_sem=a_recv.at[slot(m, x)],
            device_id={"sp": z * nx + m}, device_id_type=MESH)

    def scatter_wait(d):
        for m in range(nx):
            @pl.when(m != x)
            def _():
                pltpu.make_async_remote_copy(
                    src_ref=a_out.at[d, m], dst_ref=a_in.at[d, m],
                    send_sem=a_send.at[d, m], recv_sem=a_recv.at[slot(x, m)],
                    device_id={"sp": z * nx + m}, device_id_type=MESH).wait_recv()

    def give(d, h, totals):
        for m in range(nx):
            a_out[d, m, h, :8, :] = jnp.broadcast_to(decay[:, hd(h)], (8, DK))
            a_out[d, m, h, 8:, :] = totals[m * dvx : (m + 1) * dvx]
        for m in range(nx):
            @pl.when(m != x)
            def _():
                if d == 1:
                    for part in range(4):
                        first_part(m, h, part).start()
                elif h == heads - 1:
                    scatter_copy(d, m).start()

            @pl.when(m == x)
            def _():
                a_in[d, m, h] = a_out[d, m, h]

    loads[1].wait()
    q_all = q_ref[...].astype(F32) * scale
    q_span = (q_all * jnp.exp(span_buf[...])).astype(BF16)
    loads[2].wait()
    for h in range(heads):
        adjoint = tn(o_ref[:, hv(h)], q_span[:, hd(h)])
        if h == 0:
            pl.semaphore_wait(barrier, nx - 1 + nz - 1 + ntp - 1)
        give(1, h, adjoint)

    loads[4].wait()
    depth = x_ref.shape[1]
    for at in range(0, depth, 256):
        xt_buf[at : at + 256, :] = x_ref[:, at : at + 256].T

    own = dw_ref.shape[0]
    cols = dw_ref.shape[1]
    wide = min(cols, 128)
    chunks = cols // wide
    half_r = own // 2
    near, mirror = z + 1 - 2 * (z % 2), nz - 1 - z
    core_mate, row_mate = mine + 1 - 2 * (mine % 2), (mine + 2) % 4

    def block_rows(slab, xx, base=0, size=None):
        return pl.ds(pl.multiple_of((slab * nx + xx) * own + base, half_r), own if size is None else size)

    def x_copy(p):
        return pltpu.make_async_remote_copy(
            src_ref=xs_out.at[p], dst_ref=xr_in.at[mine, p],
            send_sem=xs_send.at[0], recv_sem=xr_recv.at[mine, p],
            device_id={"sp": near * nx + x}, device_id_type=MESH)

    def x_pass(which, block, p, mate):
        return pltpu.make_async_remote_copy(
            src_ref=xr_in.at[block, p], dst_ref=xr_in.at[block, p],
            send_sem=xs_send.at[which], recv_sem=xr_recv.at[block, p],
            device_id={"tp": mate}, device_id_type=MESH)

    def x_send(p):
        slab = jnp.where(mine < nx, nz - 1 - near, near)
        xs_out[p] = xt_buf[block_rows(slab, mine % nx, p * half_r, half_r), :].astype(F32)
        x_copy(p).start()

    def x_relay(p):
        x_copy(p).wait_recv()
        x_pass(2, mine, p, row_mate).start()
        x_pass(1, mine, p, core_mate).start()

    def x_forward():
        for p in range(2):
            x_pass(2, row_mate, p, row_mate).wait_recv()
            x_pass(3, row_mate, p, core_mate).start()

    def x_take():
        far_mate = (core_mate + 2) % 4
        for p in range(2):
            x_pass(1, core_mate, p, core_mate).wait_recv()
            x_pass(3, far_mate, p, core_mate).wait_recv()
        for j in range(2 * nx):
            for p in range(2):
                xr_buf[j, p * half_r : (p + 1) * half_r] = xr_in[j, p].astype(BF16)

    if cube:
        x_send(0)

        @pl.when(z < nz - 1)
        def _():
            x_send(1)

    loads[3].wait()
    loads[5].wait()
    k_all = k_ref[...].astype(F32)
    k_far = jnp.exp(total - span_buf[...])
    k_span = (k_all * k_far).astype(BF16)
    for h in range(heads):
        v_buf[:, hv(h)] = nn(x_ref[...], w_ref[:, hv(h)]).astype(BF16)
        give(0, h, tn(v_buf[:, hv(h)], k_span[:, hd(h)]))

    def order(d):
        return range(nx) if d == 0 else range(nx - 1, -1, -1)

    def plane_copy(dz):
        return pltpu.make_async_remote_copy(
            src_ref=z_out, dst_ref=z_in.at[z],
            send_sem=z_send.at[dz], recv_sem=z_recv.at[z],
            device_id={"sp": (z + dz) * nx + x}, device_id_type=MESH)

    def composite(d, h, rows_):
        acc, dec = None, None
        for m in order(d):
            local, rate = a_in[d, m, h, rows_, :], a_in[d, m, h, 0:1, :]
            acc = local if acc is None else local + rate * acc
            dec = rate if dec is None else rate * dec
        return acc, dec

    def forward_start():
        scatter_wait(0)
        for h in range(heads):
            acc, dec = composite(0, h, slice(8, 8 + dvx))
            z_out[h, :dvx, :] = acc
            z_out[h, dvx:, :] = jnp.broadcast_to(dec, (8, DK))
        for dz in range(1, nz):
            @pl.when(z + dz < nz)
            def _():
                plane_copy(dz).start()

    def local_side():
        tri_in = jnp.where(inside(), 1.0, 0.0).astype(BF16)
        last_in = jnp.where(col // BLOCK == row // BLOCK, 1.0, 0.0).astype(BF16)
        cum = sum(nn(tri_in, part_) for part_ in g_parts)
        c_buf[...] = cum
        block_end = sum(nn(last_in, part_) for part_ in g_parts)
        k_tail = jnp.exp(block_end - cum)
        tail_buf[...] = k_tail
        grow = jnp.exp(cum)
        qg_buf[...] = (q_all * grow).astype(BF16)
        ks_buf[...] = (k_all * jnp.exp(-cum)).astype(BF16)
        kt_buf[...] = (k_all * k_tail).astype(BF16)
        st_buf[...] = jnp.zeros_like(st_buf)

        def adjoint_step(step, carry):
            rows = pl.ds(pl.multiple_of((blocks - 1 - step) * BLOCK, BLOCK), BLOCK)
            for h in range(heads):
                keep = jnp.exp(c_buf[rows, hd(h)][BLOCK - 1 :])
                adjoint = st_buf[1, h]
                narrow = adjoint.astype(BF16)
                kp_buf[rows, hd(h)] = nn(v_buf[rows, hv(h)], narrow)
                vp_buf[rows, hv(h)] = nt(kt_buf[rows, hd(h)], narrow)
                st_buf[1, h] = keep * adjoint + tn(o_ref[rows, hv(h)], qg_buf[rows, hd(h)])
            return carry

        lax.fori_loop(0, blocks, adjoint_step, 0)

        for h in range(heads):
            dots = jnp.where(inside(), nt(qg_buf[:, hd(h)], ks_buf[:, hd(h)]), 0.0).astype(BF16)
            vp_buf[:, hv(h)] += tn(dots, o_ref[:, hv(h)])

    def state_step(step, carry):
        rows = pl.ds(pl.multiple_of(step * BLOCK, BLOCK), BLOCK)
        for h in range(heads):
            keep = jnp.exp(c_buf[rows, hd(h)][BLOCK - 1 :])
            state = st_buf[0, h]
            y_buf[rows, hd(h)] = nn(o_ref[rows, hv(h)], state.astype(BF16))
            st_buf[0, h] = keep * state + tn(v_buf[rows, hv(h)], kt_buf[rows, hd(h)])
        return carry

    def member_copy(m):
        return pltpu.make_async_remote_copy(
            src_ref=c_out.at[m], dst_ref=c_in.at[x],
            send_sem=c_send.at[m], recv_sem=c_recv.at[x],
            device_id={"sp": z * nx + m}, device_id_type=MESH)

    def forward_spread():
        z_acc[...] = jnp.zeros_like(z_acc)
        for zp in range(nz):
            @pl.when(zp < z)
            def _():
                pltpu.make_async_remote_copy(
                    src_ref=z_out, dst_ref=z_in.at[zp],
                    send_sem=z_send.at[0], recv_sem=z_recv.at[zp],
                    device_id={"sp": zp * nx + x}, device_id_type=MESH).wait_recv()
                for h in range(heads):
                    z_acc[h] = z_in[zp, h, :dvx, :] + z_in[zp, h, dvx : dvx + 1, :] * z_acc[h]
        for h in range(heads):
            acc = z_acc[h]
            for m in order(0):
                c_out[m, h] = acc
                acc = a_in[0, m, h, 8:, :] + a_in[0, m, h, 0:1, :] * acc
        for m in range(nx):
            @pl.when(m != x)
            def _():
                member_copy(m).start()

            @pl.when(m == x)
            def _():
                c_in[m] = c_out[m]

    def near_copy(c):
        return pltpu.make_async_remote_copy(
            src_ref=vx_out.at[c], dst_ref=vx_in.at[c],
            send_sem=v_send, recv_sem=v_recv.at[c],
            device_id={"sp": near * nx + x}, device_id_type=MESH)

    def side_copy(c, s, u):
        return pltpu.make_async_remote_copy(
            src_ref=sx_out.at[c, s, u], dst_ref=sx_in.at[c, s, u],
            send_sem=sx_send, recv_sem=sx_recv.at[c, s, u],
            device_id={"sp": z * nx + 1 - x}, device_id_type=MESH)

    def far_copy(c, u):
        return pltpu.make_async_remote_copy(
            src_ref=sm_out.at[c, u], dst_ref=sm_in.at[c, u],
            send_sem=sm_send, recv_sem=sm_recv.at[c, u],
            device_id={"sp": mirror * nx + x}, device_id_type=MESH)

    def emit(h, m):
        c = h * nx + m
        held = b_in[m, 4 * h : 4 * h + 4].reshape(dvx, DK).astype(BF16)
        at = pl.ds(pl.multiple_of(c * wide, wide), wide)
        value = (vp_buf[:, at] + nt(k_span[:, hd(h)], held)).astype(BF16)
        vg_buf[c] = value
        vx_out[c] = value.astype(F32)
        near_copy(c).start()

    def piece(c, s, xx):
        slab = mirror if s == 0 else z
        return nn(xt_buf[block_rows(slab, xx), :], vg_buf[c]) + nn(xr_buf[s * nx + xx], vgp_buf[c])

    def take_near(c):
        near_copy(c).wait_recv()
        vgp_buf[c] = vx_in[c].astype(BF16)

    def side_send(c, s):
        value = piece(c, s, 1 - x)
        for u in range(2):
            sx_out[c, s, u] = value[u * half_r : (u + 1) * half_r]
            side_copy(c, s, u).start()

    def keep(c, s):
        value = piece(c, s, x)
        for u in range(2):
            acc_buf[c, s, u] = value[u * half_r : (u + 1) * half_r]

    def far_send(c):
        for u in range(2):
            side_copy(c, 0, u).wait_recv()
            sm_out[c, u] = acc_buf[c, 0, u] + sx_in[c, 0, u]
            far_copy(c, u).start()

    @pl.when(z < nz - 1)
    def _():
        local_side()

    if cube:
        @pl.when(z < nz - 1)
        def _():
            x_relay(0)

    @pl.when(z < nz - 2)
    def _():
        forward_start()

    if cube:
        @pl.when(z < nz - 2)
        def _():
            x_relay(1)

        @pl.when(z == 0)
        def _():
            forward_spread()

    half_v = dvx // 4

    def chain_copy(c):
        return pltpu.make_async_remote_copy(
            src_ref=h_out.at[c], dst_ref=h_in.at[c],
            send_sem=h_send, recv_sem=h_recv.at[c],
            device_id={"sp": (z - 1) * nx + x}, device_id_type=MESH)

    def piece_copy(m, c):
        return pltpu.make_async_remote_copy(
            src_ref=b_out.at[m, c], dst_ref=b_in.at[x, c],
            send_sem=b_send.at[m], recv_sem=b_recv.at[slot(m, x), c],
            device_id={"sp": z * nx + m}, device_id_type=MESH)

    for c in range(4 * heads):
        h, rows_ = c // 4, slice(8 + c % 4 * half_v, 8 + (c % 4 + 1) * half_v)
        first_wait(h, c % 4)
        acc, dec = composite(1, h, rows_)

        @pl.when(z == nz - 1)
        def _():
            h_in[c] = jnp.zeros((half_v, DK), F32)

        @pl.when(z < nz - 1)
        def _():
            chain_copy(c).wait_recv()

        enter = h_in[c]

        @pl.when(z > 0)
        def _():
            h_out[c] = acc + dec * enter
            chain_copy(c).start()

        for m in order(1):
            b_out[m, c] = enter
            enter = a_in[1, m, h, rows_, :] + a_in[1, m, h, 0:1, :] * enter
        for m in range(nx):
            @pl.when(m != x)
            def _():
                piece_copy(m, c).start()

            @pl.when(m == x)
            def _():
                b_in[m, c] = b_out[m, c]

        if cube and c % 4 == 3:
            @pl.when(z < nz - 1)
            def _():
                emit(h, x)

    @pl.when(z == nz - 2)
    def _():
        forward_start()

    @pl.when(z == nz - 1)
    def _():
        if cube:
            x_send(1)
        local_side()
        if cube:
            for h in range(heads):
                emit(h, x)
        scatter_wait(0)

    def state_loop():
        lax.fori_loop(0, blocks, state_step, 0)

    if cube:
        @pl.when((z > 0) & (z < nz - 2))
        def _():
            forward_spread()

        state_loop()

        @pl.when(z < nz - 2)
        def _():
            x_forward()

        @pl.when(z == nz - 1)
        def _():
            x_relay(0)

        @pl.when(z >= nz - 2)
        def _():
            x_relay(1)

        for h in range(heads):
            for c in range(4 * h, 4 * (h + 1)):
                pltpu.make_async_remote_copy(
                    src_ref=b_out.at[1 - x, c], dst_ref=b_in.at[1 - x, c],
                    send_sem=b_send.at[1 - x], recv_sem=b_recv.at[0, c],
                    device_id={"sp": z * nx + 1 - x}, device_id_type=MESH).wait_recv()
            emit(h, 1 - x)
            for m in range(nx):
                fr_buf[h, m * dvx : (m + 1) * dvx, :] = b_in[m, 4 * h : 4 * h + 4].reshape(dvx, DK)
    else:
        for h in range(heads):
            for m in range(nx):
                for c in range(4 * h, 4 * (h + 1)):
                    @pl.when(m != x)
                    def _():
                        pltpu.make_async_remote_copy(
                            src_ref=b_out.at[m, c], dst_ref=b_in.at[m, c],
                            send_sem=b_send.at[m], recv_sem=b_recv.at[slot(x, m), c],
                            device_id={"sp": z * nx + m}, device_id_type=MESH).wait_recv()
                    at = m * dvx + c % 4 * half_v
                    fr_buf[h, at : at + half_v, :] = b_in[m, c]
            narrow = fr_buf[h].astype(BF16)
            vg_buf[:, hv(h)] = (vp_buf[:, hv(h)] + nt(k_span[:, hd(h)], narrow)).astype(BF16)


    half_c = cols // 2
    p = ring_place(z, x, nz, nx)
    ahead = ring_member((p + 1) % n, nz, nx)
    behind = ring_member((p + n - 1) % n, nz, nx)

    def share(d, u, owner):
        rows_ = pl.ds(pl.multiple_of(owner * own + u * half_r, half_r), half_r)
        return nn(xt_buf[rows_, :], vg_buf[:, d * half_c : (d + 1) * half_c])

    def ring_copy(step, d, u, src):
        return pltpu.make_async_remote_copy(
            src_ref=src, dst_ref=ring.at[step, d, u],
            send_sem=r_send.at[step, d, u], recv_sem=r_recv.at[step, d, u],
            device_id={"sp": ahead if d == 0 else behind}, device_id_type=MESH)

    def owner_at(step, d):
        return ring_member((p + n - step - 1) % n if d == 0 else (p + step + 1) % n, nz, nx)

    if not cube:
        for u in range(2):
            for d in range(2):
                first[d, u] = share(d, u, owner_at(0, d))
                ring_copy(0, d, u, first.at[d, u]).start()

    def key_side():
        for h in range(heads):
            dots = jnp.where(inside(), nt(o_ref[:, hv(h)], v_buf[:, hv(h)]), 0.0).astype(BF16)
            y_buf[:, hd(h)] += nn(dots, ks_buf[:, hd(h)])
            k_grad = (
                tail_buf[:, hd(h)] * kp_buf[:, hd(h)]
                + jnp.exp(-c_buf[:, hd(h)]) * tn(dots, qg_buf[:, hd(h)])
                + k_far[:, hd(h)] * nn(v_buf[:, hv(h)], fr_buf[h].astype(BF16))
            )
            kp_buf[:, hd(h)] = k_grad
            dk_ref[:, hd(h)] = k_grad.astype(BF16)

    if not cube:
        state_loop()
        key_side()

    def query_side(first_head=0, last_head=heads):
        for m in range(nx):
            if first_head:
                break

            @pl.when(m != x)
            def _():
                pltpu.make_async_remote_copy(
                    src_ref=c_out.at[m], dst_ref=c_in.at[m],
                    send_sem=c_send.at[m], recv_sem=c_recv.at[m],
                    device_id={"sp": z * nx + m}, device_id_type=MESH).wait_recv()
        upper = jnp.where(col >= row, 1.0, 0.0).astype(BF16)
        for h in range(first_head, last_head):
            state_in = jnp.concatenate([c_in[m, h] for m in range(nx)], axis=0)
            q_side = q_ref[:, hd(h)].astype(F32) * scale
            k_side = k_ref[:, hd(h)].astype(F32)
            q_grad = jnp.exp(c_buf[:, hd(h)]) * y_buf[:, hd(h)] + jnp.exp(span_buf[:, hd(h)]) * nn(
                o_ref[:, hv(h)], state_in.astype(BF16)
            )
            dq_ref[:, hd(h)] = (q_grad * scale).astype(BF16)
            terms = q_side * q_grad - k_side * kp_buf[:, hd(h)]
            far = jnp.exp(span_buf[tokens - 1 : tokens, hd(h)])
            span_end = st_buf[0, h] + far * state_in
            carry = jnp.sum(fr_buf[h] * span_end, axis=0, keepdims=True)
            dg_ref[:, hd(h)] = sum(nn(upper, part_) for part_ in pieces(terms, 3)) + carry

    def ring_step(step, carry):
        for d in range(2):
            for u in range(2):
                part[d, u] = share(d, u, owner_at(step, d))
        for u in range(2):
            for d in range(2):
                ring_copy(step - 1, d, u, first.at[d, u]).wait_recv()
                ring[step - 1, d, u] += part[d, u]
                ring_copy(step, d, u, ring.at[step - 1, d, u]).start()

        @pl.when(step == 2)
        def _():
            forward_spread()

        @pl.when(step == 4)
        def _():
            query_side()

        return carry

    if not cube:
        lax.fori_loop(1, n - 1, ring_step, 0)

        for d in range(2):
            for u in range(2):
                part[d, u] = share(d, u, me)
        for u in range(2):
            squares = 0.0
            for d in range(2):
                ring_copy(n - 2, d, u, first.at[d, u]).wait_recv()
                done = ring[n - 2, d, u] + part[d, u]
                dw_ref[u * half_r : (u + 1) * half_r, d * half_c : (d + 1) * half_c] = done
                for at in range(0, half_c, 128):
                    squares = squares + done[:, at : at + 128] * done[:, at : at + 128]
            norm_out[u] = jnp.broadcast_to(jnp.sum(squares.T, axis=0, keepdims=True), (8, half_r))
    else:
        @pl.when(z >= nz - 2)
        def _():
            x_forward()

        k0, k1, k2, k3 = x, nx + x, 1 - x, nx + 1 - x
        x_take()
        take_near(k0)
        side_send(k0, 0)
        take_near(k1)
        side_send(k1, 0)
        side_send(k0, 1)
        key_side()
        take_near(k2)
        side_send(k2, 0)
        keep(k2, 0)
        far_send(k2)
        side_send(k1, 1)
        take_near(k3)
        side_send(k3, 0)
        keep(k3, 0)
        far_send(k3)
        side_send(k2, 1)
        keep(k0, 0)
        keep(k1, 0)

        @pl.when(z >= nz - 2)
        def _():
            forward_spread()

        far_send(k0)
        side_send(k3, 1)
        keep(k2, 1)
        keep(k3, 1)
        query_side(0, 1)
        far_send(k1)
        keep(k0, 1)
        keep(k1, 1)
        query_side(1, heads)
        squares = [0.0, 0.0]
        for c in (k2, k3, k0, k1):
            at = pl.ds(pl.multiple_of(c * wide, wide), wide)
            for u in range(2):
                side_copy(c, 1, u).wait_recv()
                far_copy(c, u).wait_recv()
                done = acc_buf[c, 1, u] + sx_in[c, 1, u] + sm_in[c, u]
                dw_ref[u * half_r : (u + 1) * half_r, at] = done
                squares[u] = squares[u] + done * done
        for u in range(2):
            norm_out[u] = jnp.broadcast_to(jnp.sum(squares[u].T, axis=0, keepdims=True), (8, half_r))

    def norm_copy(off):
        return pltpu.make_async_remote_copy(
            src_ref=norm_out, dst_ref=norm_in.at[off],
            send_sem=n_send.at[off], recv_sem=n_recv.at[off],
            device_id={"tp": (mine + off) % ntp}, device_id_type=MESH)

    for off in range(1, ntp):
        norm_copy(off).start()

    for m in range(nx):
        @pl.when(m != x)
        def _():
            for d in range(2):
                pltpu.make_async_remote_copy(
                    src_ref=a_out.at[d, m], dst_ref=a_in.at[d, x],
                    send_sem=a_send.at[d, m], recv_sem=a_recv.at[slot(m, x)],
                    device_id={"sp": z * nx + m}, device_id_type=MESH).wait_send()
            pltpu.make_async_remote_copy(
                src_ref=b_out.at[m], dst_ref=b_in.at[x],
                send_sem=b_send.at[m], recv_sem=b_recv.at[slot(m, x), 0],
                device_id={"sp": z * nx + m}, device_id_type=MESH).wait_send()
            member_copy(m).wait_send()
    for dz in range(1, nz):
        @pl.when(z + dz < nz)
        def _():
            plane_copy(dz).wait_send()

    @pl.when(z > 0)
    def _():
        pltpu.make_async_remote_copy(
            src_ref=h_out, dst_ref=h_in,
            send_sem=h_send, recv_sem=h_recv.at[0],
            device_id={"sp": (z - 1) * nx + x}, device_id_type=MESH).wait_send()

    if not cube:
        def sent(step, carry):
            for u in range(2):
                for d in range(2):
                    ring_copy(step, d, u, first.at[d, u]).wait_send()
            return carry

        lax.fori_loop(0, n - 1, sent, 0)
    else:
        def all_sent(ref, sem):
            pltpu.make_async_remote_copy(
                src_ref=ref, dst_ref=ref, send_sem=sem, recv_sem=v_recv.at[0],
                device_id={"sp": near * nx + x}, device_id_type=MESH).wait_send()

        all_sent(xs_out, xs_send.at[0])
        all_sent(xr_in.at[mine], xs_send.at[1])
        all_sent(xr_in.at[mine], xs_send.at[2])
        all_sent(xr_in.at[row_mate], xs_send.at[3])
        all_sent(vx_out, v_send)
        all_sent(sx_out, sx_send)
        all_sent(sm_out, sm_send)

    norms = norm_out[...]
    for off in range(1, ntp):
        norm_copy(off).wait()
        norms = norms + norm_in[off]
    rn_ref[...] = norms


def finish(*refs):
    sems = refs[10]
    writes = [pltpu.make_async_copy(refs[i], refs[5 + i], sems.at[i]) for i in range(4)]
    for write in writes:
        write.start()
    refs[9][...] = refs[4][:, :1]
    for write in writes:
        write.wait()


def on_device(n, nx, ntp, block_input, queries, keys, w_value, log_decay, d_out):
    tokens, wide = queries.shape
    heads = wide // DK
    cols = w_value.shape[1]
    depth = block_input.shape[1]
    own = depth // n
    nz = n // nx
    dvx = DV // nx
    vm = pltpu.VMEM
    dma = pltpu.SemaphoreType.DMA
    wide_c = min(cols, 128)
    chunks, half = cols // wide_c, own // 2
    late = [
        vm((2, 2, half, cols // 2), F32),
        vm((2, 2, half, cols // 2), F32),
        vm((n - 1, 2, 2, half, cols // 2), F32),
        dma((n - 1, 2, 2)),
        dma((n - 1, 2, 2)),
    ]
    cube = is_cube(n, nx, ntp) and cols == 2 * DV
    if cube:
        late = [
            vm((2, half, tokens), F32),
            vm((ntp, 2, half, tokens), F32),
            vm((ntp, own, tokens), BF16),
            vm((chunks, tokens, wide_c), F32),
            vm((chunks, tokens, wide_c), F32),
            vm((chunks, tokens, wide_c), BF16),
            vm((chunks, 2, 2, half, wide_c), F32),
            vm((chunks, 2, 2, half, wide_c), F32),
            vm((chunks, 2, 2, half, wide_c), F32),
            vm((chunks, 2, half, wide_c), F32),
            vm((chunks, 2, half, wide_c), F32),
            dma((4,)),
            dma((ntp, 2)),
            dma,
            dma((chunks,)),
            dma,
            dma((chunks, 2, 2)),
            dma,
            dma((chunks, 2)),
        ]
    out = pl.pallas_call(
        functools.partial(kernel, n, nx, ntp),
        out_shape=(
            vm((tokens, wide), BF16),
            vm((tokens, wide), BF16),
            vm((tokens, wide), F32),
            vm((own, cols), F32),
            vm((2, 8, own // 2), F32),
        ),
        in_specs=[pl.BlockSpec(memory_space=pltpu.HBM)] * 6,
        out_specs=(pl.BlockSpec(memory_space=vm),) * 5,
        scratch_shapes=[
            vm(block_input.shape, BF16),
            vm(queries.shape, BF16),
            vm(keys.shape, BF16),
            vm(w_value.shape, BF16),
            vm(log_decay.shape, F32),
            vm(d_out.shape, BF16),
            dma((6,)),
            vm((tokens, wide), F32),
            vm((tokens, wide), F32),
            vm((tokens, cols), BF16),
            vm((tokens, wide), BF16),
            vm((tokens, wide), BF16),
            vm((tokens, wide), BF16),
            vm((tokens, wide), F32),
            vm((tokens, wide), F32),
            vm((tokens, cols), F32),
            vm((2, heads, DV, DK), F32),
            vm((depth, tokens), BF16),
            vm((chunks, tokens, wide_c) if cube else (tokens, cols), BF16),
            vm((2, nx, heads, dvx + 8, DK), F32),
            vm((2, nx, heads, dvx + 8, DK), F32),
            vm((heads, dvx + 8, DK), F32),
            vm((nz, heads, dvx + 8, DK), F32),
            vm((heads, dvx, DK), F32),
            vm((nx, heads, dvx, DK), F32),
            vm((nx, heads, dvx, DK), F32),
            vm((4 * heads, dvx // 4, DK), F32),
            vm((4 * heads, dvx // 4, DK), F32),
            vm((nx, 4 * heads, dvx // 4, DK), F32),
            vm((nx, 4 * heads, dvx // 4, DK), F32),
            vm((heads, DV, DK), F32),
            vm((2, 8, own // 2), F32),
            vm((ntp, 2, 8, own // 2), F32),
            dma((2, nx)),
            dma((nx - 1,)),
            dma((nx - 1, 4 * heads)),
            dma((nz,)),
            dma((nz,)),
            dma((nx,)),
            dma((nx,)),
            dma,
            dma((4 * heads,)),
            dma((nx,)),
            dma((nx - 1, 4 * heads)),
            dma((ntp,)),
            dma((ntp,)),
            vm((tokens, wide), F32),
            *late,
        ],
        compiler_params=pltpu.CompilerParams(
            collective_id=0, has_side_effects=True, vmem_limit_bytes=62 * 1024 * 1024
        ),
    )(block_input, queries, keys, w_value, log_decay, d_out)
    final = pl.pallas_call(
        finish,
        out_shape=tuple(jax.ShapeDtypeStruct(a.shape, a.dtype) for a in out[:4])
        + (jax.ShapeDtypeStruct((2, 1, own // 2), F32),),
        in_specs=[pl.BlockSpec(memory_space=vm)] * 5,
        out_specs=(pl.BlockSpec(memory_space=pltpu.HBM),) * 4 + (pl.BlockSpec(memory_space=vm),),
        scratch_shapes=[dma((4,))],
        compiler_params=pltpu.CompilerParams(vmem_limit_bytes=1024 * 1024),
    )(*out)
    return (*final[:4], final[4].reshape(-1))


def solution(mesh):
    n, ntp = mesh.shape["sp"], mesh.shape["tp"]
    nx = 1 << ((n.bit_length() - 1) // 2)
    placed = (
        P("sp", None),
        P("sp", "tp"),
        P("sp", "tp"),
        P(None, "tp"),
        P("sp", "tp"),
        P("sp", "tp"),
    )
    return jax.shard_map(
        functools.partial(on_device, n, nx, ntp),
        mesh=mesh,
        in_specs=placed,
        out_specs=(P("sp", "tp"), P("sp", "tp"), P("sp", "tp"), P("sp", "tp"), P("sp")),
        check_vma=False,
    )
```

```python
import functools

import jax
import jax.numpy as jnp
from jax import lax
from jax.experimental import pallas as pl
from jax.experimental.pallas import tpu as pltpu
from jax.sharding import PartitionSpec as P

DK = 128
DV = 256
BLOCK = 32
F32 = jnp.float32
BF16 = jnp.bfloat16
MESH = pl.DeviceIdType.MESH


def nn(left, right):
    return lax.dot_general(left, right, (((1,), (0,)), ((), ())), preferred_element_type=F32)


def nt(left, right):
    return lax.dot_general(left, right, (((1,), (1,)), ((), ())), preferred_element_type=F32)


def tn(left, right):
    return lax.dot_general(left, right, (((0,), (0,)), ((), ())), preferred_element_type=F32)


def pieces(value, count):
    parts = []
    for _ in range(count):
        part = value.astype(BF16)
        parts.append(part)
        value = value - part.astype(F32)
    return parts


def ring_place(z, x, nz, nx):
    r = nz - 1 - z
    across = jnp.where(r % 2 == 0, x - 1, nx - 1 - x)
    return jnp.where(x == 0, z, nz + r * (nx - 1) + across)


def ring_member(p, nz, nx):
    u = jnp.maximum(p - nz, 0)
    r = u // (nx - 1)
    w = u % (nx - 1)
    x = jnp.where(r % 2 == 0, 1 + w, nx - 1 - w)
    return jnp.where(p < nz, p * nx, (nz - 1 - r) * nx + x)


def is_cube(n, nx, ntp):
    return nx == 2 and n == 4 * nx and ntp == 2 * nx


def kernel(
    n, nx, ntp,
    x_hbm, q_hbm, k_hbm, w_hbm, g_hbm, o_hbm,
    dq_ref, dk_ref, dg_ref, dw_ref, rn_ref,
    x_ref, q_ref, k_ref, w_ref, g_ref, o_ref, in_sem,
    c_buf, span_buf, v_buf, qg_buf, kt_buf, ks_buf, y_buf, kp_buf, vp_buf, st_buf, xt_buf, vg_buf,
    a_out, a_in, z_out, z_in, z_acc, c_out, c_in, h_out, h_in, b_out, b_in, fr_buf,
    norm_out, norm_in,
    a_send, a_recv, e_recv, z_send, z_recv, c_send, c_recv, h_send, h_recv, b_send, b_recv, n_send, n_recv,
    tail_buf, *late,
):
    cube = is_cube(n, nx, ntp) and dw_ref.shape[1] == 2 * DV
    if cube:
        (xs_out, xr_in, xr_buf, vx_out, vx_in, vgp_buf, sx_out, sx_in, acc_buf, sm_out, sm_in,
         xs_send, xr_recv, v_send, v_recv, sx_send, sx_recv, sm_send, sm_recv) = late
    else:
        first, part, ring, r_send, r_recv = late
    nz = n // nx
    me = lax.axis_index("sp")
    mine = lax.axis_index("tp")
    z, x = me // nx, me % nx
    tokens, heads = q_ref.shape[0], q_ref.shape[1] // DK
    blocks = tokens // BLOCK
    dvx = DV // nx
    scale = DK ** (-0.5)
    loads = [
        pltpu.make_async_copy(source, target, in_sem.at[i])
        for i, (source, target) in enumerate(
            [(g_hbm, g_ref), (q_hbm, q_ref), (o_hbm, o_ref), (k_hbm, k_ref), (x_hbm, x_ref), (w_hbm, w_ref)]
        )
    ]
    for load in loads:
        load.start()
    barrier = pltpu.get_barrier_semaphore()
    for off in range(1, nx):
        pl.semaphore_signal(
            barrier, inc=1, device_id={"sp": z * nx + (x + off) % nx}, device_id_type=MESH)
    for off in range(1, nz):
        pl.semaphore_signal(
            barrier, inc=1, device_id={"sp": (z + off) % nz * nx + x}, device_id_type=MESH)
    for off in range(1, ntp):
        pl.semaphore_signal(barrier, inc=1, device_id={"tp": (mine + off) % ntp}, device_id_type=MESH)

    row = lax.broadcasted_iota(jnp.int32, (tokens, tokens), 0)
    col = lax.broadcasted_iota(jnp.int32, (tokens, tokens), 1)
    tri = jnp.where(col <= row, 1.0, 0.0).astype(BF16)

    def inside():
        return (col <= row) & (col // BLOCK == row // BLOCK)

    def hd(h):
        return slice(h * DK, (h + 1) * DK)

    def hv(h):
        return slice(h * DV, (h + 1) * DV)

    loads[0].wait()
    g_parts = pieces(g_ref[...], 3)
    span_buf[...] = sum(nn(tri, part_) for part_ in g_parts)
    total = span_buf[tokens - 1 : tokens, :]
    decay = jnp.exp(total)

    quarter = dvx // 4

    def part_rows(part):
        return slice(8 + part * quarter if part else 0, 8 + (part + 1) * quarter)

    def slot(to, frm):
        return (frm + nx - 1 - to) % nx

    def first_part(m, h, part):
        return pltpu.make_async_remote_copy(
            src_ref=a_out.at[1, m, h, part_rows(part), :], dst_ref=a_in.at[1, x, h, part_rows(part), :],
            send_sem=a_send.at[1, m], recv_sem=e_recv.at[slot(m, x), h * 4 + part],
            device_id={"sp": z * nx + m}, device_id_type=MESH)

    def first_wait(h, part):
        for m in range(nx):
            @pl.when(m != x)
            def _():
                pltpu.make_async_remote_copy(
                    src_ref=a_out.at[1, m, h, part_rows(part), :], dst_ref=a_in.at[1, m, h, part_rows(part), :],
                    send_sem=a_send.at[1, m], recv_sem=e_recv.at[slot(x, m), h * 4 + part],
                    device_id={"sp": z * nx + m}, device_id_type=MESH).wait_recv()

    def scatter_copy(d, m):
        return pltpu.make_async_remote_copy(
            src_ref=a_out.at[d, m], dst_ref=a_in.at[d, x],
            send_sem=a_send.at[d, m], recv_sem=a_recv.at[slot(m, x)],
            device_id={"sp": z * nx + m}, device_id_type=MESH)

    def scatter_wait(d):
        for m in range(nx):
            @pl.when(m != x)
            def _():
                pltpu.make_async_remote_copy(
                    src_ref=a_out.at[d, m], dst_ref=a_in.at[d, m],
                    send_sem=a_send.at[d, m], recv_sem=a_recv.at[slot(x, m)],
                    device_id={"sp": z * nx + m}, device_id_type=MESH).wait_recv()

    def give(d, h, totals):
        for m in range(nx):
            a_out[d, m, h, :8, :] = jnp.broadcast_to(decay[:, hd(h)], (8, DK))
            a_out[d, m, h, 8:, :] = totals[m * dvx : (m + 1) * dvx]
        for m in range(nx):
            @pl.when(m != x)
            def _():
                if d == 1:
                    for part in range(4):
                        first_part(m, h, part).start()
                elif h == heads - 1:
                    scatter_copy(d, m).start()

            @pl.when(m == x)
            def _():
                a_in[d, m, h] = a_out[d, m, h]

    loads[1].wait()
    q_all = q_ref[...].astype(F32) * scale
    q_span = (q_all * jnp.exp(span_buf[...])).astype(BF16)
    loads[2].wait()
    for h in range(heads):
        adjoint = tn(o_ref[:, hv(h)], q_span[:, hd(h)])
        if h == 0:
            pl.semaphore_wait(barrier, nx - 1 + nz - 1 + ntp - 1)
        give(1, h, adjoint)

    loads[4].wait()
    depth = x_ref.shape[1]
    for at in range(0, depth, 256):
        xt_buf[at : at + 256, :] = x_ref[:, at : at + 256].T

    own = dw_ref.shape[0]
    cols = dw_ref.shape[1]
    wide = min(cols, 128)
    chunks = cols // wide
    half_r = own // 2
    near, mirror = z + 1 - 2 * (z % 2), nz - 1 - z
    core_mate, row_mate = mine + 1 - 2 * (mine % 2), (mine + 2) % 4

    def block_rows(slab, xx, base=0, size=None):
        return pl.ds(pl.multiple_of((slab * nx + xx) * own + base, half_r), own if size is None else size)

    def x_copy(p):
        return pltpu.make_async_remote_copy(
            src_ref=xs_out.at[p], dst_ref=xr_in.at[mine, p],
            send_sem=xs_send.at[0], recv_sem=xr_recv.at[mine, p],
            device_id={"sp": near * nx + x}, device_id_type=MESH)

    def x_pass(which, block, p, mate):
        return pltpu.make_async_remote_copy(
            src_ref=xr_in.at[block, p], dst_ref=xr_in.at[block, p],
            send_sem=xs_send.at[which], recv_sem=xr_recv.at[block, p],
            device_id={"tp": mate}, device_id_type=MESH)

    def x_send(p):
        slab = jnp.where(mine < nx, nz - 1 - near, near)
        xs_out[p] = xt_buf[block_rows(slab, mine % nx, p * half_r, half_r), :].astype(F32)
        x_copy(p).start()

    def x_relay(p):
        x_copy(p).wait_recv()
        x_pass(2, mine, p, row_mate).start()
        x_pass(1, mine, p, core_mate).start()

    def x_forward():
        for p in range(2):
            x_pass(2, row_mate, p, row_mate).wait_recv()
            x_pass(3, row_mate, p, core_mate).start()

    def x_take():
        far_mate = (core_mate + 2) % 4
        for p in range(2):
            x_pass(1, core_mate, p, core_mate).wait_recv()
            x_pass(3, far_mate, p, core_mate).wait_recv()
        for j in range(2 * nx):
            for p in range(2):
                xr_buf[j, p * half_r : (p + 1) * half_r] = xr_in[j, p].astype(BF16)

    if cube:
        x_send(0)

        @pl.when(z < nz - 1)
        def _():
            x_send(1)

    loads[3].wait()
    loads[5].wait()
    k_all = k_ref[...].astype(F32)
    k_far = jnp.exp(total - span_buf[...])
    k_span = (k_all * k_far).astype(BF16)
    for h in range(heads):
        v_buf[:, hv(h)] = nn(x_ref[...], w_ref[:, hv(h)]).astype(BF16)
        give(0, h, tn(v_buf[:, hv(h)], k_span[:, hd(h)]))

    def order(d):
        return range(nx) if d == 0 else range(nx - 1, -1, -1)

    def plane_copy(dz):
        return pltpu.make_async_remote_copy(
            src_ref=z_out, dst_ref=z_in.at[z],
            send_sem=z_send.at[dz], recv_sem=z_recv.at[z],
            device_id={"sp": (z + dz) * nx + x}, device_id_type=MESH)

    def composite(d, h, rows_):
        acc, dec = None, None
        for m in order(d):
            local, rate = a_in[d, m, h, rows_, :], a_in[d, m, h, 0:1, :]
            acc = local if acc is None else local + rate * acc
            dec = rate if dec is None else rate * dec
        return acc, dec

    def forward_start():
        scatter_wait(0)
        for h in range(heads):
            acc, dec = composite(0, h, slice(8, 8 + dvx))
            z_out[h, :dvx, :] = acc
            z_out[h, dvx:, :] = jnp.broadcast_to(dec, (8, DK))
        for dz in range(1, nz):
            @pl.when(z + dz < nz)
            def _():
                plane_copy(dz).start()

    def local_side():
        tri_in = jnp.where(inside(), 1.0, 0.0).astype(BF16)
        last_in = jnp.where(col // BLOCK == row // BLOCK, 1.0, 0.0).astype(BF16)
        cum = sum(nn(tri_in, part_) for part_ in g_parts)
        c_buf[...] = cum
        block_end = sum(nn(last_in, part_) for part_ in g_parts)
        k_tail = jnp.exp(block_end - cum)
        tail_buf[...] = k_tail
        grow = jnp.exp(cum)
        qg_buf[...] = (q_all * grow).astype(BF16)
        ks_buf[...] = (k_all * jnp.exp(-cum)).astype(BF16)
        kt_buf[...] = (k_all * k_tail).astype(BF16)
        st_buf[...] = jnp.zeros_like(st_buf)

        def adjoint_step(step, carry):
            rows = pl.ds(pl.multiple_of((blocks - 1 - step) * BLOCK, BLOCK), BLOCK)
            for h in range(heads):
                keep = jnp.exp(c_buf[rows, hd(h)][BLOCK - 1 :])
                adjoint = st_buf[1, h]
                narrow = adjoint.astype(BF16)
                kp_buf[rows, hd(h)] = nn(v_buf[rows, hv(h)], narrow)
                vp_buf[rows, hv(h)] = nt(kt_buf[rows, hd(h)], narrow)
                st_buf[1, h] = keep * adjoint + tn(o_ref[rows, hv(h)], qg_buf[rows, hd(h)])
            return carry

        lax.fori_loop(0, blocks, adjoint_step, 0)

        for h in range(heads):
            dots = jnp.where(inside(), nt(qg_buf[:, hd(h)], ks_buf[:, hd(h)]), 0.0).astype(BF16)
            vp_buf[:, hv(h)] += tn(dots, o_ref[:, hv(h)])

    def state_step(step, carry):
        rows = pl.ds(pl.multiple_of(step * BLOCK, BLOCK), BLOCK)
        for h in range(heads):
            keep = jnp.exp(c_buf[rows, hd(h)][BLOCK - 1 :])
            state = st_buf[0, h]
            y_buf[rows, hd(h)] = nn(o_ref[rows, hv(h)], state.astype(BF16))
            st_buf[0, h] = keep * state + tn(v_buf[rows, hv(h)], kt_buf[rows, hd(h)])
        return carry

    def member_copy(m):
        return pltpu.make_async_remote_copy(
            src_ref=c_out.at[m], dst_ref=c_in.at[x],
            send_sem=c_send.at[m], recv_sem=c_recv.at[x],
            device_id={"sp": z * nx + m}, device_id_type=MESH)

    def forward_spread():
        z_acc[...] = jnp.zeros_like(z_acc)
        for zp in range(nz):
            @pl.when(zp < z)
            def _():
                pltpu.make_async_remote_copy(
                    src_ref=z_out, dst_ref=z_in.at[zp],
                    send_sem=z_send.at[0], recv_sem=z_recv.at[zp],
                    device_id={"sp": zp * nx + x}, device_id_type=MESH).wait_recv()
                for h in range(heads):
                    z_acc[h] = z_in[zp, h, :dvx, :] + z_in[zp, h, dvx : dvx + 1, :] * z_acc[h]
        for h in range(heads):
            acc = z_acc[h]
            for m in order(0):
                c_out[m, h] = acc
                acc = a_in[0, m, h, 8:, :] + a_in[0, m, h, 0:1, :] * acc
        for m in range(nx):
            @pl.when(m != x)
            def _():
                member_copy(m).start()

            @pl.when(m == x)
            def _():
                c_in[m] = c_out[m]

    def step_copy():
        return pltpu.make_async_remote_copy(
            src_ref=z_out, dst_ref=z_in.at[0],
            send_sem=z_send.at[0], recv_sem=z_recv.at[0],
            device_id={"sp": (z + 1) * nx + x}, device_id_type=MESH)

    def forward_step():
        @pl.when(z == 0)
        def _():
            z_acc[...] = jnp.zeros_like(z_acc)

        @pl.when(z > 0)
        def _():
            step_copy().wait_recv()
            for h in range(heads):
                z_acc[h] = z_in[0, h, :dvx, :]

        for h in range(heads):
            acc = z_acc[h]
            for m in order(0):
                c_out[m, h] = acc
                acc = a_in[0, m, h, 8:, :] + a_in[0, m, h, 0:1, :] * acc
            z_out[h, :dvx, :] = acc
            z_out[h, dvx:, :] = jnp.zeros((8, DK), F32)

        @pl.when(z < nz - 1)
        def _():
            step_copy().start()

        for m in range(nx):
            @pl.when(m != x)
            def _():
                member_copy(m).start()

            @pl.when(m == x)
            def _():
                c_in[m] = c_out[m]

    def near_copy(c):
        return pltpu.make_async_remote_copy(
            src_ref=vx_out.at[c], dst_ref=vx_in.at[c],
            send_sem=v_send, recv_sem=v_recv.at[c],
            device_id={"sp": near * nx + x}, device_id_type=MESH)

    def side_copy(c, s, u):
        return pltpu.make_async_remote_copy(
            src_ref=sx_out.at[c, s, u], dst_ref=sx_in.at[c, s, u],
            send_sem=sx_send, recv_sem=sx_recv.at[c, s, u],
            device_id={"sp": z * nx + 1 - x}, device_id_type=MESH)

    def far_copy(c, u):
        return pltpu.make_async_remote_copy(
            src_ref=sm_out.at[c, u], dst_ref=sm_in.at[c, u],
            send_sem=sm_send, recv_sem=sm_recv.at[c, u],
            device_id={"sp": mirror * nx + x}, device_id_type=MESH)

    def emit(h, m):
        c = h * nx + m
        held = b_in[m, 4 * h : 4 * h + 4].reshape(dvx, DK).astype(BF16)
        at = pl.ds(pl.multiple_of(c * wide, wide), wide)
        value = (vp_buf[:, at] + nt(k_span[:, hd(h)], held)).astype(BF16)
        vg_buf[c] = value
        vx_out[c] = value.astype(F32)
        near_copy(c).start()

    def piece(c, s, xx):
        slab = mirror if s == 0 else z
        return nn(xt_buf[block_rows(slab, xx), :], vg_buf[c]) + nn(xr_buf[s * nx + xx], vgp_buf[c])

    def take_near(c):
        near_copy(c).wait_recv()
        vgp_buf[c] = vx_in[c].astype(BF16)

    def side_send(c, s):
        value = piece(c, s, 1 - x)
        for u in range(2):
            sx_out[c, s, u] = value[u * half_r : (u + 1) * half_r]
            side_copy(c, s, u).start()

    def keep(c, s):
        value = piece(c, s, x)
        for u in range(2):
            acc_buf[c, s, u] = value[u * half_r : (u + 1) * half_r]

    def far_send(c):
        for u in range(2):
            side_copy(c, 0, u).wait_recv()
            sm_out[c, u] = acc_buf[c, 0, u] + sx_in[c, 0, u]
            far_copy(c, u).start()

    @pl.when(z < nz - 1)
    def _():
        local_side()

    if cube:
        @pl.when(z < nz - 1)
        def _():
            x_relay(0)

    if not cube:
        @pl.when(z < nz - 2)
        def _():
            forward_start()

    if cube:
        @pl.when(z < nz - 2)
        def _():
            x_relay(1)

        @pl.when(z == 0)
        def _():
            scatter_wait(0)
            forward_step()

    half_v = dvx // 4

    def chain_copy(c):
        return pltpu.make_async_remote_copy(
            src_ref=h_out.at[c], dst_ref=h_in.at[c],
            send_sem=h_send, recv_sem=h_recv.at[c],
            device_id={"sp": (z - 1) * nx + x}, device_id_type=MESH)

    def piece_copy(m, c):
        return pltpu.make_async_remote_copy(
            src_ref=b_out.at[m, c], dst_ref=b_in.at[x, c],
            send_sem=b_send.at[m], recv_sem=b_recv.at[slot(m, x), c],
            device_id={"sp": z * nx + m}, device_id_type=MESH)

    for c in range(4 * heads):
        h, rows_ = c // 4, slice(8 + c % 4 * half_v, 8 + (c % 4 + 1) * half_v)
        first_wait(h, c % 4)
        acc, dec = composite(1, h, rows_)

        @pl.when(z == nz - 1)
        def _():
            h_in[c] = jnp.zeros((half_v, DK), F32)

        @pl.when(z < nz - 1)
        def _():
            chain_copy(c).wait_recv()

        enter = h_in[c]

        @pl.when(z > 0)
        def _():
            h_out[c] = acc + dec * enter
            chain_copy(c).start()

        for m in order(1):
            b_out[m, c] = enter
            enter = a_in[1, m, h, rows_, :] + a_in[1, m, h, 0:1, :] * enter
        for m in range(nx):
            @pl.when(m != x)
            def _():
                piece_copy(m, c).start()

            @pl.when(m == x)
            def _():
                b_in[m, c] = b_out[m, c]

        if cube and c % 4 == 3:
            @pl.when((z < nz - 1) & (z % 2 == 0))
            def _():
                emit(h, x)

    if cube:
        @pl.when((z < nz - 1) & (z % 2 == 1))
        def _():
            for h in range(heads):
                emit(h, x)
    else:
        @pl.when(z == nz - 2)
        def _():
            forward_start()

    @pl.when(z == nz - 1)
    def _():
        if cube:
            x_send(1)
        local_side()
        if cube:
            x_relay(0)
            for h in range(heads):
                emit(h, x)
        else:
            scatter_wait(0)

    def state_loop():
        lax.fori_loop(0, blocks, state_step, 0)

    if cube:
        state_loop()

        @pl.when(z < nz - 2)
        def _():
            x_forward()

        @pl.when(z >= nz - 2)
        def _():
            x_relay(1)

        for h in range(heads):
            for c in range(4 * h, 4 * (h + 1)):
                pltpu.make_async_remote_copy(
                    src_ref=b_out.at[1 - x, c], dst_ref=b_in.at[1 - x, c],
                    send_sem=b_send.at[1 - x], recv_sem=b_recv.at[0, c],
                    device_id={"sp": z * nx + 1 - x}, device_id_type=MESH).wait_recv()
            emit(h, 1 - x)
            for m in range(nx):
                fr_buf[h, m * dvx : (m + 1) * dvx, :] = b_in[m, 4 * h : 4 * h + 4].reshape(dvx, DK)
    else:
        for h in range(heads):
            for m in range(nx):
                for c in range(4 * h, 4 * (h + 1)):
                    @pl.when(m != x)
                    def _():
                        pltpu.make_async_remote_copy(
                            src_ref=b_out.at[m, c], dst_ref=b_in.at[m, c],
                            send_sem=b_send.at[m], recv_sem=b_recv.at[slot(x, m), c],
                            device_id={"sp": z * nx + m}, device_id_type=MESH).wait_recv()
                    at = m * dvx + c % 4 * half_v
                    fr_buf[h, at : at + half_v, :] = b_in[m, c]
            narrow = fr_buf[h].astype(BF16)
            vg_buf[:, hv(h)] = (vp_buf[:, hv(h)] + nt(k_span[:, hd(h)], narrow)).astype(BF16)


    half_c = cols // 2
    p = ring_place(z, x, nz, nx)
    ahead = ring_member((p + 1) % n, nz, nx)
    behind = ring_member((p + n - 1) % n, nz, nx)

    def share(d, u, owner):
        rows_ = pl.ds(pl.multiple_of(owner * own + u * half_r, half_r), half_r)
        return nn(xt_buf[rows_, :], vg_buf[:, d * half_c : (d + 1) * half_c])

    def ring_copy(step, d, u, src):
        return pltpu.make_async_remote_copy(
            src_ref=src, dst_ref=ring.at[step, d, u],
            send_sem=r_send.at[step, d, u], recv_sem=r_recv.at[step, d, u],
            device_id={"sp": ahead if d == 0 else behind}, device_id_type=MESH)

    def owner_at(step, d):
        return ring_member((p + n - step - 1) % n if d == 0 else (p + step + 1) % n, nz, nx)

    if not cube:
        for u in range(2):
            for d in range(2):
                first[d, u] = share(d, u, owner_at(0, d))
                ring_copy(0, d, u, first.at[d, u]).start()

    def key_side():
        for h in range(heads):
            dots = jnp.where(inside(), nt(o_ref[:, hv(h)], v_buf[:, hv(h)]), 0.0).astype(BF16)
            y_buf[:, hd(h)] += nn(dots, ks_buf[:, hd(h)])
            k_grad = (
                tail_buf[:, hd(h)] * kp_buf[:, hd(h)]
                + jnp.exp(-c_buf[:, hd(h)]) * tn(dots, qg_buf[:, hd(h)])
                + k_far[:, hd(h)] * nn(v_buf[:, hv(h)], fr_buf[h].astype(BF16))
            )
            kp_buf[:, hd(h)] = k_grad
            dk_ref[:, hd(h)] = k_grad.astype(BF16)

    if not cube:
        state_loop()
        key_side()

    def query_side(first_head=0, last_head=heads):
        for m in range(nx):
            if first_head:
                break

            @pl.when(m != x)
            def _():
                pltpu.make_async_remote_copy(
                    src_ref=c_out.at[m], dst_ref=c_in.at[m],
                    send_sem=c_send.at[m], recv_sem=c_recv.at[m],
                    device_id={"sp": z * nx + m}, device_id_type=MESH).wait_recv()
        upper = jnp.where(col >= row, 1.0, 0.0).astype(BF16)
        for h in range(first_head, last_head):
            state_in = jnp.concatenate([c_in[m, h] for m in range(nx)], axis=0)
            q_side = q_ref[:, hd(h)].astype(F32) * scale
            k_side = k_ref[:, hd(h)].astype(F32)
            q_grad = jnp.exp(c_buf[:, hd(h)]) * y_buf[:, hd(h)] + jnp.exp(span_buf[:, hd(h)]) * nn(
                o_ref[:, hv(h)], state_in.astype(BF16)
            )
            dq_ref[:, hd(h)] = (q_grad * scale).astype(BF16)
            terms = q_side * q_grad - k_side * kp_buf[:, hd(h)]
            far = jnp.exp(span_buf[tokens - 1 : tokens, hd(h)])
            span_end = st_buf[0, h] + far * state_in
            carry = jnp.sum(fr_buf[h] * span_end, axis=0, keepdims=True)
            dg_ref[:, hd(h)] = sum(nn(upper, part_) for part_ in pieces(terms, 3)) + carry

    def ring_step(step, carry):
        for d in range(2):
            for u in range(2):
                part[d, u] = share(d, u, owner_at(step, d))
        for u in range(2):
            for d in range(2):
                ring_copy(step - 1, d, u, first.at[d, u]).wait_recv()
                ring[step - 1, d, u] += part[d, u]
                ring_copy(step, d, u, ring.at[step - 1, d, u]).start()

        @pl.when(step == 2)
        def _():
            forward_spread()

        @pl.when(step == 4)
        def _():
            query_side()

        return carry

    if not cube:
        lax.fori_loop(1, n - 1, ring_step, 0)

        for d in range(2):
            for u in range(2):
                part[d, u] = share(d, u, me)
        for u in range(2):
            squares = 0.0
            for d in range(2):
                ring_copy(n - 2, d, u, first.at[d, u]).wait_recv()
                done = ring[n - 2, d, u] + part[d, u]
                dw_ref[u * half_r : (u + 1) * half_r, d * half_c : (d + 1) * half_c] = done
                for at in range(0, half_c, 128):
                    squares = squares + done[:, at : at + 128] * done[:, at : at + 128]
            norm_out[u] = jnp.broadcast_to(jnp.sum(squares.T, axis=0, keepdims=True), (8, half_r))
    else:
        @pl.when(z >= nz - 2)
        def _():
            x_forward()

        @pl.when((z > 0) & (z < nz - 2))
        def _():
            scatter_wait(0)
            forward_step()

        k0, k1, k2, k3 = x, nx + x, 1 - x, nx + 1 - x
        x_take()
        take_near(k0)
        side_send(k0, 0)
        take_near(k1)
        side_send(k1, 0)
        key_side()
        take_near(k2)
        side_send(k2, 0)

        @pl.when(z == nz - 2)
        def _():
            scatter_wait(0)
            forward_step()

        keep(k2, 0)
        far_send(k2)
        side_send(k0, 1)
        take_near(k3)
        side_send(k3, 0)
        keep(k3, 0)
        far_send(k3)
        side_send(k1, 1)
        keep(k0, 0)
        keep(k1, 0)

        side_send(k2, 1)
        far_send(k0)
        side_send(k3, 1)

        @pl.when(z == nz - 1)
        def _():
            scatter_wait(0)
            forward_step()

        keep(k2, 1)
        keep(k3, 1)
        far_send(k1)
        keep(k0, 1)
        keep(k1, 1)
        query_side(0, heads)
        squares = [0.0, 0.0]
        for c in (k2, k3, k0, k1):
            at = pl.ds(pl.multiple_of(c * wide, wide), wide)
            for u in range(2):
                side_copy(c, 1, u).wait_recv()
                far_copy(c, u).wait_recv()
                done = acc_buf[c, 1, u] + sx_in[c, 1, u] + sm_in[c, u]
                dw_ref[u * half_r : (u + 1) * half_r, at] = done
                squares[u] = squares[u] + done * done
        for u in range(2):
            norm_out[u] = jnp.broadcast_to(jnp.sum(squares[u].T, axis=0, keepdims=True), (8, half_r))

    def norm_copy(off):
        return pltpu.make_async_remote_copy(
            src_ref=norm_out, dst_ref=norm_in.at[off],
            send_sem=n_send.at[off], recv_sem=n_recv.at[off],
            device_id={"tp": (mine + off) % ntp}, device_id_type=MESH)

    for off in range(1, ntp):
        norm_copy(off).start()

    for m in range(nx):
        @pl.when(m != x)
        def _():
            for d in range(2):
                pltpu.make_async_remote_copy(
                    src_ref=a_out.at[d, m], dst_ref=a_in.at[d, x],
                    send_sem=a_send.at[d, m], recv_sem=a_recv.at[slot(m, x)],
                    device_id={"sp": z * nx + m}, device_id_type=MESH).wait_send()
            pltpu.make_async_remote_copy(
                src_ref=b_out.at[m], dst_ref=b_in.at[x],
                send_sem=b_send.at[m], recv_sem=b_recv.at[slot(m, x), 0],
                device_id={"sp": z * nx + m}, device_id_type=MESH).wait_send()
            member_copy(m).wait_send()
    if cube:
        @pl.when(z < nz - 1)
        def _():
            step_copy().wait_send()
    else:
        for dz in range(1, nz):
            @pl.when(z + dz < nz)
            def _():
                plane_copy(dz).wait_send()

    @pl.when(z > 0)
    def _():
        pltpu.make_async_remote_copy(
            src_ref=h_out, dst_ref=h_in,
            send_sem=h_send, recv_sem=h_recv.at[0],
            device_id={"sp": (z - 1) * nx + x}, device_id_type=MESH).wait_send()

    if not cube:
        def sent(step, carry):
            for u in range(2):
                for d in range(2):
                    ring_copy(step, d, u, first.at[d, u]).wait_send()
            return carry

        lax.fori_loop(0, n - 1, sent, 0)
    else:
        def all_sent(ref, sem):
            pltpu.make_async_remote_copy(
                src_ref=ref, dst_ref=ref, send_sem=sem, recv_sem=v_recv.at[0],
                device_id={"sp": near * nx + x}, device_id_type=MESH).wait_send()

        all_sent(xs_out, xs_send.at[0])
        all_sent(xr_in.at[mine], xs_send.at[1])
        all_sent(xr_in.at[mine], xs_send.at[2])
        all_sent(xr_in.at[row_mate], xs_send.at[3])
        all_sent(vx_out, v_send)
        all_sent(sx_out, sx_send)
        all_sent(sm_out, sm_send)

    norms = norm_out[...]
    for off in range(1, ntp):
        norm_copy(off).wait()
        norms = norms + norm_in[off]
    rn_ref[...] = norms


def finish(*refs):
    sems = refs[10]
    writes = [pltpu.make_async_copy(refs[i], refs[5 + i], sems.at[i]) for i in range(4)]
    for write in writes:
        write.start()
    refs[9][...] = refs[4][:, :1]
    for write in writes:
        write.wait()


def on_device(n, nx, ntp, block_input, queries, keys, w_value, log_decay, d_out):
    tokens, wide = queries.shape
    heads = wide // DK
    cols = w_value.shape[1]
    depth = block_input.shape[1]
    own = depth // n
    nz = n // nx
    dvx = DV // nx
    vm = pltpu.VMEM
    dma = pltpu.SemaphoreType.DMA
    wide_c = min(cols, 128)
    chunks, half = cols // wide_c, own // 2
    late = [
        vm((2, 2, half, cols // 2), F32),
        vm((2, 2, half, cols // 2), F32),
        vm((n - 1, 2, 2, half, cols // 2), F32),
        dma((n - 1, 2, 2)),
        dma((n - 1, 2, 2)),
    ]
    cube = is_cube(n, nx, ntp) and cols == 2 * DV
    if cube:
        late = [
            vm((2, half, tokens), F32),
            vm((ntp, 2, half, tokens), F32),
            vm((ntp, own, tokens), BF16),
            vm((chunks, tokens, wide_c), F32),
            vm((chunks, tokens, wide_c), F32),
            vm((chunks, tokens, wide_c), BF16),
            vm((chunks, 2, 2, half, wide_c), F32),
            vm((chunks, 2, 2, half, wide_c), F32),
            vm((chunks, 2, 2, half, wide_c), F32),
            vm((chunks, 2, half, wide_c), F32),
            vm((chunks, 2, half, wide_c), F32),
            dma((4,)),
            dma((ntp, 2)),
            dma,
            dma((chunks,)),
            dma,
            dma((chunks, 2, 2)),
            dma,
            dma((chunks, 2)),
        ]
    out = pl.pallas_call(
        functools.partial(kernel, n, nx, ntp),
        out_shape=(
            vm((tokens, wide), BF16),
            vm((tokens, wide), BF16),
            vm((tokens, wide), F32),
            vm((own, cols), F32),
            vm((2, 8, own // 2), F32),
        ),
        in_specs=[pl.BlockSpec(memory_space=pltpu.HBM)] * 6,
        out_specs=(pl.BlockSpec(memory_space=vm),) * 5,
        scratch_shapes=[
            vm(block_input.shape, BF16),
            vm(queries.shape, BF16),
            vm(keys.shape, BF16),
            vm(w_value.shape, BF16),
            vm(log_decay.shape, F32),
            vm(d_out.shape, BF16),
            dma((6,)),
            vm((tokens, wide), F32),
            vm((tokens, wide), F32),
            vm((tokens, cols), BF16),
            vm((tokens, wide), BF16),
            vm((tokens, wide), BF16),
            vm((tokens, wide), BF16),
            vm((tokens, wide), F32),
            vm((tokens, wide), F32),
            vm((tokens, cols), F32),
            vm((2, heads, DV, DK), F32),
            vm((depth, tokens), BF16),
            vm((chunks, tokens, wide_c) if cube else (tokens, cols), BF16),
            vm((2, nx, heads, dvx + 8, DK), F32),
            vm((2, nx, heads, dvx + 8, DK), F32),
            vm((heads, dvx + 8, DK), F32),
            vm((nz, heads, dvx + 8, DK), F32),
            vm((heads, dvx, DK), F32),
            vm((nx, heads, dvx, DK), F32),
            vm((nx, heads, dvx, DK), F32),
            vm((4 * heads, dvx // 4, DK), F32),
            vm((4 * heads, dvx // 4, DK), F32),
            vm((nx, 4 * heads, dvx // 4, DK), F32),
            vm((nx, 4 * heads, dvx // 4, DK), F32),
            vm((heads, DV, DK), F32),
            vm((2, 8, own // 2), F32),
            vm((ntp, 2, 8, own // 2), F32),
            dma((2, nx)),
            dma((nx - 1,)),
            dma((nx - 1, 4 * heads)),
            dma((nz,)),
            dma((nz,)),
            dma((nx,)),
            dma((nx,)),
            dma,
            dma((4 * heads,)),
            dma((nx,)),
            dma((nx - 1, 4 * heads)),
            dma((ntp,)),
            dma((ntp,)),
            vm((tokens, wide), F32),
            *late,
        ],
        compiler_params=pltpu.CompilerParams(
            collective_id=0, has_side_effects=True, vmem_limit_bytes=62 * 1024 * 1024
        ),
    )(block_input, queries, keys, w_value, log_decay, d_out)
    final = pl.pallas_call(
        finish,
        out_shape=tuple(jax.ShapeDtypeStruct(a.shape, a.dtype) for a in out[:4])
        + (jax.ShapeDtypeStruct((2, 1, own // 2), F32),),
        in_specs=[pl.BlockSpec(memory_space=vm)] * 5,
        out_specs=(pl.BlockSpec(memory_space=pltpu.HBM),) * 4 + (pl.BlockSpec(memory_space=vm),),
        scratch_shapes=[dma((4,))],
        compiler_params=pltpu.CompilerParams(vmem_limit_bytes=1024 * 1024),
    )(*out)
    return (*final[:4], final[4].reshape(-1))


def solution(mesh):
    n, ntp = mesh.shape["sp"], mesh.shape["tp"]
    nx = 1 << ((n.bit_length() - 1) // 2)
    placed = (
        P("sp", None),
        P("sp", "tp"),
        P("sp", "tp"),
        P(None, "tp"),
        P("sp", "tp"),
        P("sp", "tp"),
    )
    return jax.shard_map(
        functools.partial(on_device, n, nx, ntp),
        mesh=mesh,
        in_specs=placed,
        out_specs=(P("sp", "tp"), P("sp", "tp"), P("sp", "tp"), P("sp", "tp"), P("sp")),
        check_vma=False,
    )
```

```python
import functools

import jax
import jax.numpy as jnp
from jax import lax
from jax.experimental import pallas as pl
from jax.experimental.pallas import tpu as pltpu
from jax.sharding import PartitionSpec as P

DK = 128
DV = 256
BLOCK = 32
F32 = jnp.float32
BF16 = jnp.bfloat16
MESH = pl.DeviceIdType.MESH


def nn(left, right):
    return lax.dot_general(left, right, (((1,), (0,)), ((), ())), preferred_element_type=F32)


def nt(left, right):
    return lax.dot_general(left, right, (((1,), (1,)), ((), ())), preferred_element_type=F32)


def tn(left, right):
    return lax.dot_general(left, right, (((0,), (0,)), ((), ())), preferred_element_type=F32)


def pieces(value, count):
    parts = []
    for _ in range(count):
        part = value.astype(BF16)
        parts.append(part)
        value = value - part.astype(F32)
    return parts


def ring_place(z, x, nz, nx):
    r = nz - 1 - z
    across = jnp.where(r % 2 == 0, x - 1, nx - 1 - x)
    return jnp.where(x == 0, z, nz + r * (nx - 1) + across)


def ring_member(p, nz, nx):
    u = jnp.maximum(p - nz, 0)
    r = u // (nx - 1)
    w = u % (nx - 1)
    x = jnp.where(r % 2 == 0, 1 + w, nx - 1 - w)
    return jnp.where(p < nz, p * nx, (nz - 1 - r) * nx + x)


def is_cube(n, nx, ntp):
    return nx == 2 and n == 4 * nx and ntp == 2 * nx


def kernel(
    n, nx, ntp,
    x_hbm, q_hbm, k_hbm, w_hbm, g_hbm, o_hbm,
    dq_ref, dk_ref, dg_ref, dw_ref, rn_ref,
    x_ref, q_ref, k_ref, w_ref, g_ref, o_ref, in_sem,
    c_buf, span_buf, v_buf, qg_buf, kt_buf, ks_buf, y_buf, kp_buf, vp_buf, st_buf, xt_buf, vg_buf,
    a_out, a_in, z_out, z_in, z_acc, c_out, c_in, h_out, h_in, b_out, b_in, fr_buf,
    norm_out, norm_in,
    a_send, a_recv, e_recv, z_send, z_recv, c_send, c_recv, h_send, h_recv, b_send, b_recv, n_send, n_recv,
    tail_buf, ksp_buf, *late,
):
    cube = is_cube(n, nx, ntp) and dw_ref.shape[1] == 2 * DV
    if cube:
        (xs_out, xr_in, xr_buf, vx_out, vx_in, vgp_buf, sx_out, sx_in, acc_buf, sm_out, sm_in,
         xs_send, xr_recv, xc_recv, v_send, v_recv, sx_send, sx_recv, sm_send, sm_recv) = late
    else:
        first, part, ring, r_send, r_recv = late
    nz = n // nx
    me = lax.axis_index("sp")
    mine = lax.axis_index("tp")
    z, x = me // nx, me % nx
    tokens, heads = q_ref.shape[0], q_ref.shape[1] // DK
    blocks = tokens // BLOCK
    dvx = DV // nx
    scale = DK ** (-0.5)
    loads = [
        pltpu.make_async_copy(source, target, in_sem.at[i])
        for i, (source, target) in enumerate(
            [(g_hbm, g_ref), (q_hbm, q_ref), (o_hbm, o_ref), (k_hbm, k_ref), (x_hbm, x_ref), (w_hbm, w_ref)]
        )
    ]
    for load in loads:
        load.start()
    barrier = pltpu.get_barrier_semaphore()
    for off in range(1, nx):
        pl.semaphore_signal(
            barrier, inc=1, device_id={"sp": z * nx + (x + off) % nx}, device_id_type=MESH)
    for off in range(1, nz):
        pl.semaphore_signal(
            barrier, inc=1, device_id={"sp": (z + off) % nz * nx + x}, device_id_type=MESH)
    for off in range(1, ntp):
        pl.semaphore_signal(barrier, inc=1, device_id={"tp": (mine + off) % ntp}, device_id_type=MESH)

    row = lax.broadcasted_iota(jnp.int32, (tokens, tokens), 0)
    col = lax.broadcasted_iota(jnp.int32, (tokens, tokens), 1)
    tri = jnp.where(col <= row, 1.0, 0.0).astype(BF16)

    def inside():
        return (col <= row) & (col // BLOCK == row // BLOCK)

    def hd(h):
        return slice(h * DK, (h + 1) * DK)

    def hv(h):
        return slice(h * DV, (h + 1) * DV)

    def total(h):
        return span_buf[tokens - 1 : tokens, hd(h)]

    quarter = dvx // 4

    def part_rows(part):
        return slice(8 + part * quarter if part else 0, 8 + (part + 1) * quarter)

    def slot(to, frm):
        return (frm + nx - 1 - to) % nx

    def first_part(m, h, part):
        return pltpu.make_async_remote_copy(
            src_ref=a_out.at[1, m, h, part_rows(part), :], dst_ref=a_in.at[1, x, h, part_rows(part), :],
            send_sem=a_send.at[1, m], recv_sem=e_recv.at[slot(m, x), h * 4 + part],
            device_id={"sp": z * nx + m}, device_id_type=MESH)

    def first_wait(h, part):
        for m in range(nx):
            @pl.when(m != x)
            def _():
                pltpu.make_async_remote_copy(
                    src_ref=a_out.at[1, m, h, part_rows(part), :], dst_ref=a_in.at[1, m, h, part_rows(part), :],
                    send_sem=a_send.at[1, m], recv_sem=e_recv.at[slot(x, m), h * 4 + part],
                    device_id={"sp": z * nx + m}, device_id_type=MESH).wait_recv()

    def scatter_copy(d, m):
        return pltpu.make_async_remote_copy(
            src_ref=a_out.at[d, m], dst_ref=a_in.at[d, x],
            send_sem=a_send.at[d, m], recv_sem=a_recv.at[slot(m, x)],
            device_id={"sp": z * nx + m}, device_id_type=MESH)

    def scatter_wait(d):
        for m in range(nx):
            @pl.when(m != x)
            def _():
                pltpu.make_async_remote_copy(
                    src_ref=a_out.at[d, m], dst_ref=a_in.at[d, m],
                    send_sem=a_send.at[d, m], recv_sem=a_recv.at[slot(x, m)],
                    device_id={"sp": z * nx + m}, device_id_type=MESH).wait_recv()

    def give(d, h, totals):
        for m in range(nx):
            a_out[d, m, h, :8, :] = jnp.broadcast_to(jnp.exp(total(h)), (8, DK))
            a_out[d, m, h, 8:, :] = totals[m * dvx : (m + 1) * dvx]
        for m in range(nx):
            @pl.when(m != x)
            def _():
                if d == 1:
                    for part in range(4):
                        first_part(m, h, part).start()
                elif h == heads - 1:
                    scatter_copy(d, m).start()

            @pl.when(m == x)
            def _():
                a_in[d, m, h] = a_out[d, m, h]

    loads[0].wait()
    for h in range(heads):
        span = sum(nn(tri, part_) for part_ in pieces(g_ref[:, hd(h)], 3))
        span_buf[:, hd(h)] = span
        if h == 0:
            loads[1].wait()
        q_span = (q_ref[:, hd(h)].astype(F32) * scale * jnp.exp(span)).astype(BF16)
        if h == 0:
            loads[2].wait()
        adjoint = tn(o_ref[:, hv(h)], q_span)
        if h == 0:
            pl.semaphore_wait(barrier, nx - 1 + nz - 1 + ntp - 1)
        give(1, h, adjoint)

    loads[4].wait()
    depth = x_ref.shape[1]
    for at in range(0, depth, 256):
        xt_buf[at : at + 256, :] = x_ref[:, at : at + 256].T

    own = dw_ref.shape[0]
    cols = dw_ref.shape[1]
    wide = min(cols, 128)
    chunks = cols // wide
    half_r = own // 2
    near, mirror = z + 1 - 2 * (z % 2), nz - 1 - z
    core_mate, row_mate = mine + 1 - 2 * (mine % 2), (mine + 2) % 4

    def block_rows(slab, xx, base=0, size=None):
        unit = half_r // 2
        return pl.ds(pl.multiple_of((slab * nx + xx) * own + base, unit), own if size is None else size)

    x_parts = 4
    x_rows = own // x_parts

    def x_copy(p):
        return pltpu.make_async_remote_copy(
            src_ref=xs_out.at[p], dst_ref=xr_in.at[mine, p],
            send_sem=xs_send.at[0], recv_sem=xr_recv.at[4 + p],
            device_id={"sp": near * nx + x}, device_id_type=MESH)

    def x_pass(which, block, p, mate):
        return pltpu.make_async_remote_copy(
            src_ref=xr_in.at[block, p], dst_ref=xr_in.at[block, p],
            send_sem=xs_send.at[which], recv_sem=xr_recv.at[p] if which == 2 else xc_recv.at[which // 2],
            device_id={"tp": mate}, device_id_type=MESH)

    def x_send(p):
        slab = jnp.where(mine < nx, nz - 1 - near, near)
        xs_out[p] = xt_buf[block_rows(slab, mine % nx, p * x_rows, x_rows), :].astype(F32)
        x_copy(p).start()

    def x_relay(p):
        x_copy(p).wait_recv()
        x_pass(2, mine, p, row_mate).start()
        x_pass(1, mine, p, core_mate).start()

    def x_forward():
        for p in range(x_parts):
            x_pass(2, row_mate, p, row_mate).wait_recv()
            x_pass(3, row_mate, p, core_mate).start()

    def x_take():
        far_mate = (core_mate + 2) % 4
        for i, block in enumerate((core_mate, far_mate)):
            pltpu.make_async_remote_copy(
                src_ref=xr_in.at[block], dst_ref=xr_in.at[block],
                send_sem=xs_send.at[1], recv_sem=xc_recv.at[i],
                device_id={"tp": core_mate}, device_id_type=MESH).wait_recv()
        for j in range(2 * nx):
            for p in range(x_parts):
                xr_buf[j, p * x_rows : (p + 1) * x_rows] = xr_in[j, p].astype(BF16)

    if cube:
        x_send(0)

        @pl.when(z < nz - 1)
        def _():
            for p in range(1, x_parts):
                x_send(p)

    loads[3].wait()
    loads[5].wait()

    def value_side(first_head=0, last_head=heads):
        for h in range(first_head, last_head):
            k_far = jnp.exp(total(h) - span_buf[:, hd(h)])
            ksp_buf[:, hd(h)] = (k_ref[:, hd(h)].astype(F32) * k_far).astype(BF16)
            v_buf[:, hv(h)] = nn(x_ref[...], w_ref[:, hv(h)]).astype(BF16)
            give(0, h, tn(v_buf[:, hv(h)], ksp_buf[:, hd(h)]))

    def order(d):
        return range(nx) if d == 0 else range(nx - 1, -1, -1)

    def plane_copy(dz):
        return pltpu.make_async_remote_copy(
            src_ref=z_out, dst_ref=z_in.at[z],
            send_sem=z_send.at[dz], recv_sem=z_recv.at[z],
            device_id={"sp": (z + dz) * nx + x}, device_id_type=MESH)

    def composite(d, h, rows_):
        acc, dec = None, None
        for m in order(d):
            local, rate = a_in[d, m, h, rows_, :], a_in[d, m, h, 0:1, :]
            acc = local if acc is None else local + rate * acc
            dec = rate if dec is None else rate * dec
        return acc, dec

    def forward_start():
        scatter_wait(0)
        for h in range(heads):
            acc, dec = composite(0, h, slice(8, 8 + dvx))
            z_out[h, :dvx, :] = acc
            z_out[h, dvx:, :] = jnp.broadcast_to(dec, (8, DK))
        for dz in range(1, nz):
            @pl.when(z + dz < nz)
            def _():
                plane_copy(dz).start()

    def local_side():
        tri_in = jnp.where(inside(), 1.0, 0.0).astype(BF16)
        g_parts = pieces(g_ref[...], 3)
        q_all = q_ref[...].astype(F32) * scale
        k_all = k_ref[...].astype(F32)
        last_in = jnp.where(col // BLOCK == row // BLOCK, 1.0, 0.0).astype(BF16)
        cum = sum(nn(tri_in, part_) for part_ in g_parts)
        c_buf[...] = cum
        block_end = sum(nn(last_in, part_) for part_ in g_parts)
        k_tail = jnp.exp(block_end - cum)
        tail_buf[...] = k_tail
        grow = jnp.exp(cum)
        qg_buf[...] = (q_all * grow).astype(BF16)
        ks_buf[...] = (k_all * jnp.exp(-cum)).astype(BF16)
        kt_buf[...] = (k_all * k_tail).astype(BF16)
        st_buf[...] = jnp.zeros_like(st_buf)

        def adjoint_step(step, carry):
            rows = pl.ds(pl.multiple_of((blocks - 1 - step) * BLOCK, BLOCK), BLOCK)
            for h in range(heads):
                keep = jnp.exp(c_buf[rows, hd(h)][BLOCK - 1 :])
                adjoint = st_buf[1, h]
                narrow = adjoint.astype(BF16)
                kp_buf[rows, hd(h)] = nn(v_buf[rows, hv(h)], narrow)
                vp_buf[rows, hv(h)] = nt(kt_buf[rows, hd(h)], narrow)
                st_buf[1, h] = keep * adjoint + tn(o_ref[rows, hv(h)], qg_buf[rows, hd(h)])
            return carry

        lax.fori_loop(0, blocks, adjoint_step, 0)

        for h in range(heads):
            dots = jnp.where(inside(), nt(qg_buf[:, hd(h)], ks_buf[:, hd(h)]), 0.0).astype(BF16)
            vp_buf[:, hv(h)] += tn(dots, o_ref[:, hv(h)])

    def state_step(step, carry):
        rows = pl.ds(pl.multiple_of(step * BLOCK, BLOCK), BLOCK)
        for h in range(heads):
            keep = jnp.exp(c_buf[rows, hd(h)][BLOCK - 1 :])
            state = st_buf[0, h]
            y_buf[rows, hd(h)] = nn(o_ref[rows, hv(h)], state.astype(BF16))
            st_buf[0, h] = keep * state + tn(v_buf[rows, hv(h)], kt_buf[rows, hd(h)])
        return carry

    def member_copy(m):
        return pltpu.make_async_remote_copy(
            src_ref=c_out.at[m], dst_ref=c_in.at[x],
            send_sem=c_send.at[slot(x, m)], recv_sem=c_recv.at[slot(m, x)],
            device_id={"sp": z * nx + m}, device_id_type=MESH)

    def forward_spread():
        z_acc[...] = jnp.zeros_like(z_acc)
        for zp in range(nz):
            @pl.when(zp < z)
            def _():
                pltpu.make_async_remote_copy(
                    src_ref=z_out, dst_ref=z_in.at[zp],
                    send_sem=z_send.at[0], recv_sem=z_recv.at[zp],
                    device_id={"sp": zp * nx + x}, device_id_type=MESH).wait_recv()
                for h in range(heads):
                    z_acc[h] = z_in[zp, h, :dvx, :] + z_in[zp, h, dvx : dvx + 1, :] * z_acc[h]
        for h in range(heads):
            acc = z_acc[h]
            for m in order(0):
                c_out[m, h] = acc
                acc = a_in[0, m, h, 8:, :] + a_in[0, m, h, 0:1, :] * acc
        for m in range(nx):
            @pl.when(m != x)
            def _():
                member_copy(m).start()

            @pl.when(m == x)
            def _():
                c_in[m] = c_out[m]

    def step_copy():
        return pltpu.make_async_remote_copy(
            src_ref=z_out, dst_ref=z_in.at[0],
            send_sem=z_send.at[0], recv_sem=z_recv.at[0],
            device_id={"sp": (z + 1) * nx + x}, device_id_type=MESH)

    def forward_step():
        @pl.when(z == 0)
        def _():
            z_acc[...] = jnp.zeros_like(z_acc)

        @pl.when(z > 0)
        def _():
            step_copy().wait_recv()
            for h in range(heads):
                z_acc[h] = z_in[0, h, :dvx, :]

        for h in range(heads):
            acc = z_acc[h]
            for m in order(0):
                c_out[m, h] = acc
                acc = a_in[0, m, h, 8:, :] + a_in[0, m, h, 0:1, :] * acc
            z_out[h, :dvx, :] = acc
            z_out[h, dvx:, :] = jnp.zeros((8, DK), F32)

        @pl.when(z < nz - 1)
        def _():
            step_copy().start()

        for m in range(nx):
            @pl.when(m != x)
            def _():
                member_copy(m).start()

            @pl.when(m == x)
            def _():
                c_in[m] = c_out[m]

    def near_copy(c):
        return pltpu.make_async_remote_copy(
            src_ref=vx_out.at[c], dst_ref=vx_in.at[c],
            send_sem=v_send, recv_sem=v_recv.at[c],
            device_id={"sp": near * nx + x}, device_id_type=MESH)

    def side_copy(c, s, u):
        return pltpu.make_async_remote_copy(
            src_ref=sx_out.at[c, s, u], dst_ref=sx_in.at[c, s, u],
            send_sem=sx_send, recv_sem=sx_recv.at[c, s, u],
            device_id={"sp": z * nx + 1 - x}, device_id_type=MESH)

    def far_copy(c, u):
        return pltpu.make_async_remote_copy(
            src_ref=sm_out.at[c, u], dst_ref=sm_in.at[c, u],
            send_sem=sm_send, recv_sem=sm_recv.at[c, u],
            device_id={"sp": mirror * nx + x}, device_id_type=MESH)

    def emit(h, m):
        c = h * nx + m
        held = b_in[m, 4 * h : 4 * h + 4].reshape(dvx, DK).astype(BF16)
        at = pl.ds(pl.multiple_of(c * wide, wide), wide)
        value = (vp_buf[:, at] + nt(ksp_buf[:, hd(h)], held)).astype(BF16)
        vg_buf[c] = value
        vx_out[c] = value.astype(F32)
        near_copy(c).start()

    def piece(c, s, xx):
        slab = mirror if s == 0 else z
        return nn(xt_buf[block_rows(slab, xx), :], vg_buf[c]) + nn(xr_buf[s * nx + xx], vgp_buf[c])

    def take_near(c):
        near_copy(c).wait_recv()
        vgp_buf[c] = vx_in[c].astype(BF16)

    def side_send(c, s):
        value = piece(c, s, 1 - x)
        for u in range(2):
            sx_out[c, s, u] = value[u * half_r : (u + 1) * half_r]
            side_copy(c, s, u).start()

    def keep(c, s):
        value = piece(c, s, x)
        for u in range(2):
            acc_buf[c, s, u] = value[u * half_r : (u + 1) * half_r]

    def far_send(c):
        for u in range(2):
            side_copy(c, 0, u).wait_recv()
            sm_out[c, u] = acc_buf[c, 0, u] + sx_in[c, 0, u]
            far_copy(c, u).start()

    @pl.when(z < nz - 1)
    def _():
        value_side()
        local_side()

    if cube:
        @pl.when(z < nz - 1)
        def _():
            x_relay(0)

        @pl.when(z < nz - 2)
        def _():
            x_relay(1)

    if not cube:
        @pl.when(z < nz - 2)
        def _():
            forward_start()

    if cube:
        @pl.when(z < nz - 2)
        def _():
            for p in range(2, x_parts):
                x_relay(p)

        @pl.when(z == 0)
        def _():
            scatter_wait(0)
            forward_step()

    @pl.when(z == nz - 1)
    def _():
        value_side(0, 1)

    half_v = dvx // 4

    def chain_copy(c):
        return pltpu.make_async_remote_copy(
            src_ref=h_out.at[c], dst_ref=h_in.at[c],
            send_sem=h_send, recv_sem=h_recv.at[c],
            device_id={"sp": (z - 1) * nx + x}, device_id_type=MESH)

    def piece_copy(m, c):
        return pltpu.make_async_remote_copy(
            src_ref=b_out.at[m, c], dst_ref=b_in.at[x, c],
            send_sem=b_send.at[m], recv_sem=b_recv.at[slot(m, x), c],
            device_id={"sp": z * nx + m}, device_id_type=MESH)

    for c in range(4 * heads):
        h, rows_ = c // 4, slice(8 + c % 4 * half_v, 8 + (c % 4 + 1) * half_v)
        first_wait(h, c % 4)
        acc, dec = composite(1, h, rows_)

        @pl.when(z == nz - 1)
        def _():
            h_in[c] = jnp.zeros((half_v, DK), F32)

        @pl.when(z < nz - 1)
        def _():
            chain_copy(c).wait_recv()

        enter = h_in[c]

        @pl.when(z > 0)
        def _():
            h_out[c] = acc + dec * enter
            chain_copy(c).start()

        for m in order(1):
            b_out[m, c] = enter
            enter = a_in[1, m, h, rows_, :] + a_in[1, m, h, 0:1, :] * enter
        for m in range(nx):
            @pl.when(m != x)
            def _():
                piece_copy(m, c).start()

            @pl.when(m == x)
            def _():
                b_in[m, c] = b_out[m, c]

        if cube and c == 3:
            @pl.when((z < nz - 1) & (z % 2 == 0))
            def _():
                emit(0, x)

            @pl.when(z == 0)
            def _():
                x_forward()

    if cube:
        @pl.when((z < nz - 1) & (z % 2 == 1))
        def _():
            emit(0, x)
    else:
        @pl.when(z == nz - 2)
        def _():
            forward_start()

    @pl.when(z == nz - 1)
    def _():
        if cube:
            for p in range(1, x_parts):
                x_send(p)
            x_relay(0)
        value_side(1, heads)
        if cube:
            x_relay(1)
        local_side()
        if cube:
            for p in range(2, x_parts):
                x_relay(p)
        else:
            scatter_wait(0)

    def state_loop():
        lax.fori_loop(0, blocks, state_step, 0)

    if cube:
        @pl.when(z < nz - 1)
        def _():
            state_loop()

        @pl.when((z > 0) & (z < nz - 2))
        def _():
            x_forward()

        @pl.when(z == nz - 2)
        def _():
            for p in range(1, x_parts - 1):
                x_relay(p)

        for h in range(heads):
            for c in range(4 * h, 4 * (h + 1)):
                pltpu.make_async_remote_copy(
                    src_ref=b_out.at[1 - x, c], dst_ref=b_in.at[1 - x, c],
                    send_sem=b_send.at[1 - x], recv_sem=b_recv.at[0, c],
                    device_id={"sp": z * nx + 1 - x}, device_id_type=MESH).wait_recv()

            @pl.when(z < nz - 1)
            def _():
                emit(h, 1 - x)
                if h == 0:
                    emit(1, x)

                    @pl.when(z == nz - 2)
                    def _():
                        x_relay(x_parts - 1)

            @pl.when(z == nz - 1)
            def _():
                for m in range(nx):
                    emit(h, m)

            for m in range(nx):
                fr_buf[h, m * dvx : (m + 1) * dvx, :] = b_in[m, 4 * h : 4 * h + 4].reshape(dvx, DK)

        @pl.when(z == nz - 1)
        def _():
            state_loop()
    else:
        for h in range(heads):
            for m in range(nx):
                for c in range(4 * h, 4 * (h + 1)):
                    @pl.when(m != x)
                    def _():
                        pltpu.make_async_remote_copy(
                            src_ref=b_out.at[m, c], dst_ref=b_in.at[m, c],
                            send_sem=b_send.at[m], recv_sem=b_recv.at[slot(x, m), c],
                            device_id={"sp": z * nx + m}, device_id_type=MESH).wait_recv()
                    at = m * dvx + c % 4 * half_v
                    fr_buf[h, at : at + half_v, :] = b_in[m, c]
            narrow = fr_buf[h].astype(BF16)
            vg_buf[:, hv(h)] = (vp_buf[:, hv(h)] + nt(ksp_buf[:, hd(h)], narrow)).astype(BF16)


    half_c = cols // 2
    p = ring_place(z, x, nz, nx)
    ahead = ring_member((p + 1) % n, nz, nx)
    behind = ring_member((p + n - 1) % n, nz, nx)

    def share(d, u, owner):
        rows_ = pl.ds(pl.multiple_of(owner * own + u * half_r, half_r), half_r)
        return nn(xt_buf[rows_, :], vg_buf[:, d * half_c : (d + 1) * half_c])

    def ring_copy(step, d, u, src):
        return pltpu.make_async_remote_copy(
            src_ref=src, dst_ref=ring.at[step, d, u],
            send_sem=r_send.at[step, d, u], recv_sem=r_recv.at[step, d, u],
            device_id={"sp": ahead if d == 0 else behind}, device_id_type=MESH)

    def owner_at(step, d):
        return ring_member((p + n - step - 1) % n if d == 0 else (p + step + 1) % n, nz, nx)

    if not cube:
        for u in range(2):
            for d in range(2):
                first[d, u] = share(d, u, owner_at(0, d))
                ring_copy(0, d, u, first.at[d, u]).start()

    def key_side():
        for h in range(heads):
            dots = jnp.where(inside(), nt(o_ref[:, hv(h)], v_buf[:, hv(h)]), 0.0).astype(BF16)
            y_buf[:, hd(h)] += nn(dots, ks_buf[:, hd(h)])
            k_grad = (
                tail_buf[:, hd(h)] * kp_buf[:, hd(h)]
                + jnp.exp(-c_buf[:, hd(h)]) * tn(dots, qg_buf[:, hd(h)])
                + jnp.exp(total(h) - span_buf[:, hd(h)]) * nn(v_buf[:, hv(h)], fr_buf[h].astype(BF16))
            )
            kp_buf[:, hd(h)] = k_grad
            dk_ref[:, hd(h)] = k_grad.astype(BF16)

    if not cube:
        state_loop()
        key_side()

    def query_side(first_head=0, last_head=heads):
        for m in range(nx):
            if first_head:
                break

            @pl.when(m != x)
            def _():
                pltpu.make_async_remote_copy(
                    src_ref=c_out.at[m], dst_ref=c_in.at[m],
                    send_sem=c_send.at[slot(x, m)], recv_sem=c_recv.at[slot(x, m)],
                    device_id={"sp": z * nx + m}, device_id_type=MESH).wait_recv()
        upper = jnp.where(col >= row, 1.0, 0.0).astype(BF16)
        for h in range(first_head, last_head):
            state_in = jnp.concatenate([c_in[m, h] for m in range(nx)], axis=0)
            q_side = q_ref[:, hd(h)].astype(F32) * scale
            k_side = k_ref[:, hd(h)].astype(F32)
            q_grad = jnp.exp(c_buf[:, hd(h)]) * y_buf[:, hd(h)] + jnp.exp(span_buf[:, hd(h)]) * nn(
                o_ref[:, hv(h)], state_in.astype(BF16)
            )
            dq_ref[:, hd(h)] = (q_grad * scale).astype(BF16)
            terms = q_side * q_grad - k_side * kp_buf[:, hd(h)]
            far = jnp.exp(span_buf[tokens - 1 : tokens, hd(h)])
            span_end = st_buf[0, h] + far * state_in
            carry = jnp.sum(fr_buf[h] * span_end, axis=0, keepdims=True)
            dg_ref[:, hd(h)] = sum(nn(upper, part_) for part_ in pieces(terms, 3)) + carry

    def ring_step(step, carry):
        for d in range(2):
            for u in range(2):
                part[d, u] = share(d, u, owner_at(step, d))
        for u in range(2):
            for d in range(2):
                ring_copy(step - 1, d, u, first.at[d, u]).wait_recv()
                ring[step - 1, d, u] += part[d, u]
                ring_copy(step, d, u, ring.at[step - 1, d, u]).start()

        @pl.when(step == 2)
        def _():
            forward_spread()

        @pl.when(step == 4)
        def _():
            query_side()

        return carry

    if not cube:
        lax.fori_loop(1, n - 1, ring_step, 0)

        for d in range(2):
            for u in range(2):
                part[d, u] = share(d, u, me)
        for u in range(2):
            squares = 0.0
            for d in range(2):
                ring_copy(n - 2, d, u, first.at[d, u]).wait_recv()
                done = ring[n - 2, d, u] + part[d, u]
                dw_ref[u * half_r : (u + 1) * half_r, d * half_c : (d + 1) * half_c] = done
                for at in range(0, half_c, 128):
                    squares = squares + done[:, at : at + 128] * done[:, at : at + 128]
            norm_out[u] = jnp.broadcast_to(jnp.sum(squares.T, axis=0, keepdims=True), (8, half_r))
    else:
        @pl.when(z >= nz - 2)
        def _():
            x_forward()

        @pl.when((z > 0) & (z < nz - 2))
        def _():
            scatter_wait(0)
            forward_step()

        late_half = z >= nz - 2
        turns = [jnp.where(late_half, i, (i // nx) * nx + (x if i % nx == 0 else 1 - x)) for i in range(chunks)]
        s0, s1, s2, s3 = turns
        f0, f1, f2, f3 = [jnp.where(late_half, turns[i], turns[i ^ 1]) for i in range(chunks)]
        x_take()
        take_near(s0)
        side_send(s0, 0)

        @pl.when(z < nz - 1)
        def _():
            keep(s0, 0)
            key_side()
            take_near(s1)
            side_send(s1, 0)
            keep(s1, 0)
            far_send(f0)
            take_near(s2)
            side_send(s2, 0)

            @pl.when(z == nz - 2)
            def _():
                scatter_wait(0)
                forward_step()

            take_near(s3)
            side_send(s3, 0)
            far_send(f1)
            side_send(s0, 1)
            side_send(s1, 1)
            keep(s2, 0)
            keep(s3, 0)
            far_send(f2)
            side_send(s2, 1)
            side_send(s3, 1)
            far_send(f3)
            for c in range(chunks):
                keep(c, 1)

        @pl.when(z == nz - 1)
        def _():
            for c in (s1, s2, s3):
                take_near(c)
                side_send(c, 0)
            key_side()
            for c in range(chunks):
                keep(c, 0)
                side_send(c, 1)
                keep(c, 1)
            far_send(0)
            far_copy(1 - x, 0).wait_recv()
            for c in range(1, chunks):
                far_send(c)
            scatter_wait(0)
            forward_step()

        query_side(0, heads)
        squares = [0.0, 0.0]
        for c in range(chunks):
            at = slice(c * wide, (c + 1) * wide)
            for u in range(2):
                side_copy(c, 1, u).wait_recv()
                if c < nx and u == 0:
                    @pl.when((z < nz - 1) | (c != 1 - x))
                    def _():
                        far_copy(c, u).wait_recv()
                else:
                    far_copy(c, u).wait_recv()
                done = acc_buf[c, 1, u] + sx_in[c, 1, u] + sm_in[c, u]
                dw_ref[u * half_r : (u + 1) * half_r, at] = done
                squares[u] = squares[u] + done * done
        for u in range(2):
            norm_out[u] = jnp.broadcast_to(jnp.sum(squares[u].T, axis=0, keepdims=True), (8, half_r))

    def norm_copy(off):
        return pltpu.make_async_remote_copy(
            src_ref=norm_out, dst_ref=norm_in.at[off],
            send_sem=n_send, recv_sem=n_recv.at[off - 1],
            device_id={"tp": (mine + off) % ntp}, device_id_type=MESH)

    for off in range(1, ntp):
        norm_copy(off).start()

    for m in range(nx):
        @pl.when(m != x)
        def _():
            for d in range(2):
                pltpu.make_async_remote_copy(
                    src_ref=a_out.at[d, m], dst_ref=a_in.at[d, x],
                    send_sem=a_send.at[d, m], recv_sem=a_recv.at[slot(m, x)],
                    device_id={"sp": z * nx + m}, device_id_type=MESH).wait_send()
            pltpu.make_async_remote_copy(
                src_ref=b_out.at[m], dst_ref=b_in.at[x],
                send_sem=b_send.at[m], recv_sem=b_recv.at[slot(m, x), 0],
                device_id={"sp": z * nx + m}, device_id_type=MESH).wait_send()
            member_copy(m).wait_send()
    if cube:
        @pl.when(z < nz - 1)
        def _():
            step_copy().wait_send()
    else:
        for dz in range(1, nz):
            @pl.when(z + dz < nz)
            def _():
                plane_copy(dz).wait_send()

    @pl.when(z > 0)
    def _():
        pltpu.make_async_remote_copy(
            src_ref=h_out, dst_ref=h_in,
            send_sem=h_send, recv_sem=h_recv.at[0],
            device_id={"sp": (z - 1) * nx + x}, device_id_type=MESH).wait_send()

    if not cube:
        def sent(step, carry):
            for u in range(2):
                for d in range(2):
                    ring_copy(step, d, u, first.at[d, u]).wait_send()
            return carry

        lax.fori_loop(0, n - 1, sent, 0)
    else:
        def all_sent(ref, sem):
            pltpu.make_async_remote_copy(
                src_ref=ref, dst_ref=ref, send_sem=sem, recv_sem=v_recv.at[0],
                device_id={"sp": near * nx + x}, device_id_type=MESH).wait_send()

        all_sent(xs_out, xs_send.at[0])
        all_sent(xr_in.at[mine], xs_send.at[1])
        all_sent(xr_in.at[mine], xs_send.at[2])
        all_sent(xr_in.at[row_mate], xs_send.at[3])
        all_sent(vx_out, v_send)
        all_sent(sx_out, sx_send)
        all_sent(sm_out, sm_send)

    norms = norm_out[...]
    for off in range(1, ntp):
        norm_copy(off).wait_recv()
        norms = norms + norm_in[off]
    rn_ref[...] = norms[:, :1]
    pltpu.make_async_remote_copy(
        src_ref=norm_in.at[pl.ds(1, ntp - 1)], dst_ref=norm_in.at[pl.ds(1, ntp - 1)],
        send_sem=n_send, recv_sem=n_recv.at[0],
        device_id={"tp": (mine + 1) % ntp}, device_id_type=MESH).wait_send()


def finish(*refs):
    sems = refs[10]
    writes = [pltpu.make_async_copy(refs[i], refs[5 + i], sems.at[i]) for i in range(5)]
    for write in writes:
        write.start()
    for write in writes:
        write.wait()


def on_device(n, nx, ntp, block_input, queries, keys, w_value, log_decay, d_out):
    tokens, wide = queries.shape
    heads = wide // DK
    cols = w_value.shape[1]
    depth = block_input.shape[1]
    own = depth // n
    nz = n // nx
    dvx = DV // nx
    vm = pltpu.VMEM
    dma = pltpu.SemaphoreType.DMA
    wide_c = min(cols, 128)
    chunks, half = cols // wide_c, own // 2
    late = [
        vm((2, 2, half, cols // 2), F32),
        vm((2, 2, half, cols // 2), F32),
        vm((n - 1, 2, 2, half, cols // 2), F32),
        dma((n - 1, 2, 2)),
        dma((n - 1, 2, 2)),
    ]
    cube = is_cube(n, nx, ntp) and cols == 2 * DV
    if cube:
        late = [
            vm((4, own // 4, tokens), F32),
            vm((ntp, 4, own // 4, tokens), F32),
            vm((ntp, own, tokens), BF16),
            vm((chunks, tokens, wide_c), F32),
            vm((chunks, tokens, wide_c), F32),
            vm((chunks, tokens, wide_c), BF16),
            vm((chunks, 2, 2, half, wide_c), F32),
            vm((chunks, 2, 2, half, wide_c), F32),
            vm((chunks, 2, 2, half, wide_c), F32),
            vm((chunks, 2, half, wide_c), F32),
            vm((chunks, 2, half, wide_c), F32),
            dma((4,)),
            dma((8,)),
            dma((2,)),
            dma,
            dma((chunks,)),
            dma,
            dma((chunks, 2, 2)),
            dma,
            dma((chunks, 2)),
        ]
    out = pl.pallas_call(
        functools.partial(kernel, n, nx, ntp),
        out_shape=(
            vm((tokens, wide), BF16),
            vm((tokens, wide), BF16),
            vm((tokens, wide), F32),
            vm((own, cols), F32),
            vm((2, 1, own // 2), F32),
        ),
        in_specs=[pl.BlockSpec(memory_space=pltpu.HBM)] * 6,
        out_specs=(pl.BlockSpec(memory_space=vm),) * 5,
        scratch_shapes=[
            vm(block_input.shape, BF16),
            vm(queries.shape, BF16),
            vm(keys.shape, BF16),
            vm(w_value.shape, BF16),
            vm(log_decay.shape, F32),
            vm(d_out.shape, BF16),
            dma((6,)),
            vm((tokens, wide), F32),
            vm((tokens, wide), F32),
            vm((tokens, cols), BF16),
            vm((tokens, wide), BF16),
            vm((tokens, wide), BF16),
            vm((tokens, wide), BF16),
            vm((tokens, wide), F32),
            vm((tokens, wide), F32),
            vm((tokens, cols), F32),
            vm((2, heads, DV, DK), F32),
            vm((depth, tokens), BF16),
            vm((chunks, tokens, wide_c) if cube else (tokens, cols), BF16),
            vm((2, nx, heads, dvx + 8, DK), F32),
            vm((2, nx, heads, dvx + 8, DK), F32),
            vm((heads, dvx + 8, DK), F32),
            vm((nz, heads, dvx + 8, DK), F32),
            vm((heads, dvx, DK), F32),
            vm((nx, heads, dvx, DK), F32),
            vm((nx, heads, dvx, DK), F32),
            vm((4 * heads, dvx // 4, DK), F32),
            vm((4 * heads, dvx // 4, DK), F32),
            vm((nx, 4 * heads, dvx // 4, DK), F32),
            vm((nx, 4 * heads, dvx // 4, DK), F32),
            vm((heads, DV, DK), F32),
            vm((2, 8, own // 2), F32),
            vm((ntp, 2, 8, own // 2), F32),
            dma((2, nx)),
            dma((nx - 1,)),
            dma((nx - 1, 4 * heads)),
            dma((1 if cube else nz,)),
            dma((1 if cube else nz,)),
            dma((nx - 1,)),
            dma((nx - 1,)),
            dma,
            dma((4 * heads,)),
            dma((nx,)),
            dma((nx - 1, 4 * heads)),
            dma,
            dma((ntp - 1,)),
            vm((tokens, wide), F32),
            vm((tokens, wide), BF16),
            *late,
        ],
        compiler_params=pltpu.CompilerParams(
            collective_id=0, has_side_effects=True, vmem_limit_bytes=62 * 1024 * 1024
        ),
    )(block_input, queries, keys, w_value, log_decay, d_out)
    final = pl.pallas_call(
        finish,
        out_shape=tuple(jax.ShapeDtypeStruct(a.shape, a.dtype) for a in out[:4])
        + (jax.ShapeDtypeStruct((2, 1, own // 2), F32),),
        in_specs=[pl.BlockSpec(memory_space=vm)] * 5,
        out_specs=(pl.BlockSpec(memory_space=pltpu.HBM),) * 5,
        scratch_shapes=[dma((5,))],
        compiler_params=pltpu.CompilerParams(vmem_limit_bytes=1024 * 1024),
    )(*out)
    return (*final[:4], final[4].reshape(-1))


def solution(mesh):
    n, ntp = mesh.shape["sp"], mesh.shape["tp"]
    nx = 1 << ((n.bit_length() - 1) // 2)
    placed = (
        P("sp", None),
        P("sp", "tp"),
        P("sp", "tp"),
        P(None, "tp"),
        P("sp", "tp"),
        P("sp", "tp"),
    )
    return jax.shard_map(
        functools.partial(on_device, n, nx, ntp),
        mesh=mesh,
        in_specs=placed,
        out_specs=(P("sp", "tp"), P("sp", "tp"), P("sp", "tp"), P("sp", "tp"), P("sp")),
        check_vma=False,
    )
```

```python
import functools

import jax
import jax.numpy as jnp
from jax import lax
from jax.experimental import pallas as pl
from jax.experimental.pallas import tpu as pltpu
from jax.sharding import PartitionSpec as P

DK = 128
DV = 256
BLOCK = 32
F32 = jnp.float32
BF16 = jnp.bfloat16
MESH = pl.DeviceIdType.MESH


def nn(left, right):
    return lax.dot_general(left, right, (((1,), (0,)), ((), ())), preferred_element_type=F32)


def nt(left, right):
    return lax.dot_general(left, right, (((1,), (1,)), ((), ())), preferred_element_type=F32)


def tn(left, right):
    return lax.dot_general(left, right, (((0,), (0,)), ((), ())), preferred_element_type=F32)


def pieces(value, count):
    parts = []
    for _ in range(count):
        part = value.astype(BF16)
        parts.append(part)
        value = value - part.astype(F32)
    return parts


def ring_place(z, x, nz, nx):
    r = nz - 1 - z
    across = jnp.where(r % 2 == 0, x - 1, nx - 1 - x)
    return jnp.where(x == 0, z, nz + r * (nx - 1) + across)


def ring_member(p, nz, nx):
    u = jnp.maximum(p - nz, 0)
    r = u // (nx - 1)
    w = u % (nx - 1)
    x = jnp.where(r % 2 == 0, 1 + w, nx - 1 - w)
    return jnp.where(p < nz, p * nx, (nz - 1 - r) * nx + x)


def is_cube(n, nx, ntp):
    return nx == 2 and n == 4 * nx and ntp == 2 * nx


def kernel(
    n, nx, ntp,
    x_hbm, q_hbm, k_hbm, w_hbm, g_hbm, o_hbm,
    dq_ref, dk_ref, dg_ref, dw_ref, rn_ref,
    x_ref, q_ref, k_ref, w_ref, g_ref, o_ref, in_sem,
    c_buf, span_buf, v_buf, qg_buf, kt_buf, ks_buf, y_buf, kp_buf, vp_buf, st_buf, xt_buf, vg_buf,
    a_out, a_in, z_out, z_in, z_acc, c_out, c_in, h_out, h_in, b_out, b_in, fr_buf,
    norm_out, norm_in,
    a_send, a_recv, e_recv, z_send, z_recv, c_send, c_recv, h_send, h_recv, b_send, b_recv, n_send, n_recv,
    tail_buf, ksp_buf, *late,
):
    cube = is_cube(n, nx, ntp) and dw_ref.shape[1] == 2 * DV
    if cube:
        (xs_out, xr_in, xr_buf, vx_out, vx_in, vgp_buf, sx_out, sx_in, acc_buf, sm_out, sm_in,
         xs_send, xr_recv, xc_recv, v_send, v_recv, sx_send, sx_recv, sm_send, sm_recv) = late
    else:
        first, part, ring, r_send, r_recv = late
    nz = n // nx
    me = lax.axis_index("sp")
    mine = lax.axis_index("tp")
    z, x = me // nx, me % nx
    tokens, heads = q_ref.shape[0], q_ref.shape[1] // DK
    blocks = tokens // BLOCK
    dvx = DV // nx
    scale = DK ** (-0.5)
    loads = [
        pltpu.make_async_copy(source, target, in_sem.at[i])
        for i, (source, target) in enumerate(
            [(g_hbm, g_ref), (q_hbm, q_ref), (o_hbm, o_ref), (k_hbm, k_ref), (x_hbm, x_ref), (w_hbm, w_ref)]
        )
    ]
    for load in loads[:3]:
        load.start()
    barrier = pltpu.get_barrier_semaphore()
    for off in range(1, nx):
        pl.semaphore_signal(
            barrier, inc=1, device_id={"sp": z * nx + (x + off) % nx}, device_id_type=MESH)
    for off in range(1, nz):
        pl.semaphore_signal(
            barrier, inc=1, device_id={"sp": (z + off) % nz * nx + x}, device_id_type=MESH)
    for off in range(1, ntp):
        pl.semaphore_signal(barrier, inc=1, device_id={"tp": (mine + off) % ntp}, device_id_type=MESH)

    row = lax.broadcasted_iota(jnp.int32, (tokens, tokens), 0)
    col = lax.broadcasted_iota(jnp.int32, (tokens, tokens), 1)
    tri = jnp.where(col <= row, 1.0, 0.0).astype(BF16)

    def inside():
        return (col <= row) & (col // BLOCK == row // BLOCK)

    def hd(h):
        return slice(h * DK, (h + 1) * DK)

    def hv(h):
        return slice(h * DV, (h + 1) * DV)

    def total(h):
        return span_buf[tokens - 1 : tokens, hd(h)]

    quarter = dvx // 4

    def part_rows(part):
        return slice(8 + part * quarter if part else 0, 8 + (part + 1) * quarter)

    def slot(to, frm):
        return (frm + nx - 1 - to) % nx

    def first_part(m, h, part):
        return pltpu.make_async_remote_copy(
            src_ref=a_out.at[1, m, h, part_rows(part), :], dst_ref=a_in.at[1, x, h, part_rows(part), :],
            send_sem=a_send.at[1, m], recv_sem=e_recv.at[slot(m, x), h * 4 + part],
            device_id={"sp": z * nx + m}, device_id_type=MESH)

    def first_wait(h, part):
        for m in range(nx):
            @pl.when(m != x)
            def _():
                pltpu.make_async_remote_copy(
                    src_ref=a_out.at[1, m, h, part_rows(part), :], dst_ref=a_in.at[1, m, h, part_rows(part), :],
                    send_sem=a_send.at[1, m], recv_sem=e_recv.at[slot(x, m), h * 4 + part],
                    device_id={"sp": z * nx + m}, device_id_type=MESH).wait_recv()

    def scatter_copy(d, m):
        return pltpu.make_async_remote_copy(
            src_ref=a_out.at[d, m], dst_ref=a_in.at[d, x],
            send_sem=a_send.at[d, m], recv_sem=a_recv.at[slot(m, x)],
            device_id={"sp": z * nx + m}, device_id_type=MESH)

    def scatter_wait(d):
        for m in range(nx):
            @pl.when(m != x)
            def _():
                pltpu.make_async_remote_copy(
                    src_ref=a_out.at[d, m], dst_ref=a_in.at[d, m],
                    send_sem=a_send.at[d, m], recv_sem=a_recv.at[slot(x, m)],
                    device_id={"sp": z * nx + m}, device_id_type=MESH).wait_recv()

    def give(d, h, totals):
        for m in range(nx):
            a_out[d, m, h, :8, :] = jnp.broadcast_to(jnp.exp(total(h)), (8, DK))
            a_out[d, m, h, 8:, :] = totals[m * dvx : (m + 1) * dvx]
        for m in range(nx):
            @pl.when(m != x)
            def _():
                if d == 1:
                    for part in range(4):
                        first_part(m, h, part).start()
                elif h == heads - 1:
                    scatter_copy(d, m).start()

            @pl.when(m == x)
            def _():
                a_in[d, m, h] = a_out[d, m, h]

    loads[0].wait()
    for i in (4, 5, 3):
        loads[i].start()
    for h in range(heads):
        span = sum(nn(tri, part_) for part_ in pieces(g_ref[:, hd(h)], 3))
        span_buf[:, hd(h)] = span
        if h == 0:
            loads[1].wait()
        q_span = (q_ref[:, hd(h)].astype(F32) * scale * jnp.exp(span)).astype(BF16)
        if h == 0:
            loads[2].wait()
        adjoint = tn(o_ref[:, hv(h)], q_span)
        if h == 0:
            pl.semaphore_wait(barrier, nx - 1 + nz - 1 + ntp - 1)
        give(1, h, adjoint)

    loads[4].wait()
    depth = x_ref.shape[1]
    for at in range(0, depth, 256):
        xt_buf[at : at + 256, :] = x_ref[:, at : at + 256].T

    own = dw_ref.shape[0]
    cols = dw_ref.shape[1]
    wide = min(cols, 128)
    chunks = cols // wide
    half_r = own // 2
    near, mirror = z + 1 - 2 * (z % 2), nz - 1 - z
    core_mate, row_mate = mine + 1 - 2 * (mine % 2), (mine + 2) % 4

    def block_rows(slab, xx, base=0, size=None):
        unit = half_r // 2
        return pl.ds(pl.multiple_of((slab * nx + xx) * own + base, unit), own if size is None else size)

    x_parts = 4
    x_rows = own // x_parts

    def x_copy(p):
        return pltpu.make_async_remote_copy(
            src_ref=xs_out.at[p], dst_ref=xr_in.at[mine, p],
            send_sem=xs_send.at[0], recv_sem=xr_recv.at[4 + p],
            device_id={"sp": near * nx + x}, device_id_type=MESH)

    def x_pass(which, block, p, mate):
        return pltpu.make_async_remote_copy(
            src_ref=xr_in.at[block, p], dst_ref=xr_in.at[block, p],
            send_sem=xs_send.at[which], recv_sem=xr_recv.at[p] if which == 2 else xc_recv.at[which // 2],
            device_id={"tp": mate}, device_id_type=MESH)

    def x_send(p):
        slab = jnp.where(mine < nx, nz - 1 - near, near)
        xs_out[p] = xt_buf[block_rows(slab, mine % nx, p * x_rows, x_rows), :].astype(F32)
        x_copy(p).start()

    def x_relay(p):
        x_copy(p).wait_recv()
        x_pass(2, mine, p, row_mate).start()
        x_pass(1, mine, p, core_mate).start()

    def x_forward():
        for p in range(x_parts):
            x_pass(2, row_mate, p, row_mate).wait_recv()
            x_pass(3, row_mate, p, core_mate).start()

    def x_take():
        far_mate = (core_mate + 2) % 4
        for i, block in enumerate((core_mate, far_mate)):
            pltpu.make_async_remote_copy(
                src_ref=xr_in.at[block], dst_ref=xr_in.at[block],
                send_sem=xs_send.at[1], recv_sem=xc_recv.at[i],
                device_id={"tp": core_mate}, device_id_type=MESH).wait_recv()
        for j in range(2 * nx):
            for p in range(x_parts):
                xr_buf[j, p * x_rows : (p + 1) * x_rows] = xr_in[j, p].astype(BF16)

    if cube:
        x_send(0)

        @pl.when(z < nz - 1)
        def _():
            for p in range(1, x_parts):
                x_send(p)

    loads[3].wait()
    loads[5].wait()

    def value_side(first_head=0, last_head=heads):
        for h in range(first_head, last_head):
            k_far = jnp.exp(total(h) - span_buf[:, hd(h)])
            ksp_buf[:, hd(h)] = (k_ref[:, hd(h)].astype(F32) * k_far).astype(BF16)
            v_buf[:, hv(h)] = nn(x_ref[...], w_ref[:, hv(h)]).astype(BF16)
            give(0, h, tn(v_buf[:, hv(h)], ksp_buf[:, hd(h)]))

    def order(d):
        return range(nx) if d == 0 else range(nx - 1, -1, -1)

    def plane_copy(dz):
        return pltpu.make_async_remote_copy(
            src_ref=z_out, dst_ref=z_in.at[z],
            send_sem=z_send.at[dz], recv_sem=z_recv.at[z],
            device_id={"sp": (z + dz) * nx + x}, device_id_type=MESH)

    def composite(d, h, rows_):
        acc, dec = None, None
        for m in order(d):
            local, rate = a_in[d, m, h, rows_, :], a_in[d, m, h, 0:1, :]
            acc = local if acc is None else local + rate * acc
            dec = rate if dec is None else rate * dec
        return acc, dec

    def forward_start():
        scatter_wait(0)
        for h in range(heads):
            acc, dec = composite(0, h, slice(8, 8 + dvx))
            z_out[h, :dvx, :] = acc
            z_out[h, dvx:, :] = jnp.broadcast_to(dec, (8, DK))
        for dz in range(1, nz):
            @pl.when(z + dz < nz)
            def _():
                plane_copy(dz).start()

    def local_side():
        tri_in = jnp.where(inside(), 1.0, 0.0).astype(BF16)
        g_parts = pieces(g_ref[...], 3)
        q_all = q_ref[...].astype(F32) * scale
        k_all = k_ref[...].astype(F32)
        last_in = jnp.where(col // BLOCK == row // BLOCK, 1.0, 0.0).astype(BF16)
        cum = sum(nn(tri_in, part_) for part_ in g_parts)
        c_buf[...] = cum
        block_end = sum(nn(last_in, part_) for part_ in g_parts)
        k_tail = jnp.exp(block_end - cum)
        tail_buf[...] = k_tail
        grow = jnp.exp(cum)
        qg_buf[...] = (q_all * grow).astype(BF16)
        ks_buf[...] = (k_all * jnp.exp(-cum)).astype(BF16)
        kt_buf[...] = (k_all * k_tail).astype(BF16)
        st_buf[...] = jnp.zeros_like(st_buf)

        def adjoint_step(step, carry):
            rows = pl.ds(pl.multiple_of((blocks - 1 - step) * BLOCK, BLOCK), BLOCK)
            for h in range(heads):
                keep = jnp.exp(c_buf[rows, hd(h)][BLOCK - 1 :])
                adjoint = st_buf[1, h]
                narrow = adjoint.astype(BF16)
                kp_buf[rows, hd(h)] = nn(v_buf[rows, hv(h)], narrow)
                vp_buf[rows, hv(h)] = nt(kt_buf[rows, hd(h)], narrow)
                st_buf[1, h] = keep * adjoint + tn(o_ref[rows, hv(h)], qg_buf[rows, hd(h)])
            return carry

        lax.fori_loop(0, blocks, adjoint_step, 0)

        for h in range(heads):
            dots = jnp.where(inside(), nt(qg_buf[:, hd(h)], ks_buf[:, hd(h)]), 0.0).astype(BF16)
            vp_buf[:, hv(h)] += tn(dots, o_ref[:, hv(h)])

    def state_step(step, carry):
        rows = pl.ds(pl.multiple_of(step * BLOCK, BLOCK), BLOCK)
        for h in range(heads):
            keep = jnp.exp(c_buf[rows, hd(h)][BLOCK - 1 :])
            state = st_buf[0, h]
            y_buf[rows, hd(h)] = nn(o_ref[rows, hv(h)], state.astype(BF16))
            st_buf[0, h] = keep * state + tn(v_buf[rows, hv(h)], kt_buf[rows, hd(h)])
        return carry

    def member_copy(m):
        return pltpu.make_async_remote_copy(
            src_ref=c_out.at[m], dst_ref=c_in.at[x],
            send_sem=c_send.at[slot(x, m)], recv_sem=c_recv.at[slot(m, x)],
            device_id={"sp": z * nx + m}, device_id_type=MESH)

    def forward_spread():
        z_acc[...] = jnp.zeros_like(z_acc)
        for zp in range(nz):
            @pl.when(zp < z)
            def _():
                pltpu.make_async_remote_copy(
                    src_ref=z_out, dst_ref=z_in.at[zp],
                    send_sem=z_send.at[0], recv_sem=z_recv.at[zp],
                    device_id={"sp": zp * nx + x}, device_id_type=MESH).wait_recv()
                for h in range(heads):
                    z_acc[h] = z_in[zp, h, :dvx, :] + z_in[zp, h, dvx : dvx + 1, :] * z_acc[h]
        for h in range(heads):
            acc = z_acc[h]
            for m in order(0):
                c_out[m, h] = acc
                acc = a_in[0, m, h, 8:, :] + a_in[0, m, h, 0:1, :] * acc
        for m in range(nx):
            @pl.when(m != x)
            def _():
                member_copy(m).start()

            @pl.when(m == x)
            def _():
                c_in[m] = c_out[m]

    def step_copy():
        return pltpu.make_async_remote_copy(
            src_ref=z_out, dst_ref=z_in.at[0],
            send_sem=z_send.at[0], recv_sem=z_recv.at[0],
            device_id={"sp": (z + 1) * nx + x}, device_id_type=MESH)

    def forward_step():
        @pl.when(z == 0)
        def _():
            z_acc[...] = jnp.zeros_like(z_acc)

        @pl.when(z > 0)
        def _():
            step_copy().wait_recv()
            for h in range(heads):
                z_acc[h] = z_in[0, h, :dvx, :]

        for h in range(heads):
            acc = z_acc[h]
            for m in order(0):
                c_out[m, h] = acc
                acc = a_in[0, m, h, 8:, :] + a_in[0, m, h, 0:1, :] * acc
            z_out[h, :dvx, :] = acc
            z_out[h, dvx:, :] = jnp.zeros((8, DK), F32)

        @pl.when(z < nz - 1)
        def _():
            step_copy().start()

        for m in range(nx):
            @pl.when(m != x)
            def _():
                member_copy(m).start()

            @pl.when(m == x)
            def _():
                c_in[m] = c_out[m]

    def near_copy(c):
        return pltpu.make_async_remote_copy(
            src_ref=vx_out.at[c], dst_ref=vx_in.at[c],
            send_sem=v_send, recv_sem=v_recv.at[c],
            device_id={"sp": near * nx + x}, device_id_type=MESH)

    def side_copy(c, s, u):
        return pltpu.make_async_remote_copy(
            src_ref=sx_out.at[c, s, u], dst_ref=sx_in.at[c, s, u],
            send_sem=sx_send, recv_sem=sx_recv.at[c, s, u],
            device_id={"sp": z * nx + 1 - x}, device_id_type=MESH)

    def far_copy(c, u):
        return pltpu.make_async_remote_copy(
            src_ref=sm_out.at[c, u], dst_ref=sm_in.at[c, u],
            send_sem=sm_send, recv_sem=sm_recv.at[c, u],
            device_id={"sp": mirror * nx + x}, device_id_type=MESH)

    def emit(h, m):
        c = h * nx + m
        held = b_in[m, 4 * h : 4 * h + 4].reshape(dvx, DK).astype(BF16)
        at = pl.ds(pl.multiple_of(c * wide, wide), wide)
        value = (vp_buf[:, at] + nt(ksp_buf[:, hd(h)], held)).astype(BF16)
        vg_buf[c] = value
        vx_out[c] = value.astype(F32)
        near_copy(c).start()

    def piece(c, s, xx):
        slab = mirror if s == 0 else z
        return nn(xt_buf[block_rows(slab, xx), :], vg_buf[c]) + nn(xr_buf[s * nx + xx], vgp_buf[c])

    def take_near(c):
        near_copy(c).wait_recv()
        vgp_buf[c] = vx_in[c].astype(BF16)

    def side_send(c, s):
        value = piece(c, s, 1 - x)
        for u in range(2):
            sx_out[c, s, u] = value[u * half_r : (u + 1) * half_r]
            side_copy(c, s, u).start()

    def keep(c, s):
        value = piece(c, s, x)
        for u in range(2):
            acc_buf[c, s, u] = value[u * half_r : (u + 1) * half_r]

    def far_send(c):
        for u in range(2):
            side_copy(c, 0, u).wait_recv()
            sm_out[c, u] = acc_buf[c, 0, u] + sx_in[c, 0, u]
            far_copy(c, u).start()

    @pl.when(z < nz - 1)
    def _():
        value_side()
        local_side()

    if cube:
        @pl.when(z < nz - 1)
        def _():
            x_relay(0)

        @pl.when(z < nz - 2)
        def _():
            x_relay(1)

    if not cube:
        @pl.when(z < nz - 2)
        def _():
            forward_start()

    if cube:
        @pl.when(z < nz - 2)
        def _():
            for p in range(2, x_parts):
                x_relay(p)

        @pl.when(z == 0)
        def _():
            scatter_wait(0)
            forward_step()

    @pl.when(z == nz - 1)
    def _():
        value_side(0, 1)

    half_v = dvx // 4

    def chain_copy(c):
        return pltpu.make_async_remote_copy(
            src_ref=h_out.at[c], dst_ref=h_in.at[c],
            send_sem=h_send, recv_sem=h_recv.at[c],
            device_id={"sp": (z - 1) * nx + x}, device_id_type=MESH)

    def piece_copy(m, c):
        return pltpu.make_async_remote_copy(
            src_ref=b_out.at[m, c], dst_ref=b_in.at[x, c],
            send_sem=b_send.at[m], recv_sem=b_recv.at[slot(m, x), c],
            device_id={"sp": z * nx + m}, device_id_type=MESH)

    late_half = z >= nz - 2
    turns = [
        jnp.where(late_half, i, (i // nx) * nx + (x if i % nx == 0 else 1 - x)) for i in range(2 * nx)]
    s0, s1, s2, s3 = turns if cube else (0, 0, 0, 0)

    def open_side():
        x_take()
        take_near(s0)
        side_send(s0, 0)

    def other_slice(h):
        for c in range(4 * h, 4 * (h + 1)):
            pltpu.make_async_remote_copy(
                src_ref=b_out.at[1 - x, c], dst_ref=b_in.at[1 - x, c],
                send_sem=b_send.at[1 - x], recv_sem=b_recv.at[0, c],
                device_id={"sp": z * nx + 1 - x}, device_id_type=MESH).wait_recv()

    for c in range(4 * heads):
        if cube and c == 4:
            @pl.when(z == 0)
            def _():
                open_side()

        if cube and c == 6:
            @pl.when(z == 0)
            def _():
                other_slice(0)
                emit(0, 1 - x)

        h, rows_ = c // 4, slice(8 + c % 4 * half_v, 8 + (c % 4 + 1) * half_v)
        first_wait(h, c % 4)
        acc, dec = composite(1, h, rows_)

        @pl.when(z == nz - 1)
        def _():
            h_in[c] = jnp.zeros((half_v, DK), F32)

        @pl.when(z < nz - 1)
        def _():
            chain_copy(c).wait_recv()

        enter = h_in[c]

        @pl.when(z > 0)
        def _():
            h_out[c] = acc + dec * enter
            chain_copy(c).start()

        for m in order(1):
            b_out[m, c] = enter
            enter = a_in[1, m, h, rows_, :] + a_in[1, m, h, 0:1, :] * enter
        for m in range(nx):
            @pl.when(m != x)
            def _():
                piece_copy(m, c).start()

            @pl.when(m == x)
            def _():
                b_in[m, c] = b_out[m, c]

        if cube and c == 3:
            @pl.when(z < nz - 1)
            def _():
                emit(0, x)

            @pl.when(z == 0)
            def _():
                x_forward()

    if cube:
        @pl.when(z == 0)
        def _():
            emit(1, x)
    else:
        @pl.when(z == nz - 2)
        def _():
            forward_start()

    @pl.when(z == nz - 1)
    def _():
        if cube:
            for p in range(1, x_parts):
                x_send(p)
            x_relay(0)
        value_side(1, heads)
        if cube:
            x_relay(1)
        local_side()
        if cube:
            for p in range(2, x_parts):
                x_relay(p)
        else:
            scatter_wait(0)

    def state_loop():
        lax.fori_loop(0, blocks, state_step, 0)

    if cube:
        @pl.when(z < nz - 1)
        def _():
            state_loop()

        @pl.when((z > 0) & (z < nz - 2))
        def _():
            x_forward()

        @pl.when(z == nz - 2)
        def _():
            for p in range(1, x_parts - 1):
                x_relay(p)

        def keep_pieces():
            for h in range(heads):
                for m in range(nx):
                    fr_buf[h, m * dvx : (m + 1) * dvx, :] = b_in[m, 4 * h : 4 * h + 4].reshape(dvx, DK)

        @pl.when((z > 0) & (z < nz - 1))
        def _():
            other_slice(0)
            emit(0, 1 - x)
            emit(1, x)

            @pl.when(z == nz - 2)
            def _():
                x_relay(x_parts - 1)

            other_slice(1)
            emit(1, 1 - x)
            keep_pieces()

        @pl.when(z == nz - 1)
        def _():
            for h in range(heads):
                other_slice(h)
                for m in range(nx):
                    emit(h, m)
            keep_pieces()

        @pl.when(z == nz - 1)
        def _():
            state_loop()
    else:
        for h in range(heads):
            for m in range(nx):
                for c in range(4 * h, 4 * (h + 1)):
                    @pl.when(m != x)
                    def _():
                        pltpu.make_async_remote_copy(
                            src_ref=b_out.at[m, c], dst_ref=b_in.at[m, c],
                            send_sem=b_send.at[m], recv_sem=b_recv.at[slot(x, m), c],
                            device_id={"sp": z * nx + m}, device_id_type=MESH).wait_recv()
                    at = m * dvx + c % 4 * half_v
                    fr_buf[h, at : at + half_v, :] = b_in[m, c]
            narrow = fr_buf[h].astype(BF16)
            vg_buf[:, hv(h)] = (vp_buf[:, hv(h)] + nt(ksp_buf[:, hd(h)], narrow)).astype(BF16)


    half_c = cols // 2
    p = ring_place(z, x, nz, nx)
    ahead = ring_member((p + 1) % n, nz, nx)
    behind = ring_member((p + n - 1) % n, nz, nx)

    def share(d, u, owner):
        rows_ = pl.ds(pl.multiple_of(owner * own + u * half_r, half_r), half_r)
        return nn(xt_buf[rows_, :], vg_buf[:, d * half_c : (d + 1) * half_c])

    def ring_copy(step, d, u, src):
        return pltpu.make_async_remote_copy(
            src_ref=src, dst_ref=ring.at[step, d, u],
            send_sem=r_send.at[step, d, u], recv_sem=r_recv.at[step, d, u],
            device_id={"sp": ahead if d == 0 else behind}, device_id_type=MESH)

    def owner_at(step, d):
        return ring_member((p + n - step - 1) % n if d == 0 else (p + step + 1) % n, nz, nx)

    if not cube:
        for u in range(2):
            for d in range(2):
                first[d, u] = share(d, u, owner_at(0, d))
                ring_copy(0, d, u, first.at[d, u]).start()

    def key_side():
        for h in range(heads):
            dots = jnp.where(inside(), nt(o_ref[:, hv(h)], v_buf[:, hv(h)]), 0.0).astype(BF16)
            y_buf[:, hd(h)] += nn(dots, ks_buf[:, hd(h)])
            k_grad = (
                tail_buf[:, hd(h)] * kp_buf[:, hd(h)]
                + jnp.exp(-c_buf[:, hd(h)]) * tn(dots, qg_buf[:, hd(h)])
                + jnp.exp(total(h) - span_buf[:, hd(h)]) * nn(v_buf[:, hv(h)], fr_buf[h].astype(BF16))
            )
            kp_buf[:, hd(h)] = k_grad
            dk_ref[:, hd(h)] = k_grad.astype(BF16)

    if not cube:
        state_loop()
        key_side()

    def query_side(first_head=0, last_head=heads):
        for m in range(nx):
            if first_head:
                break

            @pl.when(m != x)
            def _():
                pltpu.make_async_remote_copy(
                    src_ref=c_out.at[m], dst_ref=c_in.at[m],
                    send_sem=c_send.at[slot(x, m)], recv_sem=c_recv.at[slot(x, m)],
                    device_id={"sp": z * nx + m}, device_id_type=MESH).wait_recv()
        upper = jnp.where(col >= row, 1.0, 0.0).astype(BF16)
        for h in range(first_head, last_head):
            state_in = jnp.concatenate([c_in[m, h] for m in range(nx)], axis=0)
            q_side = q_ref[:, hd(h)].astype(F32) * scale
            k_side = k_ref[:, hd(h)].astype(F32)
            q_grad = jnp.exp(c_buf[:, hd(h)]) * y_buf[:, hd(h)] + jnp.exp(span_buf[:, hd(h)]) * nn(
                o_ref[:, hv(h)], state_in.astype(BF16)
            )
            dq_ref[:, hd(h)] = (q_grad * scale).astype(BF16)
            terms = q_side * q_grad - k_side * kp_buf[:, hd(h)]
            far = jnp.exp(span_buf[tokens - 1 : tokens, hd(h)])
            span_end = st_buf[0, h] + far * state_in
            carry = jnp.sum(fr_buf[h] * span_end, axis=0, keepdims=True)
            dg_ref[:, hd(h)] = sum(nn(upper, part_) for part_ in pieces(terms, 3)) + carry

    def ring_step(step, carry):
        for d in range(2):
            for u in range(2):
                part[d, u] = share(d, u, owner_at(step, d))
        for u in range(2):
            for d in range(2):
                ring_copy(step - 1, d, u, first.at[d, u]).wait_recv()
                ring[step - 1, d, u] += part[d, u]
                ring_copy(step, d, u, ring.at[step - 1, d, u]).start()

        @pl.when(step == 2)
        def _():
            forward_spread()

        @pl.when(step == 4)
        def _():
            query_side()

        return carry

    if not cube:
        lax.fori_loop(1, n - 1, ring_step, 0)

        for d in range(2):
            for u in range(2):
                part[d, u] = share(d, u, me)
        for u in range(2):
            squares = 0.0
            for d in range(2):
                ring_copy(n - 2, d, u, first.at[d, u]).wait_recv()
                done = ring[n - 2, d, u] + part[d, u]
                dw_ref[u * half_r : (u + 1) * half_r, d * half_c : (d + 1) * half_c] = done
                for at in range(0, half_c, 128):
                    squares = squares + done[:, at : at + 128] * done[:, at : at + 128]
            norm_out[u] = jnp.broadcast_to(jnp.sum(squares.T, axis=0, keepdims=True), (8, half_r))
    else:
        @pl.when(z >= nz - 2)
        def _():
            x_forward()

        @pl.when((z > 0) & (z < nz - 2))
        def _():
            scatter_wait(0)
            forward_step()

        f0, f1, f2, f3 = [jnp.where(late_half, turns[i], turns[i ^ 1]) for i in range(chunks)]
        @pl.when(z > 0)
        def _():
            open_side()

        @pl.when(z < nz - 1)
        def _():
            keep(s0, 0)

            @pl.when(z > 0)
            def _():
                key_side()

            take_near(s1)
            side_send(s1, 0)
            keep(s1, 0)
            far_send(f0)

            @pl.when(z == 0)
            def _():
                other_slice(1)
                emit(1, 1 - x)
                keep_pieces()
                key_side()

            take_near(s2)
            side_send(s2, 0)

            @pl.when(z == nz - 2)
            def _():
                scatter_wait(0)
                forward_step()

            take_near(s3)
            side_send(s3, 0)
            far_send(f1)
            side_send(s0, 1)
            side_send(s1, 1)
            keep(s2, 0)
            keep(s3, 0)
            far_send(f2)
            side_send(s2, 1)
            side_send(s3, 1)
            far_send(f3)
            for c in range(chunks):
                keep(c, 1)

        @pl.when(z == nz - 1)
        def _():
            for c in (s1, s2, s3):
                take_near(c)
                side_send(c, 0)
            key_side()
            for c in range(chunks):
                keep(c, 0)
                side_send(c, 1)
                keep(c, 1)
            far_send(0)
            far_copy(1 - x, 0).wait_recv()
            for c in range(1, chunks):
                far_send(c)
            scatter_wait(0)
            forward_step()

        query_side(0, heads)
        squares = [0.0, 0.0]
        for c in range(chunks):
            at = slice(c * wide, (c + 1) * wide)
            for u in range(2):
                side_copy(c, 1, u).wait_recv()
                if c < nx and u == 0:
                    @pl.when((z < nz - 1) | (c != 1 - x))
                    def _():
                        far_copy(c, u).wait_recv()
                else:
                    far_copy(c, u).wait_recv()
                done = acc_buf[c, 1, u] + sx_in[c, 1, u] + sm_in[c, u]
                dw_ref[u * half_r : (u + 1) * half_r, at] = done
                squares[u] = squares[u] + done * done
        for u in range(2):
            norm_out[u] = jnp.broadcast_to(jnp.sum(squares[u].T, axis=0, keepdims=True), (8, half_r))

    def norm_copy(off):
        return pltpu.make_async_remote_copy(
            src_ref=norm_out, dst_ref=norm_in.at[off],
            send_sem=n_send, recv_sem=n_recv.at[off - 1],
            device_id={"tp": (mine + off) % ntp}, device_id_type=MESH)

    for off in range(1, ntp):
        norm_copy(off).start()

    for m in range(nx):
        @pl.when(m != x)
        def _():
            for d in range(2):
                pltpu.make_async_remote_copy(
                    src_ref=a_out.at[d, m], dst_ref=a_in.at[d, x],
                    send_sem=a_send.at[d, m], recv_sem=a_recv.at[slot(m, x)],
                    device_id={"sp": z * nx + m}, device_id_type=MESH).wait_send()
            pltpu.make_async_remote_copy(
                src_ref=b_out.at[m], dst_ref=b_in.at[x],
                send_sem=b_send.at[m], recv_sem=b_recv.at[slot(m, x), 0],
                device_id={"sp": z * nx + m}, device_id_type=MESH).wait_send()
            member_copy(m).wait_send()
    if cube:
        @pl.when(z < nz - 1)
        def _():
            step_copy().wait_send()
    else:
        for dz in range(1, nz):
            @pl.when(z + dz < nz)
            def _():
                plane_copy(dz).wait_send()

    @pl.when(z > 0)
    def _():
        pltpu.make_async_remote_copy(
            src_ref=h_out, dst_ref=h_in,
            send_sem=h_send, recv_sem=h_recv.at[0],
            device_id={"sp": (z - 1) * nx + x}, device_id_type=MESH).wait_send()

    if not cube:
        def sent(step, carry):
            for u in range(2):
                for d in range(2):
                    ring_copy(step, d, u, first.at[d, u]).wait_send()
            return carry

        lax.fori_loop(0, n - 1, sent, 0)
    else:
        def all_sent(ref, sem):
            pltpu.make_async_remote_copy(
                src_ref=ref, dst_ref=ref, send_sem=sem, recv_sem=v_recv.at[0],
                device_id={"sp": near * nx + x}, device_id_type=MESH).wait_send()

        all_sent(xs_out, xs_send.at[0])
        all_sent(xr_in.at[mine], xs_send.at[1])
        all_sent(xr_in.at[mine], xs_send.at[2])
        all_sent(xr_in.at[row_mate], xs_send.at[3])
        all_sent(vx_out, v_send)
        all_sent(sx_out, sx_send)
        all_sent(sm_out, sm_send)

    norms = norm_out[...]
    for off in range(1, ntp):
        norm_copy(off).wait_recv()
        norms = norms + norm_in[off]
    rn_ref[...] = norms[:, :1]
    pltpu.make_async_remote_copy(
        src_ref=norm_in.at[pl.ds(1, ntp - 1)], dst_ref=norm_in.at[pl.ds(1, ntp - 1)],
        send_sem=n_send, recv_sem=n_recv.at[0],
        device_id={"tp": (mine + 1) % ntp}, device_id_type=MESH).wait_send()


def finish(*refs):
    sems = refs[10]
    writes = [pltpu.make_async_copy(refs[i], refs[5 + i], sems.at[i]) for i in range(5)]
    for write in writes:
        write.start()
    for write in writes:
        write.wait()


def on_device(n, nx, ntp, block_input, queries, keys, w_value, log_decay, d_out):
    tokens, wide = queries.shape
    heads = wide // DK
    cols = w_value.shape[1]
    depth = block_input.shape[1]
    own = depth // n
    nz = n // nx
    dvx = DV // nx
    vm = pltpu.VMEM
    dma = pltpu.SemaphoreType.DMA
    wide_c = min(cols, 128)
    chunks, half = cols // wide_c, own // 2
    late = [
        vm((2, 2, half, cols // 2), F32),
        vm((2, 2, half, cols // 2), F32),
        vm((n - 1, 2, 2, half, cols // 2), F32),
        dma((n - 1, 2, 2)),
        dma((n - 1, 2, 2)),
    ]
    cube = is_cube(n, nx, ntp) and cols == 2 * DV
    if cube:
        late = [
            vm((4, own // 4, tokens), F32),
            vm((ntp, 4, own // 4, tokens), F32),
            vm((ntp, own, tokens), BF16),
            vm((chunks, tokens, wide_c), F32),
            vm((chunks, tokens, wide_c), F32),
            vm((chunks, tokens, wide_c), BF16),
            vm((chunks, 2, 2, half, wide_c), F32),
            vm((chunks, 2, 2, half, wide_c), F32),
            vm((chunks, 2, 2, half, wide_c), F32),
            vm((chunks, 2, half, wide_c), F32),
            vm((chunks, 2, half, wide_c), F32),
            dma((4,)),
            dma((8,)),
            dma((2,)),
            dma,
            dma((chunks,)),
            dma,
            dma((chunks, 2, 2)),
            dma,
            dma((chunks, 2)),
        ]
    out = pl.pallas_call(
        functools.partial(kernel, n, nx, ntp),
        out_shape=(
            vm((tokens, wide), BF16),
            vm((tokens, wide), BF16),
            vm((tokens, wide), F32),
            vm((own, cols), F32),
            vm((2, 1, own // 2), F32),
        ),
        in_specs=[pl.BlockSpec(memory_space=pltpu.HBM)] * 6,
        out_specs=(pl.BlockSpec(memory_space=vm),) * 5,
        scratch_shapes=[
            vm(block_input.shape, BF16),
            vm(queries.shape, BF16),
            vm(keys.shape, BF16),
            vm(w_value.shape, BF16),
            vm(log_decay.shape, F32),
            vm(d_out.shape, BF16),
            dma((6,)),
            vm((tokens, wide), F32),
            vm((tokens, wide), F32),
            vm((tokens, cols), BF16),
            vm((tokens, wide), BF16),
            vm((tokens, wide), BF16),
            vm((tokens, wide), BF16),
            vm((tokens, wide), F32),
            vm((tokens, wide), F32),
            vm((tokens, cols), F32),
            vm((2, heads, DV, DK), F32),
            vm((depth, tokens), BF16),
            vm((chunks, tokens, wide_c) if cube else (tokens, cols), BF16),
            vm((2, nx, heads, dvx + 8, DK), F32),
            vm((2, nx, heads, dvx + 8, DK), F32),
            vm((heads, dvx + 8, DK), F32),
            vm((nz, heads, dvx + 8, DK), F32),
            vm((heads, dvx, DK), F32),
            vm((nx, heads, dvx, DK), F32),
            vm((nx, heads, dvx, DK), F32),
            vm((4 * heads, dvx // 4, DK), F32),
            vm((4 * heads, dvx // 4, DK), F32),
            vm((nx, 4 * heads, dvx // 4, DK), F32),
            vm((nx, 4 * heads, dvx // 4, DK), F32),
            vm((heads, DV, DK), F32),
            vm((2, 8, own // 2), F32),
            vm((ntp, 2, 8, own // 2), F32),
            dma((2, nx)),
            dma((nx - 1,)),
            dma((nx - 1, 4 * heads)),
            dma((1 if cube else nz,)),
            dma((1 if cube else nz,)),
            dma((nx - 1,)),
            dma((nx - 1,)),
            dma,
            dma((4 * heads,)),
            dma((nx,)),
            dma((nx - 1, 4 * heads)),
            dma,
            dma((ntp - 1,)),
            vm((tokens, wide), F32),
            vm((tokens, wide), BF16),
            *late,
        ],
        compiler_params=pltpu.CompilerParams(
            collective_id=0, has_side_effects=True, vmem_limit_bytes=62 * 1024 * 1024
        ),
    )(block_input, queries, keys, w_value, log_decay, d_out)
    final = pl.pallas_call(
        finish,
        out_shape=tuple(jax.ShapeDtypeStruct(a.shape, a.dtype) for a in out[:4])
        + (jax.ShapeDtypeStruct((2, 1, own // 2), F32),),
        in_specs=[pl.BlockSpec(memory_space=vm)] * 5,
        out_specs=(pl.BlockSpec(memory_space=pltpu.HBM),) * 5,
        scratch_shapes=[dma((5,))],
        compiler_params=pltpu.CompilerParams(vmem_limit_bytes=1024 * 1024),
    )(*out)
    return (*final[:4], final[4].reshape(-1))


def solution(mesh):
    n, ntp = mesh.shape["sp"], mesh.shape["tp"]
    nx = 1 << ((n.bit_length() - 1) // 2)
    placed = (
        P("sp", None),
        P("sp", "tp"),
        P("sp", "tp"),
        P(None, "tp"),
        P("sp", "tp"),
        P("sp", "tp"),
    )
    return jax.shard_map(
        functools.partial(on_device, n, nx, ntp),
        mesh=mesh,
        in_specs=placed,
        out_specs=(P("sp", "tp"), P("sp", "tp"), P("sp", "tp"), P("sp", "tp"), P("sp")),
        check_vma=False,
    )
```

```python
import functools

import jax
import jax.numpy as jnp
from jax import lax
from jax.experimental import pallas as pl
from jax.experimental.pallas import tpu as pltpu
from jax.sharding import PartitionSpec as P

DK = 128
DV = 256
BLOCK = 32
F32 = jnp.float32
BF16 = jnp.bfloat16
MESH = pl.DeviceIdType.MESH


def nn(left, right):
    return lax.dot_general(left, right, (((1,), (0,)), ((), ())), preferred_element_type=F32)


def nt(left, right):
    return lax.dot_general(left, right, (((1,), (1,)), ((), ())), preferred_element_type=F32)


def tn(left, right):
    return lax.dot_general(left, right, (((0,), (0,)), ((), ())), preferred_element_type=F32)


def pieces(value, count):
    parts = []
    for _ in range(count):
        part = value.astype(BF16)
        parts.append(part)
        value = value - part.astype(F32)
    return parts


def ring_place(z, x, nz, nx):
    r = nz - 1 - z
    across = jnp.where(r % 2 == 0, x - 1, nx - 1 - x)
    return jnp.where(x == 0, z, nz + r * (nx - 1) + across)


def ring_member(p, nz, nx):
    u = jnp.maximum(p - nz, 0)
    r = u // (nx - 1)
    w = u % (nx - 1)
    x = jnp.where(r % 2 == 0, 1 + w, nx - 1 - w)
    return jnp.where(p < nz, p * nx, (nz - 1 - r) * nx + x)


def is_cube(n, nx, ntp):
    return nx == 2 and n == 4 * nx and ntp == 2 * nx


def kernel(
    n, nx, ntp,
    x_hbm, q_hbm, k_hbm, w_hbm, g_hbm, o_hbm,
    dq_ref, dk_ref, dg_ref, dw_ref, rn_ref,
    x_ref, q_ref, k_ref, w_ref, g_ref, o_ref, in_sem,
    c_buf, span_buf, v_buf, qg_buf, kt_buf, ks_buf, y_buf, kp_buf, vp_buf, st_buf, xt_buf, vg_buf,
    a_out, a_in, z_out, z_in, z_acc, c_out, c_in, h_out, h_in, b_out, b_in, fr_buf,
    norm_out, norm_in,
    a_send, a_recv, e_recv, z_send, z_recv, c_send, c_recv, h_send, h_recv, b_send, b_recv, n_send, n_recv,
    tail_buf, ksp_buf, *late,
):
    cube = is_cube(n, nx, ntp) and dw_ref.shape[1] == 2 * DV
    if cube:
        (xs_out, xr_in, xr_buf, vx_out, vx_in, vgp_buf, sx_out, sx_in, acc_buf, sm_out, sm_in,
         xs_send, xr_recv, xc_recv, v_send, v_recv, sx_send, sx_recv, sb_recv, sm_send, sm_recv) = late
    else:
        first, part, ring, r_send, r_recv = late
    nz = n // nx
    me = lax.axis_index("sp")
    mine = lax.axis_index("tp")
    z, x = me // nx, me % nx
    tokens, heads = q_ref.shape[0], q_ref.shape[1] // DK
    blocks = tokens // BLOCK
    dvx = DV // nx
    scale = DK ** (-0.5)
    loads = [
        pltpu.make_async_copy(source, target, in_sem.at[i])
        for i, (source, target) in enumerate(
            [(g_hbm, g_ref), (q_hbm, q_ref), (o_hbm, o_ref), (k_hbm, k_ref), (x_hbm, x_ref), (w_hbm, w_ref)]
        )
    ]
    for load in loads[:3]:
        load.start()
    barrier = pltpu.get_barrier_semaphore()
    for off in range(1, nx):
        pl.semaphore_signal(
            barrier, inc=1, device_id={"sp": z * nx + (x + off) % nx}, device_id_type=MESH)
    for off in range(1, nz):
        pl.semaphore_signal(
            barrier, inc=1, device_id={"sp": (z + off) % nz * nx + x}, device_id_type=MESH)
    for off in range(1, ntp):
        pl.semaphore_signal(barrier, inc=1, device_id={"tp": (mine + off) % ntp}, device_id_type=MESH)

    row = lax.broadcasted_iota(jnp.int32, (tokens, tokens), 0)
    col = lax.broadcasted_iota(jnp.int32, (tokens, tokens), 1)
    tri = jnp.where(col <= row, 1.0, 0.0).astype(BF16)

    def inside():
        return (col <= row) & (col // BLOCK == row // BLOCK)

    def hd(h):
        return slice(h * DK, (h + 1) * DK)

    def hv(h):
        return slice(h * DV, (h + 1) * DV)

    def total(h):
        return span_buf[tokens - 1 : tokens, hd(h)]

    quarter = dvx // 4

    def part_rows(part):
        return slice(8 + part * quarter if part else 0, 8 + (part + 1) * quarter)

    def slot(to, frm):
        return (frm + nx - 1 - to) % nx

    def first_part(m, h, part):
        return pltpu.make_async_remote_copy(
            src_ref=a_out.at[1, m, h, part_rows(part), :], dst_ref=a_in.at[1, x, h, part_rows(part), :],
            send_sem=a_send.at[1, m], recv_sem=e_recv.at[slot(m, x), h * 4 + part],
            device_id={"sp": z * nx + m}, device_id_type=MESH)

    def first_wait(h, part):
        for m in range(nx):
            @pl.when(m != x)
            def _():
                pltpu.make_async_remote_copy(
                    src_ref=a_out.at[1, m, h, part_rows(part), :], dst_ref=a_in.at[1, m, h, part_rows(part), :],
                    send_sem=a_send.at[1, m], recv_sem=e_recv.at[slot(x, m), h * 4 + part],
                    device_id={"sp": z * nx + m}, device_id_type=MESH).wait_recv()

    def scatter_copy(d, m):
        return pltpu.make_async_remote_copy(
            src_ref=a_out.at[d, m], dst_ref=a_in.at[d, x],
            send_sem=a_send.at[d, m], recv_sem=a_recv.at[slot(m, x)],
            device_id={"sp": z * nx + m}, device_id_type=MESH)

    def scatter_wait(d):
        for m in range(nx):
            @pl.when(m != x)
            def _():
                pltpu.make_async_remote_copy(
                    src_ref=a_out.at[d, m], dst_ref=a_in.at[d, m],
                    send_sem=a_send.at[d, m], recv_sem=a_recv.at[slot(x, m)],
                    device_id={"sp": z * nx + m}, device_id_type=MESH).wait_recv()

    def give(d, h, totals):
        for m in range(nx):
            a_out[d, m, h, :8, :] = jnp.broadcast_to(jnp.exp(total(h)), (8, DK))
            a_out[d, m, h, 8:, :] = totals[m * dvx : (m + 1) * dvx]
        for m in range(nx):
            @pl.when(m != x)
            def _():
                if d == 1:
                    for part in range(4):
                        first_part(m, h, part).start()
                elif h == heads - 1:
                    scatter_copy(d, m).start()

            @pl.when(m == x)
            def _():
                a_in[d, m, h] = a_out[d, m, h]

    loads[0].wait()
    for i in (4, 5, 3):
        loads[i].start()
    for h in range(heads):
        span = sum(nn(tri, part_) for part_ in pieces(g_ref[:, hd(h)], 3))
        span_buf[:, hd(h)] = span
        if h == 0:
            loads[1].wait()
        q_span = (q_ref[:, hd(h)].astype(F32) * scale * jnp.exp(span)).astype(BF16)
        if h == 0:
            loads[2].wait()
        adjoint = tn(o_ref[:, hv(h)], q_span)
        if h == 0:
            pl.semaphore_wait(barrier, nx - 1 + nz - 1 + ntp - 1)
        give(1, h, adjoint)

    loads[4].wait()
    depth = x_ref.shape[1]
    for at in range(0, depth, 256):
        xt_buf[at : at + 256, :] = x_ref[:, at : at + 256].T

    own = dw_ref.shape[0]
    cols = dw_ref.shape[1]
    wide = min(cols, 128)
    chunks = cols // wide
    half_r = own // 2
    near, mirror = z + 1 - 2 * (z % 2), nz - 1 - z
    core_mate, row_mate = mine + 1 - 2 * (mine % 2), (mine + 2) % 4

    def block_rows(slab, xx, base=0, size=None):
        unit = half_r // 2
        return pl.ds(pl.multiple_of((slab * nx + xx) * own + base, unit), own if size is None else size)

    x_parts = 4
    x_rows = own // x_parts

    def x_copy(p):
        return pltpu.make_async_remote_copy(
            src_ref=xs_out.at[p], dst_ref=xr_in.at[p, mine],
            send_sem=xs_send.at[0], recv_sem=xr_recv.at[4 + p],
            device_id={"sp": near * nx + x}, device_id_type=MESH)

    def x_pass(which, quart, p, mate):
        return pltpu.make_async_remote_copy(
            src_ref=xr_in.at[p, quart], dst_ref=xr_in.at[p, quart],
            send_sem=xs_send.at[which],
            recv_sem=xr_recv.at[p] if which == 2 else xc_recv.at[which // 2, p // nx],
            device_id={"tp": mate}, device_id_type=MESH)

    def x_send(p):
        slab = nz - 1 - near if p < nx else near
        xs_out[p] = xt_buf[block_rows(slab, p % nx, mine * x_rows, x_rows), :].astype(F32)
        x_copy(p).start()

    def x_relay(p):
        x_copy(p).wait_recv()
        x_pass(2, mine, p, row_mate).start()
        x_pass(1, mine, p, core_mate).start()

    def x_forward(first_part=0, last_part=4):
        for p in range(first_part, last_part):
            x_pass(2, row_mate, p, row_mate).wait_recv()
            x_pass(3, row_mate, p, core_mate).start()

    def x_take(part):
        for i in range(2):
            pltpu.make_async_remote_copy(
                src_ref=xr_in.at[nx * part, pl.ds(0, nx)], dst_ref=xr_in.at[nx * part, pl.ds(0, nx)],
                send_sem=xs_send.at[1], recv_sem=xc_recv.at[i, part],
                device_id={"tp": core_mate}, device_id_type=MESH).wait_recv()
        for j in range(nx * part, nx * (part + 1)):
            for p in range(x_parts):
                xr_buf[j, p * x_rows : (p + 1) * x_rows] = xr_in[j, p].astype(BF16)

    if cube:
        x_send(0)

        @pl.when(z < nz - 1)
        def _():
            for p in range(1, x_parts):
                x_send(p)

    loads[3].wait()
    loads[5].wait()

    def value_side(first_head=0, last_head=heads):
        for h in range(first_head, last_head):
            k_far = jnp.exp(total(h) - span_buf[:, hd(h)])
            ksp_buf[:, hd(h)] = (k_ref[:, hd(h)].astype(F32) * k_far).astype(BF16)
            v_buf[:, hv(h)] = nn(x_ref[...], w_ref[:, hv(h)]).astype(BF16)
            give(0, h, tn(v_buf[:, hv(h)], ksp_buf[:, hd(h)]))

    def order(d):
        return range(nx) if d == 0 else range(nx - 1, -1, -1)

    def plane_copy(dz):
        return pltpu.make_async_remote_copy(
            src_ref=z_out, dst_ref=z_in.at[z],
            send_sem=z_send.at[dz], recv_sem=z_recv.at[z],
            device_id={"sp": (z + dz) * nx + x}, device_id_type=MESH)

    def composite(d, h, rows_):
        acc, dec = None, None
        for m in order(d):
            local, rate = a_in[d, m, h, rows_, :], a_in[d, m, h, 0:1, :]
            acc = local if acc is None else local + rate * acc
            dec = rate if dec is None else rate * dec
        return acc, dec

    def forward_start():
        scatter_wait(0)
        for h in range(heads):
            acc, dec = composite(0, h, slice(8, 8 + dvx))
            z_out[h, :dvx, :] = acc
            z_out[h, dvx:, :] = jnp.broadcast_to(dec, (8, DK))
        for dz in range(1, nz):
            @pl.when(z + dz < nz)
            def _():
                plane_copy(dz).start()

    def local_side():
        tri_in = jnp.where(inside(), 1.0, 0.0).astype(BF16)
        g_parts = pieces(g_ref[...], 3)
        q_all = q_ref[...].astype(F32) * scale
        k_all = k_ref[...].astype(F32)
        last_in = jnp.where(col // BLOCK == row // BLOCK, 1.0, 0.0).astype(BF16)
        cum = sum(nn(tri_in, part_) for part_ in g_parts)
        c_buf[...] = cum
        block_end = sum(nn(last_in, part_) for part_ in g_parts)
        k_tail = jnp.exp(block_end - cum)
        tail_buf[...] = k_tail
        grow = jnp.exp(cum)
        qg_buf[...] = (q_all * grow).astype(BF16)
        ks_buf[...] = (k_all * jnp.exp(-cum)).astype(BF16)
        kt_buf[...] = (k_all * k_tail).astype(BF16)
        st_buf[...] = jnp.zeros_like(st_buf)

        def adjoint_step(step, carry):
            rows = pl.ds(pl.multiple_of((blocks - 1 - step) * BLOCK, BLOCK), BLOCK)
            for h in range(heads):
                keep = jnp.exp(c_buf[rows, hd(h)][BLOCK - 1 :])
                adjoint = st_buf[1, h]
                narrow = adjoint.astype(BF16)
                kp_buf[rows, hd(h)] = nn(v_buf[rows, hv(h)], narrow)
                vp_buf[rows, hv(h)] = nt(kt_buf[rows, hd(h)], narrow)
                st_buf[1, h] = keep * adjoint + tn(o_ref[rows, hv(h)], qg_buf[rows, hd(h)])
            return carry

        lax.fori_loop(0, blocks, adjoint_step, 0)

        for h in range(heads):
            dots = jnp.where(inside(), nt(qg_buf[:, hd(h)], ks_buf[:, hd(h)]), 0.0).astype(BF16)
            vp_buf[:, hv(h)] += tn(dots, o_ref[:, hv(h)])

    def state_step(step, carry):
        rows = pl.ds(pl.multiple_of(step * BLOCK, BLOCK), BLOCK)
        for h in range(heads):
            keep = jnp.exp(c_buf[rows, hd(h)][BLOCK - 1 :])
            state = st_buf[0, h]
            y_buf[rows, hd(h)] = nn(o_ref[rows, hv(h)], state.astype(BF16))
            st_buf[0, h] = keep * state + tn(v_buf[rows, hv(h)], kt_buf[rows, hd(h)])
        return carry

    def member_copy(m):
        return pltpu.make_async_remote_copy(
            src_ref=c_out.at[m], dst_ref=c_in.at[x],
            send_sem=c_send.at[slot(x, m)], recv_sem=c_recv.at[slot(m, x)],
            device_id={"sp": z * nx + m}, device_id_type=MESH)

    def forward_spread():
        z_acc[...] = jnp.zeros_like(z_acc)
        for zp in range(nz):
            @pl.when(zp < z)
            def _():
                pltpu.make_async_remote_copy(
                    src_ref=z_out, dst_ref=z_in.at[zp],
                    send_sem=z_send.at[0], recv_sem=z_recv.at[zp],
                    device_id={"sp": zp * nx + x}, device_id_type=MESH).wait_recv()
                for h in range(heads):
                    z_acc[h] = z_in[zp, h, :dvx, :] + z_in[zp, h, dvx : dvx + 1, :] * z_acc[h]
        for h in range(heads):
            acc = z_acc[h]
            for m in order(0):
                c_out[m, h] = acc
                acc = a_in[0, m, h, 8:, :] + a_in[0, m, h, 0:1, :] * acc
        for m in range(nx):
            @pl.when(m != x)
            def _():
                member_copy(m).start()

            @pl.when(m == x)
            def _():
                c_in[m] = c_out[m]

    def step_copy():
        return pltpu.make_async_remote_copy(
            src_ref=z_out, dst_ref=z_in.at[0],
            send_sem=z_send.at[0], recv_sem=z_recv.at[0],
            device_id={"sp": (z + 1) * nx + x}, device_id_type=MESH)

    def forward_step():
        @pl.when(z == 0)
        def _():
            z_acc[...] = jnp.zeros_like(z_acc)

        @pl.when(z > 0)
        def _():
            step_copy().wait_recv()
            for h in range(heads):
                z_acc[h] = z_in[0, h, :dvx, :]

        for h in range(heads):
            acc = z_acc[h]
            for m in order(0):
                c_out[m, h] = acc
                acc = a_in[0, m, h, 8:, :] + a_in[0, m, h, 0:1, :] * acc
            z_out[h, :dvx, :] = acc
            z_out[h, dvx:, :] = jnp.zeros((8, DK), F32)

        @pl.when(z < nz - 1)
        def _():
            step_copy().start()

        for m in range(nx):
            @pl.when(m != x)
            def _():
                member_copy(m).start()

            @pl.when(m == x)
            def _():
                c_in[m] = c_out[m]

    def near_copy(c):
        return pltpu.make_async_remote_copy(
            src_ref=vx_out.at[c], dst_ref=vx_in.at[c],
            send_sem=v_send, recv_sem=v_recv.at[c],
            device_id={"sp": near * nx + x}, device_id_type=MESH)

    def side_copy(c, s, u):
        return pltpu.make_async_remote_copy(
            src_ref=sx_out.at[c, s, u], dst_ref=sx_in.at[c, s, u],
            send_sem=sx_send, recv_sem=sx_recv.at[c, u] if s == 0 else sb_recv,
            device_id={"sp": z * nx + 1 - x}, device_id_type=MESH)

    def far_copy(c, u):
        return pltpu.make_async_remote_copy(
            src_ref=sm_out.at[c, u], dst_ref=sm_in.at[c, u],
            send_sem=sm_send, recv_sem=sm_recv.at[c],
            device_id={"sp": mirror * nx + x}, device_id_type=MESH)

    def emit(h, m):
        c = h * nx + m
        held = b_in[m, 4 * h : 4 * h + 4].reshape(dvx, DK).astype(BF16)
        at = pl.ds(pl.multiple_of(c * wide, wide), wide)
        value = (vp_buf[:, at] + nt(ksp_buf[:, hd(h)], held)).astype(BF16)
        vg_buf[c] = value
        vx_out[c] = value.astype(F32)
        near_copy(c).start()

    def far_take(c):
        pltpu.make_async_remote_copy(
            src_ref=sm_in.at[c], dst_ref=sm_in.at[c],
            send_sem=sm_send, recv_sem=sm_recv.at[c],
            device_id={"sp": mirror * nx + x}, device_id_type=MESH).wait_recv()

    def piece(c, s, xx):
        slab = mirror if s == 0 else z
        return nn(xt_buf[block_rows(slab, xx), :], vg_buf[c]) + nn(xr_buf[s * nx + xx], vgp_buf[c])

    def take_near(c):
        near_copy(c).wait_recv()
        vgp_buf[c] = vx_in[c].astype(BF16)

    def side_send(c, s):
        value = piece(c, s, 1 - x)
        for u in range(2):
            sx_out[c, s, u] = value[u * half_r : (u + 1) * half_r]
            side_copy(c, s, u).start()

    def keep(c, s):
        value = piece(c, s, x)
        for u in range(2):
            acc_buf[c, s, u] = value[u * half_r : (u + 1) * half_r]

    def far_send(c):
        for u in range(2):
            side_copy(c, 0, u).wait_recv()
            sm_out[c, u] = acc_buf[c, 0, u] + sx_in[c, 0, u]
            far_copy(c, u).start()

    @pl.when(z < nz - 1)
    def _():
        value_side()
        local_side()

    if cube:
        @pl.when(z < nz - 1)
        def _():
            x_relay(0)

        @pl.when(z < nz - 2)
        def _():
            x_relay(1)

    if not cube:
        @pl.when(z < nz - 2)
        def _():
            forward_start()

    if cube:
        @pl.when(z < nz - 2)
        def _():
            for p in range(2, x_parts):
                x_relay(p)

        @pl.when(z == 0)
        def _():
            scatter_wait(0)
            forward_step()

    @pl.when(z == nz - 1)
    def _():
        value_side(0, 1)

    half_v = dvx // 4

    def chain_copy(c):
        return pltpu.make_async_remote_copy(
            src_ref=h_out.at[c], dst_ref=h_in.at[c],
            send_sem=h_send, recv_sem=h_recv.at[c],
            device_id={"sp": (z - 1) * nx + x}, device_id_type=MESH)

    def piece_copy(m, c):
        return pltpu.make_async_remote_copy(
            src_ref=b_out.at[m, c], dst_ref=b_in.at[x, c],
            send_sem=b_send.at[m], recv_sem=b_recv.at[slot(m, x), c // 4],
            device_id={"sp": z * nx + m}, device_id_type=MESH)

    late_half = z >= nz - 2
    turns = [
        jnp.where(late_half, i, (i // nx) * nx + (x if i % nx == 0 else 1 - x)) for i in range(2 * nx)]
    s0, s1, s2, s3 = turns if cube else (0, 0, 0, 0)

    def open_side():
        x_take(0)
        take_near(s0)
        side_send(s0, 0)

    def other_slice(h):
        part = pl.ds(4 * h, 4)
        pltpu.make_async_remote_copy(
            src_ref=b_out.at[1 - x, part], dst_ref=b_in.at[1 - x, part],
            send_sem=b_send.at[1 - x], recv_sem=b_recv.at[0, h],
            device_id={"sp": z * nx + 1 - x}, device_id_type=MESH).wait_recv()

    for c in range(4 * heads):
        if cube and c == 4:
            @pl.when(z == 0)
            def _():
                open_side()

        if cube and c == 6:
            @pl.when(z == 0)
            def _():
                other_slice(0)
                emit(0, 1 - x)

        h, rows_ = c // 4, slice(8 + c % 4 * half_v, 8 + (c % 4 + 1) * half_v)
        first_wait(h, c % 4)
        acc, dec = composite(1, h, rows_)

        @pl.when(z == nz - 1)
        def _():
            h_in[c] = jnp.zeros((half_v, DK), F32)

        @pl.when(z < nz - 1)
        def _():
            chain_copy(c).wait_recv()

        enter = h_in[c]

        @pl.when(z > 0)
        def _():
            h_out[c] = acc + dec * enter
            chain_copy(c).start()

        for m in order(1):
            b_out[m, c] = enter
            enter = a_in[1, m, h, rows_, :] + a_in[1, m, h, 0:1, :] * enter
        for m in range(nx):
            @pl.when(m != x)
            def _():
                piece_copy(m, c).start()

            @pl.when(m == x)
            def _():
                b_in[m, c] = b_out[m, c]

        if cube and c == 3:
            @pl.when(z < nz - 1)
            def _():
                emit(0, x)

            @pl.when(z == 0)
            def _():
                x_forward()

    if cube:
        @pl.when(z == 0)
        def _():
            emit(1, x)
    else:
        @pl.when(z == nz - 2)
        def _():
            forward_start()

    @pl.when(z == nz - 1)
    def _():
        if cube:
            for p in range(1, x_parts):
                x_send(p)
            x_relay(0)
        value_side(1, heads)
        if cube:
            x_relay(1)
        local_side()
        if cube:
            for p in range(2, x_parts):
                x_relay(p)
        else:
            scatter_wait(0)

    def state_loop():
        lax.fori_loop(0, blocks, state_step, 0)

    if cube:
        @pl.when(z < nz - 1)
        def _():
            state_loop()

        @pl.when((z > 0) & (z < nz - 2))
        def _():
            x_forward()

        @pl.when(z == nz - 2)
        def _():
            for p in range(1, x_parts - 1):
                x_relay(p)

        def keep_pieces():
            for h in range(heads):
                for m in range(nx):
                    fr_buf[h, m * dvx : (m + 1) * dvx, :] = b_in[m, 4 * h : 4 * h + 4].reshape(dvx, DK)

        @pl.when((z > 0) & (z < nz - 1))
        def _():
            other_slice(0)
            emit(0, 1 - x)
            emit(1, x)

            @pl.when(z == nz - 2)
            def _():
                x_relay(x_parts - 1)

            other_slice(1)
            emit(1, 1 - x)
            keep_pieces()

        @pl.when(z == nz - 1)
        def _():
            for h in range(heads):
                other_slice(h)
                for m in range(nx):
                    emit(h, m)
            keep_pieces()

        @pl.when(z == nz - 1)
        def _():
            state_loop()
    else:
        for h in range(heads):
            for m in range(nx):
                @pl.when(m != x)
                def _():
                    pltpu.make_async_remote_copy(
                        src_ref=b_out.at[m, pl.ds(4 * h, 4)], dst_ref=b_in.at[m, pl.ds(4 * h, 4)],
                        send_sem=b_send.at[m], recv_sem=b_recv.at[slot(x, m), h],
                        device_id={"sp": z * nx + m}, device_id_type=MESH).wait_recv()
                fr_buf[h, m * dvx : (m + 1) * dvx, :] = b_in[m, 4 * h : 4 * h + 4].reshape(dvx, DK)
            narrow = fr_buf[h].astype(BF16)
            vg_buf[:, hv(h)] = (vp_buf[:, hv(h)] + nt(ksp_buf[:, hd(h)], narrow)).astype(BF16)


    half_c = cols // 2
    p = ring_place(z, x, nz, nx)
    ahead = ring_member((p + 1) % n, nz, nx)
    behind = ring_member((p + n - 1) % n, nz, nx)

    def share(d, u, owner):
        rows_ = pl.ds(pl.multiple_of(owner * own + u * half_r, half_r), half_r)
        return nn(xt_buf[rows_, :], vg_buf[:, d * half_c : (d + 1) * half_c])

    def ring_copy(step, d, u, src):
        return pltpu.make_async_remote_copy(
            src_ref=src, dst_ref=ring.at[step, d, u],
            send_sem=r_send.at[step, d, u], recv_sem=r_recv.at[step, d, u],
            device_id={"sp": ahead if d == 0 else behind}, device_id_type=MESH)

    def owner_at(step, d):
        return ring_member((p + n - step - 1) % n if d == 0 else (p + step + 1) % n, nz, nx)

    if not cube:
        for u in range(2):
            for d in range(2):
                first[d, u] = share(d, u, owner_at(0, d))
                ring_copy(0, d, u, first.at[d, u]).start()

    def key_side():
        for h in range(heads):
            dots = jnp.where(inside(), nt(o_ref[:, hv(h)], v_buf[:, hv(h)]), 0.0).astype(BF16)
            y_buf[:, hd(h)] += nn(dots, ks_buf[:, hd(h)])
            k_grad = (
                tail_buf[:, hd(h)] * kp_buf[:, hd(h)]
                + jnp.exp(-c_buf[:, hd(h)]) * tn(dots, qg_buf[:, hd(h)])
                + jnp.exp(total(h) - span_buf[:, hd(h)]) * nn(v_buf[:, hv(h)], fr_buf[h].astype(BF16))
            )
            kp_buf[:, hd(h)] = k_grad
            dk_ref[:, hd(h)] = k_grad.astype(BF16)

    if not cube:
        state_loop()
        key_side()

    def query_side(first_head=0, last_head=heads):
        for m in range(nx):
            if first_head:
                break

            @pl.when(m != x)
            def _():
                pltpu.make_async_remote_copy(
                    src_ref=c_out.at[m], dst_ref=c_in.at[m],
                    send_sem=c_send.at[slot(x, m)], recv_sem=c_recv.at[slot(x, m)],
                    device_id={"sp": z * nx + m}, device_id_type=MESH).wait_recv()
        upper = jnp.where(col >= row, 1.0, 0.0).astype(BF16)
        for h in range(first_head, last_head):
            state_in = jnp.concatenate([c_in[m, h] for m in range(nx)], axis=0)
            q_side = q_ref[:, hd(h)].astype(F32) * scale
            k_side = k_ref[:, hd(h)].astype(F32)
            q_grad = jnp.exp(c_buf[:, hd(h)]) * y_buf[:, hd(h)] + jnp.exp(span_buf[:, hd(h)]) * nn(
                o_ref[:, hv(h)], state_in.astype(BF16)
            )
            dq_ref[:, hd(h)] = (q_grad * scale).astype(BF16)
            terms = q_side * q_grad - k_side * kp_buf[:, hd(h)]
            far = jnp.exp(span_buf[tokens - 1 : tokens, hd(h)])
            span_end = st_buf[0, h] + far * state_in
            carry = jnp.sum(fr_buf[h] * span_end, axis=0, keepdims=True)
            dg_ref[:, hd(h)] = sum(nn(upper, part_) for part_ in pieces(terms, 3)) + carry

    def ring_step(step, carry):
        for d in range(2):
            for u in range(2):
                part[d, u] = share(d, u, owner_at(step, d))
        for u in range(2):
            for d in range(2):
                ring_copy(step - 1, d, u, first.at[d, u]).wait_recv()
                ring[step - 1, d, u] += part[d, u]
                ring_copy(step, d, u, ring.at[step - 1, d, u]).start()

        @pl.when(step == 2)
        def _():
            forward_spread()

        @pl.when(step == 4)
        def _():
            query_side()

        return carry

    if not cube:
        lax.fori_loop(1, n - 1, ring_step, 0)

        for d in range(2):
            for u in range(2):
                part[d, u] = share(d, u, me)
        for u in range(2):
            squares = 0.0
            for d in range(2):
                ring_copy(n - 2, d, u, first.at[d, u]).wait_recv()
                done = ring[n - 2, d, u] + part[d, u]
                dw_ref[u * half_r : (u + 1) * half_r, d * half_c : (d + 1) * half_c] = done
                for at in range(0, half_c, 128):
                    squares = squares + done[:, at : at + 128] * done[:, at : at + 128]
            norm_out[u] = jnp.broadcast_to(jnp.sum(squares.T, axis=0, keepdims=True), (8, half_r))
    else:
        @pl.when(z >= nz - 2)
        def _():
            x_forward(0, 2)

        @pl.when((z > 0) & (z < nz - 2))
        def _():
            scatter_wait(0)
            forward_step()

        f0, f1, f2, f3 = [jnp.where(late_half, turns[i], turns[i ^ 1]) for i in range(chunks)]
        @pl.when(z > 0)
        def _():
            open_side()

        @pl.when(z < nz - 1)
        def _():
            keep(s0, 0)

            @pl.when(z > 0)
            def _():
                key_side()

            take_near(s1)
            side_send(s1, 0)
            keep(s1, 0)
            far_send(f0)

            @pl.when(z == 0)
            def _():
                other_slice(1)
                emit(1, 1 - x)
                keep_pieces()
                key_side()

            @pl.when(z == nz - 2)
            def _():
                x_forward(2, 4)

            take_near(s2)
            side_send(s2, 0)

            @pl.when(z == nz - 2)
            def _():
                scatter_wait(0)
                forward_step()

            take_near(s3)
            side_send(s3, 0)
            far_send(f1)
            x_take(1)
            side_send(s0, 1)
            side_send(s1, 1)
            keep(s2, 0)
            keep(s3, 0)
            far_send(f2)
            side_send(s2, 1)
            side_send(s3, 1)
            far_send(f3)
            for c in range(chunks):
                keep(c, 1)

        @pl.when(z == nz - 1)
        def _():
            for c in (s1, s2, s3):
                take_near(c)
                side_send(c, 0)
            x_forward(2, 4)
            key_side()
            x_take(1)
            for c in range(chunks):
                keep(c, 0)
                side_send(c, 1)
                keep(c, 1)
            far_send(0)
            far_take(1 - x)
            for c in range(1, chunks):
                far_send(c)
            scatter_wait(0)
            forward_step()

        query_side(0, heads)
        squares = [0.0, 0.0]
        pltpu.make_async_remote_copy(
            src_ref=sm_in, dst_ref=sm_in, send_sem=sx_send, recv_sem=sb_recv,
            device_id={"sp": z * nx + 1 - x}, device_id_type=MESH).wait_recv()
        for c in range(chunks):
            at = slice(c * wide, (c + 1) * wide)
            if c < nx:
                @pl.when((z < nz - 1) | (c != 1 - x))
                def _():
                    far_take(c)
            else:
                far_take(c)
            for u in range(2):
                done = acc_buf[c, 1, u] + sx_in[c, 1, u] + sm_in[c, u]
                dw_ref[u * half_r : (u + 1) * half_r, at] = done
                squares[u] = squares[u] + done * done
        for u in range(2):
            norm_out[u] = jnp.broadcast_to(jnp.sum(squares[u].T, axis=0, keepdims=True), (8, half_r))

    def norm_copy(off):
        return pltpu.make_async_remote_copy(
            src_ref=norm_out, dst_ref=norm_in.at[off],
            send_sem=n_send, recv_sem=n_recv.at[off - 1],
            device_id={"tp": (mine + off) % ntp}, device_id_type=MESH)

    for off in range(1, ntp):
        norm_copy(off).start()

    for m in range(nx):
        @pl.when(m != x)
        def _():
            for d in range(2):
                pltpu.make_async_remote_copy(
                    src_ref=a_out.at[d, m], dst_ref=a_in.at[d, x],
                    send_sem=a_send.at[d, m], recv_sem=a_recv.at[slot(m, x)],
                    device_id={"sp": z * nx + m}, device_id_type=MESH).wait_send()
            pltpu.make_async_remote_copy(
                src_ref=b_out.at[m], dst_ref=b_in.at[x],
                send_sem=b_send.at[m], recv_sem=b_recv.at[slot(m, x), 0],
                device_id={"sp": z * nx + m}, device_id_type=MESH).wait_send()
            member_copy(m).wait_send()
    if cube:
        @pl.when(z < nz - 1)
        def _():
            step_copy().wait_send()
    else:
        for dz in range(1, nz):
            @pl.when(z + dz < nz)
            def _():
                plane_copy(dz).wait_send()

    @pl.when(z > 0)
    def _():
        pltpu.make_async_remote_copy(
            src_ref=h_out, dst_ref=h_in,
            send_sem=h_send, recv_sem=h_recv.at[0],
            device_id={"sp": (z - 1) * nx + x}, device_id_type=MESH).wait_send()

    if not cube:
        def sent(step, carry):
            for u in range(2):
                for d in range(2):
                    ring_copy(step, d, u, first.at[d, u]).wait_send()
            return carry

        lax.fori_loop(0, n - 1, sent, 0)
    else:
        def all_sent(ref, sem):
            pltpu.make_async_remote_copy(
                src_ref=ref, dst_ref=ref, send_sem=sem, recv_sem=v_recv.at[0],
                device_id={"sp": near * nx + x}, device_id_type=MESH).wait_send()

        all_sent(xs_out, xs_send.at[0])
        all_sent(xr_in.at[0], xs_send.at[1])
        all_sent(xr_in.at[0], xs_send.at[2])
        all_sent(xr_in.at[0], xs_send.at[3])
        all_sent(vx_out, v_send)
        all_sent(sx_out, sx_send)
        all_sent(sm_out, sm_send)

    norms = norm_out[...]
    for off in range(1, ntp):
        norm_copy(off).wait_recv()
        norms = norms + norm_in[off]
    rn_ref[...] = norms[:, :1]
    pltpu.make_async_remote_copy(
        src_ref=norm_in.at[pl.ds(1, ntp - 1)], dst_ref=norm_in.at[pl.ds(1, ntp - 1)],
        send_sem=n_send, recv_sem=n_recv.at[0],
        device_id={"tp": (mine + 1) % ntp}, device_id_type=MESH).wait_send()


def finish(*refs):
    sems = refs[10]
    writes = [pltpu.make_async_copy(refs[i], refs[5 + i], sems.at[i]) for i in range(5)]
    for write in writes:
        write.start()
    for write in writes:
        write.wait()


def on_device(n, nx, ntp, block_input, queries, keys, w_value, log_decay, d_out):
    tokens, wide = queries.shape
    heads = wide // DK
    cols = w_value.shape[1]
    depth = block_input.shape[1]
    own = depth // n
    nz = n // nx
    dvx = DV // nx
    vm = pltpu.VMEM
    dma = pltpu.SemaphoreType.DMA
    wide_c = min(cols, 128)
    chunks, half = cols // wide_c, own // 2
    late = [
        vm((2, 2, half, cols // 2), F32),
        vm((2, 2, half, cols // 2), F32),
        vm((n - 1, 2, 2, half, cols // 2), F32),
        dma((n - 1, 2, 2)),
        dma((n - 1, 2, 2)),
    ]
    cube = is_cube(n, nx, ntp) and cols == 2 * DV
    if cube:
        late = [
            vm((4, own // 4, tokens), F32),
            vm((ntp, 4, own // 4, tokens), F32),
            vm((ntp, own, tokens), BF16),
            vm((chunks, tokens, wide_c), F32),
            vm((chunks, tokens, wide_c), F32),
            vm((chunks, tokens, wide_c), BF16),
            vm((chunks, 2, 2, half, wide_c), F32),
            vm((chunks, 2, 2, half, wide_c), F32),
            vm((chunks, 2, 2, half, wide_c), F32),
            vm((chunks, 2, half, wide_c), F32),
            vm((chunks, 2, half, wide_c), F32),
            dma((4,)),
            dma((8,)),
            dma((2, 2)),
            dma,
            dma((chunks,)),
            dma,
            dma((chunks, 2)),
            dma,
            dma,
            dma((chunks,)),
        ]
    out = pl.pallas_call(
        functools.partial(kernel, n, nx, ntp),
        out_shape=(
            vm((tokens, wide), BF16),
            vm((tokens, wide), BF16),
            vm((tokens, wide), F32),
            vm((own, cols), F32),
            vm((2, 1, own // 2), F32),
        ),
        in_specs=[pl.BlockSpec(memory_space=pltpu.HBM)] * 6,
        out_specs=(pl.BlockSpec(memory_space=vm),) * 5,
        scratch_shapes=[
            vm(block_input.shape, BF16),
            vm(queries.shape, BF16),
            vm(keys.shape, BF16),
            vm(w_value.shape, BF16),
            vm(log_decay.shape, F32),
            vm(d_out.shape, BF16),
            dma((6,)),
            vm((tokens, wide), F32),
            vm((tokens, wide), F32),
            vm((tokens, cols), BF16),
            vm((tokens, wide), BF16),
            vm((tokens, wide), BF16),
            vm((tokens, wide), BF16),
            vm((tokens, wide), F32),
            vm((tokens, wide), F32),
            vm((tokens, cols), F32),
            vm((2, heads, DV, DK), F32),
            vm((depth, tokens), BF16),
            vm((chunks, tokens, wide_c) if cube else (tokens, cols), BF16),
            vm((2, nx, heads, dvx + 8, DK), F32),
            vm((2, nx, heads, dvx + 8, DK), F32),
            vm((heads, dvx + 8, DK), F32),
            vm((nz, heads, dvx + 8, DK), F32),
            vm((heads, dvx, DK), F32),
            vm((nx, heads, dvx, DK), F32),
            vm((nx, heads, dvx, DK), F32),
            vm((4 * heads, dvx // 4, DK), F32),
            vm((4 * heads, dvx // 4, DK), F32),
            vm((nx, 4 * heads, dvx // 4, DK), F32),
            vm((nx, 4 * heads, dvx // 4, DK), F32),
            vm((heads, DV, DK), F32),
            vm((2, 8, own // 2), F32),
            vm((ntp, 2, 8, own // 2), F32),
            dma((2, nx)),
            dma((nx - 1,)),
            dma((nx - 1, 4 * heads)),
            dma((1 if cube else nz,)),
            dma((1 if cube else nz,)),
            dma((nx - 1,)),
            dma((nx - 1,)),
            dma,
            dma((4 * heads,)),
            dma((nx,)),
            dma((nx - 1, heads)),
            dma,
            dma((ntp - 1,)),
            vm((tokens, wide), F32),
            vm((tokens, wide), BF16),
            *late,
        ],
        compiler_params=pltpu.CompilerParams(
            collective_id=0, has_side_effects=True, vmem_limit_bytes=62 * 1024 * 1024
        ),
    )(block_input, queries, keys, w_value, log_decay, d_out)
    final = pl.pallas_call(
        finish,
        out_shape=tuple(jax.ShapeDtypeStruct(a.shape, a.dtype) for a in out[:4])
        + (jax.ShapeDtypeStruct((2, 1, own // 2), F32),),
        in_specs=[pl.BlockSpec(memory_space=vm)] * 5,
        out_specs=(pl.BlockSpec(memory_space=pltpu.HBM),) * 5,
        scratch_shapes=[dma((5,))],
        compiler_params=pltpu.CompilerParams(vmem_limit_bytes=1024 * 1024),
    )(*out)
    return (*final[:4], final[4].reshape(-1))


def solution(mesh):
    n, ntp = mesh.shape["sp"], mesh.shape["tp"]
    nx = 1 << ((n.bit_length() - 1) // 2)
    placed = (
        P("sp", None),
        P("sp", "tp"),
        P("sp", "tp"),
        P(None, "tp"),
        P("sp", "tp"),
        P("sp", "tp"),
    )
    return jax.shard_map(
        functools.partial(on_device, n, nx, ntp),
        mesh=mesh,
        in_specs=placed,
        out_specs=(P("sp", "tp"), P("sp", "tp"), P("sp", "tp"), P("sp", "tp"), P("sp")),
        check_vma=False,
    )
```

```python
import functools

import jax
import jax.numpy as jnp
from jax import lax
from jax.experimental import pallas as pl
from jax.experimental.pallas import tpu as pltpu
from jax.sharding import PartitionSpec as P

DK = 128
DV = 256
BLOCK = 32
F32 = jnp.float32
BF16 = jnp.bfloat16
MESH = pl.DeviceIdType.MESH


def nn(left, right):
    return lax.dot_general(left, right, (((1,), (0,)), ((), ())), preferred_element_type=F32)


def nt(left, right):
    return lax.dot_general(left, right, (((1,), (1,)), ((), ())), preferred_element_type=F32)


def tn(left, right):
    return lax.dot_general(left, right, (((0,), (0,)), ((), ())), preferred_element_type=F32)


def pieces(value, count):
    parts = []
    for _ in range(count):
        part = value.astype(BF16)
        parts.append(part)
        value = value - part.astype(F32)
    return parts


def ring_place(z, x, nz, nx):
    r = nz - 1 - z
    across = jnp.where(r % 2 == 0, x - 1, nx - 1 - x)
    return jnp.where(x == 0, z, nz + r * (nx - 1) + across)


def ring_member(p, nz, nx):
    u = jnp.maximum(p - nz, 0)
    r = u // (nx - 1)
    w = u % (nx - 1)
    x = jnp.where(r % 2 == 0, 1 + w, nx - 1 - w)
    return jnp.where(p < nz, p * nx, (nz - 1 - r) * nx + x)


def is_cube(n, nx, ntp):
    return nx == 2 and n == 4 * nx and ntp == 2 * nx


def kernel(
    n, nx, ntp,
    x_hbm, q_hbm, k_hbm, w_hbm, g_hbm, o_hbm,
    dq_ref, dk_ref, dg_ref, dw_ref, rn_ref,
    x_ref, q_ref, k_ref, w_ref, g_ref, o_ref, in_sem,
    c_buf, span_buf, v_buf, qg_buf, kt_buf, ks_buf, y_buf, kp_buf, vp_buf, st_buf, xt_buf, vg_buf,
    a_out, a_in, z_out, z_in, z_acc, c_out, c_in, h_out, h_in, b_out, b_in, fr_buf,
    norm_out, norm_in,
    a_send, a_recv, e_recv, z_send, z_recv, c_send, c_recv, h_send, h_recv, b_send, b_recv, n_send, n_recv,
    tail_buf, ksp_buf, *late,
):
    cube = is_cube(n, nx, ntp) and dw_ref.shape[1] == 2 * DV
    if cube:
        (xs_out, xr_in, xr_buf, vx_out, vx_in, vgp_buf, sx_out, sx_in, acc_buf, sm_out, sm_in,
         xs_send, xr_recv, xc_recv, v_send, v_recv, sx_send, sx_recv, sb_recv, sm_send, sm_recv) = late
    else:
        first, part, ring, r_send, r_recv = late
    nz = n // nx
    me = lax.axis_index("sp")
    mine = lax.axis_index("tp")
    z, x = me // nx, me % nx
    tokens, heads = q_ref.shape[0], q_ref.shape[1] // DK
    blocks = tokens // BLOCK
    dvx = DV // nx
    scale = DK ** (-0.5)
    loads = [
        pltpu.make_async_copy(source, target, in_sem.at[i])
        for i, (source, target) in enumerate(
            [(g_hbm, g_ref), (q_hbm, q_ref), (o_hbm, o_ref), (k_hbm, k_ref), (x_hbm, x_ref), (w_hbm, w_ref)]
        )
    ]
    for load in loads[:3]:
        load.start()
    barrier = pltpu.get_barrier_semaphore()
    for off in range(1, nx):
        pl.semaphore_signal(
            barrier, inc=1, device_id={"sp": z * nx + (x + off) % nx}, device_id_type=MESH)
    for off in range(1, nz):
        pl.semaphore_signal(
            barrier, inc=1, device_id={"sp": (z + off) % nz * nx + x}, device_id_type=MESH)
    for off in range(1, ntp):
        pl.semaphore_signal(barrier, inc=1, device_id={"tp": (mine + off) % ntp}, device_id_type=MESH)

    row = lax.broadcasted_iota(jnp.int32, (tokens, tokens), 0)
    col = lax.broadcasted_iota(jnp.int32, (tokens, tokens), 1)
    tri = jnp.where(col <= row, 1.0, 0.0).astype(BF16)

    def inside():
        return (col <= row) & (col // BLOCK == row // BLOCK)

    def hd(h):
        return slice(h * DK, (h + 1) * DK)

    def hv(h):
        return slice(h * DV, (h + 1) * DV)

    def total(h):
        return span_buf[tokens - 1 : tokens, hd(h)]

    quarter = dvx // 4

    def part_rows(part):
        return slice(8 + part * quarter if part else 0, 8 + (part + 1) * quarter)

    def slot(to, frm):
        return (frm + nx - 1 - to) % nx

    def first_part(m, h, part):
        return pltpu.make_async_remote_copy(
            src_ref=a_out.at[1, m, h, part_rows(part), :], dst_ref=a_in.at[1, x, h, part_rows(part), :],
            send_sem=a_send.at[1, m], recv_sem=e_recv.at[slot(m, x), h * 4 + part],
            device_id={"sp": z * nx + m}, device_id_type=MESH)

    def first_wait(h, part):
        for m in range(nx):
            @pl.when(m != x)
            def _():
                pltpu.make_async_remote_copy(
                    src_ref=a_out.at[1, m, h, part_rows(part), :], dst_ref=a_in.at[1, m, h, part_rows(part), :],
                    send_sem=a_send.at[1, m], recv_sem=e_recv.at[slot(x, m), h * 4 + part],
                    device_id={"sp": z * nx + m}, device_id_type=MESH).wait_recv()

    def scatter_copy(d, m):
        return pltpu.make_async_remote_copy(
            src_ref=a_out.at[d, m], dst_ref=a_in.at[d, x],
            send_sem=a_send.at[d, m], recv_sem=a_recv.at[slot(m, x)],
            device_id={"sp": z * nx + m}, device_id_type=MESH)

    def scatter_wait(d):
        for m in range(nx):
            @pl.when(m != x)
            def _():
                pltpu.make_async_remote_copy(
                    src_ref=a_out.at[d, m], dst_ref=a_in.at[d, m],
                    send_sem=a_send.at[d, m], recv_sem=a_recv.at[slot(x, m)],
                    device_id={"sp": z * nx + m}, device_id_type=MESH).wait_recv()

    def give(d, h, totals):
        for m in range(nx):
            a_out[d, m, h, :8, :] = jnp.broadcast_to(jnp.exp(total(h)), (8, DK))
            a_out[d, m, h, 8:, :] = totals[m * dvx : (m + 1) * dvx]
        for m in range(nx):
            @pl.when(m != x)
            def _():
                if d == 1:
                    for part in range(4):
                        first_part(m, h, part).start()
                elif h == heads - 1:
                    scatter_copy(d, m).start()

            @pl.when(m == x)
            def _():
                a_in[d, m, h] = a_out[d, m, h]

    loads[0].wait()
    for i in (4, 5, 3):
        loads[i].start()
    for h in range(heads):
        span = sum(nn(tri, part_) for part_ in pieces(g_ref[:, hd(h)], 3))
        span_buf[:, hd(h)] = span
        if h == 0:
            loads[1].wait()
        q_span = (q_ref[:, hd(h)].astype(F32) * scale * jnp.exp(span)).astype(BF16)
        if h == 0:
            loads[2].wait()
        adjoint = tn(o_ref[:, hv(h)], q_span)
        if h == 0:
            pl.semaphore_wait(barrier, nx - 1 + nz - 1 + ntp - 1)
        give(1, h, adjoint)

    loads[4].wait()
    depth = x_ref.shape[1]
    for at in range(0, depth, 256):
        xt_buf[at : at + 256, :] = x_ref[:, at : at + 256].T

    own = dw_ref.shape[0]
    cols = dw_ref.shape[1]
    wide = min(cols, 128)
    chunks = cols // wide
    half_r = own // 2
    near, mirror = z + 1 - 2 * (z % 2), nz - 1 - z
    core_mate, row_mate = mine + 1 - 2 * (mine % 2), (mine + 2) % 4

    def block_rows(slab, xx, base=0, size=None):
        unit = half_r // 2
        return pl.ds(pl.multiple_of((slab * nx + xx) * own + base, unit), own if size is None else size)

    x_parts = 4
    x_rows = own // x_parts

    def x_copy(p):
        return pltpu.make_async_remote_copy(
            src_ref=xs_out.at[p], dst_ref=xr_in.at[p, mine],
            send_sem=xs_send.at[0], recv_sem=xr_recv.at[4 + p],
            device_id={"sp": near * nx + x}, device_id_type=MESH)

    def x_pass(which, quart, p, mate):
        return pltpu.make_async_remote_copy(
            src_ref=xr_in.at[p, quart], dst_ref=xr_in.at[p, quart],
            send_sem=xs_send.at[which],
            recv_sem=xr_recv.at[p] if which == 2 else xc_recv.at[which // 2, p // nx],
            device_id={"tp": mate}, device_id_type=MESH)

    def x_send(p):
        slab = nz - 1 - near if p < nx else near
        xs_out[p] = xt_buf[block_rows(slab, p % nx, mine * x_rows, x_rows), :].astype(F32)
        x_copy(p).start()

    def x_relay(p):
        x_copy(p).wait_recv()
        x_pass(2, mine, p, row_mate).start()
        x_pass(1, mine, p, core_mate).start()

    def x_forward(first_part=0, last_part=4):
        for p in range(first_part, last_part):
            x_pass(2, row_mate, p, row_mate).wait_recv()
            x_pass(3, row_mate, p, core_mate).start()

    def x_take(part):
        for i in range(2):
            pltpu.make_async_remote_copy(
                src_ref=xr_in.at[nx * part, pl.ds(0, nx)], dst_ref=xr_in.at[nx * part, pl.ds(0, nx)],
                send_sem=xs_send.at[1], recv_sem=xc_recv.at[i, part],
                device_id={"tp": core_mate}, device_id_type=MESH).wait_recv()
        for j in range(nx * part, nx * (part + 1)):
            for p in range(x_parts):
                xr_buf[j, p * x_rows : (p + 1) * x_rows] = xr_in[j, p].astype(BF16)

    if cube:
        x_send(0)

        @pl.when(z < nz - 1)
        def _():
            for p in range(1, x_parts):
                x_send(p)

    loads[3].wait()
    loads[5].wait()

    def value_side(first_head=0, last_head=heads):
        for h in range(first_head, last_head):
            k_far = jnp.exp(total(h) - span_buf[:, hd(h)])
            ksp_buf[:, hd(h)] = (k_ref[:, hd(h)].astype(F32) * k_far).astype(BF16)
            v_buf[:, hv(h)] = nn(x_ref[...], w_ref[:, hv(h)]).astype(BF16)
            give(0, h, tn(v_buf[:, hv(h)], ksp_buf[:, hd(h)]))

    def order(d):
        return range(nx) if d == 0 else range(nx - 1, -1, -1)

    def plane_copy(dz):
        return pltpu.make_async_remote_copy(
            src_ref=z_out, dst_ref=z_in.at[z],
            send_sem=z_send.at[dz], recv_sem=z_recv.at[z],
            device_id={"sp": (z + dz) * nx + x}, device_id_type=MESH)

    def composite(d, h, rows_):
        acc, dec = None, None
        for m in order(d):
            local, rate = a_in[d, m, h, rows_, :], a_in[d, m, h, 0:1, :]
            acc = local if acc is None else local + rate * acc
            dec = rate if dec is None else rate * dec
        return acc, dec

    def forward_start():
        scatter_wait(0)
        for h in range(heads):
            acc, dec = composite(0, h, slice(8, 8 + dvx))
            z_out[h, :dvx, :] = acc
            z_out[h, dvx:, :] = jnp.broadcast_to(dec, (8, DK))
        for dz in range(1, nz):
            @pl.when(z + dz < nz)
            def _():
                plane_copy(dz).start()

    def local_side():
        tri_in = jnp.where(inside(), 1.0, 0.0).astype(BF16)
        g_parts = pieces(g_ref[...], 3)
        q_all = q_ref[...].astype(F32) * scale
        k_all = k_ref[...].astype(F32)
        last_in = jnp.where(col // BLOCK == row // BLOCK, 1.0, 0.0).astype(BF16)
        cum = sum(nn(tri_in, part_) for part_ in g_parts)
        c_buf[...] = cum
        block_end = sum(nn(last_in, part_) for part_ in g_parts)
        k_tail = jnp.exp(block_end - cum)
        tail_buf[...] = k_tail
        grow = jnp.exp(cum)
        qg_buf[...] = (q_all * grow).astype(BF16)
        ks_buf[...] = (k_all * jnp.exp(-cum)).astype(BF16)
        kt_buf[...] = (k_all * k_tail).astype(BF16)
        st_buf[...] = jnp.zeros_like(st_buf)

        def adjoint_step(step, carry):
            rows = pl.ds(pl.multiple_of((blocks - 1 - step) * BLOCK, BLOCK), BLOCK)
            for h in range(heads):
                keep = jnp.exp(c_buf[rows, hd(h)][BLOCK - 1 :])
                adjoint = st_buf[1, h]
                narrow = adjoint.astype(BF16)
                kp_buf[rows, hd(h)] = nn(v_buf[rows, hv(h)], narrow)
                vp_buf[rows, hv(h)] = nt(kt_buf[rows, hd(h)], narrow)
                st_buf[1, h] = keep * adjoint + tn(o_ref[rows, hv(h)], qg_buf[rows, hd(h)])
            return carry

        lax.fori_loop(0, blocks, adjoint_step, 0)

        for h in range(heads):
            dots = jnp.where(inside(), nt(qg_buf[:, hd(h)], ks_buf[:, hd(h)]), 0.0).astype(BF16)
            vp_buf[:, hv(h)] += tn(dots, o_ref[:, hv(h)])

    def state_step(step, carry):
        rows = pl.ds(pl.multiple_of(step * BLOCK, BLOCK), BLOCK)
        for h in range(heads):
            keep = jnp.exp(c_buf[rows, hd(h)][BLOCK - 1 :])
            state = st_buf[0, h]
            y_buf[rows, hd(h)] = nn(o_ref[rows, hv(h)], state.astype(BF16))
            st_buf[0, h] = keep * state + tn(v_buf[rows, hv(h)], kt_buf[rows, hd(h)])
        return carry

    def member_copy(m):
        return pltpu.make_async_remote_copy(
            src_ref=c_out.at[m], dst_ref=c_in.at[x],
            send_sem=c_send.at[slot(x, m)], recv_sem=c_recv.at[slot(m, x)],
            device_id={"sp": z * nx + m}, device_id_type=MESH)

    def forward_spread():
        z_acc[...] = jnp.zeros_like(z_acc)
        for zp in range(nz):
            @pl.when(zp < z)
            def _():
                pltpu.make_async_remote_copy(
                    src_ref=z_out, dst_ref=z_in.at[zp],
                    send_sem=z_send.at[0], recv_sem=z_recv.at[zp],
                    device_id={"sp": zp * nx + x}, device_id_type=MESH).wait_recv()
                for h in range(heads):
                    z_acc[h] = z_in[zp, h, :dvx, :] + z_in[zp, h, dvx : dvx + 1, :] * z_acc[h]
        for h in range(heads):
            acc = z_acc[h]
            for m in order(0):
                c_out[m, h] = acc
                acc = a_in[0, m, h, 8:, :] + a_in[0, m, h, 0:1, :] * acc
        for m in range(nx):
            @pl.when(m != x)
            def _():
                member_copy(m).start()

            @pl.when(m == x)
            def _():
                c_in[m] = c_out[m]

    def step_copy():
        return pltpu.make_async_remote_copy(
            src_ref=z_out, dst_ref=z_in.at[0],
            send_sem=z_send.at[0], recv_sem=z_recv.at[0],
            device_id={"sp": (z + 1) * nx + x}, device_id_type=MESH)

    def forward_step():
        @pl.when(z == 0)
        def _():
            z_acc[...] = jnp.zeros_like(z_acc)

        @pl.when(z > 0)
        def _():
            step_copy().wait_recv()
            for h in range(heads):
                z_acc[h] = z_in[0, h, :dvx, :]

        for h in range(heads):
            acc = z_acc[h]
            for m in order(0):
                c_out[m, h] = acc
                acc = a_in[0, m, h, 8:, :] + a_in[0, m, h, 0:1, :] * acc
            z_out[h, :dvx, :] = acc
            z_out[h, dvx:, :] = jnp.zeros((8, DK), F32)

        @pl.when(z < nz - 1)
        def _():
            step_copy().start()

        for m in range(nx):
            @pl.when(m != x)
            def _():
                member_copy(m).start()

            @pl.when(m == x)
            def _():
                c_in[m] = c_out[m]

    def near_copy(c):
        return pltpu.make_async_remote_copy(
            src_ref=vx_out.at[c], dst_ref=vx_in.at[c],
            send_sem=v_send, recv_sem=v_recv.at[c],
            device_id={"sp": near * nx + x}, device_id_type=MESH)

    def side_copy(c, s, u):
        return pltpu.make_async_remote_copy(
            src_ref=sx_out.at[c, s, u], dst_ref=sx_in.at[c, s, u],
            send_sem=sx_send, recv_sem=sx_recv.at[c, u] if s == 0 else sb_recv,
            device_id={"sp": z * nx + 1 - x}, device_id_type=MESH)

    def far_copy(c, u):
        return pltpu.make_async_remote_copy(
            src_ref=sm_out.at[c, u], dst_ref=sm_in.at[c, u],
            send_sem=sm_send, recv_sem=sm_recv.at[c],
            device_id={"sp": mirror * nx + x}, device_id_type=MESH)

    def emit(h, m):
        c = h * nx + m
        held = b_in[m, 4 * h : 4 * h + 4].reshape(dvx, DK).astype(BF16)
        at = pl.ds(pl.multiple_of(c * wide, wide), wide)
        value = (vp_buf[:, at] + nt(ksp_buf[:, hd(h)], held)).astype(BF16)
        vg_buf[c] = value
        vx_out[c] = value.astype(F32)
        near_copy(c).start()

    def far_take(c):
        pltpu.make_async_remote_copy(
            src_ref=sm_in.at[c], dst_ref=sm_in.at[c],
            send_sem=sm_send, recv_sem=sm_recv.at[c],
            device_id={"sp": mirror * nx + x}, device_id_type=MESH).wait_recv()

    def piece(c, s, xx):
        slab = mirror if s == 0 else z
        return nn(xt_buf[block_rows(slab, xx), :], vg_buf[c]) + nn(xr_buf[s * nx + xx], vgp_buf[c])

    def take_near(c):
        near_copy(c).wait_recv()
        vgp_buf[c] = vx_in[c].astype(BF16)

    def side_send(c, s):
        value = piece(c, s, 1 - x)
        for u in range(2):
            sx_out[c, s, u] = value[u * half_r : (u + 1) * half_r]
            side_copy(c, s, u).start()

    def keep(c, s):
        value = piece(c, s, x)
        for u in range(2):
            acc_buf[c, s, u] = value[u * half_r : (u + 1) * half_r]

    def far_send(c):
        for u in range(2):
            side_copy(c, 0, u).wait_recv()
            sm_out[c, u] = acc_buf[c, 0, u] + sx_in[c, 0, u]
            far_copy(c, u).start()

    @pl.when(z < nz - 1)
    def _():
        value_side()
        local_side()

    if cube:
        @pl.when(z < nz - 1)
        def _():
            x_relay(0)

        @pl.when(z < nz - 2)
        def _():
            x_relay(1)

    if not cube:
        @pl.when(z < nz - 2)
        def _():
            forward_start()

    if cube:
        @pl.when(z < nz - 2)
        def _():
            for p in range(2, x_parts):
                x_relay(p)

        @pl.when(z == 0)
        def _():
            scatter_wait(0)
            forward_step()

    @pl.when(z == nz - 1)
    def _():
        value_side(0, 1)

    half_v = dvx // 4

    def chain_copy(c):
        return pltpu.make_async_remote_copy(
            src_ref=h_out.at[c], dst_ref=h_in.at[c],
            send_sem=h_send, recv_sem=h_recv.at[c],
            device_id={"sp": (z - 1) * nx + x}, device_id_type=MESH)

    def piece_copy(m, c):
        return pltpu.make_async_remote_copy(
            src_ref=b_out.at[m, c], dst_ref=b_in.at[x, c],
            send_sem=b_send.at[m], recv_sem=b_recv.at[slot(m, x), c // 4],
            device_id={"sp": z * nx + m}, device_id_type=MESH)

    late_half = z >= nz - 2
    turns = [
        jnp.where(late_half, i, (i // nx) * nx + (x if i % nx == 0 else 1 - x)) for i in range(2 * nx)]
    s0, s1, s2, s3 = turns if cube else (0, 0, 0, 0)

    def open_side():
        x_take(0)
        take_near(s0)
        side_send(s0, 0)

    def other_slice(h):
        part = pl.ds(4 * h, 4)
        pltpu.make_async_remote_copy(
            src_ref=b_out.at[1 - x, part], dst_ref=b_in.at[1 - x, part],
            send_sem=b_send.at[1 - x], recv_sem=b_recv.at[0, h],
            device_id={"sp": z * nx + 1 - x}, device_id_type=MESH).wait_recv()

    for c in range(4 * heads):
        if cube and c == 4:
            @pl.when(z == 0)
            def _():
                open_side()

        if cube and c == 6:
            @pl.when(z == 0)
            def _():
                other_slice(0)
                emit(0, 1 - x)

        h, rows_ = c // 4, slice(8 + c % 4 * half_v, 8 + (c % 4 + 1) * half_v)
        first_wait(h, c % 4)
        acc, dec = composite(1, h, rows_)

        @pl.when(z == nz - 1)
        def _():
            h_in[c] = jnp.zeros((half_v, DK), F32)

        @pl.when(z < nz - 1)
        def _():
            chain_copy(c).wait_recv()

        enter = h_in[c]

        @pl.when(z > 0)
        def _():
            h_out[c] = acc + dec * enter
            chain_copy(c).start()

        for m in order(1):
            b_out[m, c] = enter
            enter = a_in[1, m, h, rows_, :] + a_in[1, m, h, 0:1, :] * enter
        for m in range(nx):
            @pl.when(m != x)
            def _():
                piece_copy(m, c).start()

            @pl.when(m == x)
            def _():
                b_in[m, c] = b_out[m, c]

        if cube and c == 3:
            @pl.when(z < nz - 1)
            def _():
                emit(0, x)

            @pl.when(z == 0)
            def _():
                x_forward()

    if cube:
        @pl.when(z == 0)
        def _():
            emit(1, x)
    else:
        @pl.when(z == nz - 2)
        def _():
            forward_start()

    @pl.when(z == nz - 1)
    def _():
        if cube:
            for p in range(1, x_parts):
                x_send(p)
            x_relay(0)
        value_side(1, heads)
        if cube:
            x_relay(1)
        local_side()
        if cube:
            for p in range(2, x_parts):
                x_relay(p)
        else:
            scatter_wait(0)

    def state_loop():
        lax.fori_loop(0, blocks, state_step, 0)

    if cube:
        @pl.when(z < nz - 1)
        def _():
            state_loop()

        @pl.when((z > 0) & (z < nz - 2))
        def _():
            x_forward()

        @pl.when(z == nz - 2)
        def _():
            for p in range(1, x_parts - 1):
                x_relay(p)

        def keep_pieces():
            for h in range(heads):
                for m in range(nx):
                    fr_buf[h, m * dvx : (m + 1) * dvx, :] = b_in[m, 4 * h : 4 * h + 4].reshape(dvx, DK)

        @pl.when((z > 0) & (z < nz - 1))
        def _():
            other_slice(0)
            emit(0, 1 - x)
            emit(1, x)

            @pl.when(z == nz - 2)
            def _():
                x_relay(x_parts - 1)

            other_slice(1)
            emit(1, 1 - x)
            keep_pieces()

        @pl.when(z == nz - 1)
        def _():
            for h in range(heads):
                other_slice(h)
                for m in range(nx):
                    emit(h, m)
            keep_pieces()

        @pl.when(z == nz - 1)
        def _():
            state_loop()
    else:
        for h in range(heads):
            for m in range(nx):
                @pl.when(m != x)
                def _():
                    pltpu.make_async_remote_copy(
                        src_ref=b_out.at[m, pl.ds(4 * h, 4)], dst_ref=b_in.at[m, pl.ds(4 * h, 4)],
                        send_sem=b_send.at[m], recv_sem=b_recv.at[slot(x, m), h],
                        device_id={"sp": z * nx + m}, device_id_type=MESH).wait_recv()
                fr_buf[h, m * dvx : (m + 1) * dvx, :] = b_in[m, 4 * h : 4 * h + 4].reshape(dvx, DK)
            narrow = fr_buf[h].astype(BF16)
            vg_buf[:, hv(h)] = (vp_buf[:, hv(h)] + nt(ksp_buf[:, hd(h)], narrow)).astype(BF16)


    half_c = cols // 2
    p = ring_place(z, x, nz, nx)
    ahead = ring_member((p + 1) % n, nz, nx)
    behind = ring_member((p + n - 1) % n, nz, nx)

    def share(d, u, owner):
        rows_ = pl.ds(pl.multiple_of(owner * own + u * half_r, half_r), half_r)
        return nn(xt_buf[rows_, :], vg_buf[:, d * half_c : (d + 1) * half_c])

    def ring_copy(step, d, u, src):
        return pltpu.make_async_remote_copy(
            src_ref=src, dst_ref=ring.at[step, d, u],
            send_sem=r_send.at[step, d, u], recv_sem=r_recv.at[step, d, u],
            device_id={"sp": ahead if d == 0 else behind}, device_id_type=MESH)

    def owner_at(step, d):
        return ring_member((p + n - step - 1) % n if d == 0 else (p + step + 1) % n, nz, nx)

    if not cube:
        for u in range(2):
            for d in range(2):
                first[d, u] = share(d, u, owner_at(0, d))
                ring_copy(0, d, u, first.at[d, u]).start()

    def key_side():
        for h in range(heads):
            dots = jnp.where(inside(), nt(o_ref[:, hv(h)], v_buf[:, hv(h)]), 0.0).astype(BF16)
            y_buf[:, hd(h)] += nn(dots, ks_buf[:, hd(h)])
            k_grad = (
                tail_buf[:, hd(h)] * kp_buf[:, hd(h)]
                + jnp.exp(-c_buf[:, hd(h)]) * tn(dots, qg_buf[:, hd(h)])
                + jnp.exp(total(h) - span_buf[:, hd(h)]) * nn(v_buf[:, hv(h)], fr_buf[h].astype(BF16))
            )
            kp_buf[:, hd(h)] = k_grad
            dk_ref[:, hd(h)] = k_grad.astype(BF16)

    if not cube:
        state_loop()
        key_side()

    def query_side(first_head=0, last_head=heads):
        for m in range(nx):
            if first_head:
                break

            @pl.when(m != x)
            def _():
                pltpu.make_async_remote_copy(
                    src_ref=c_out.at[m], dst_ref=c_in.at[m],
                    send_sem=c_send.at[slot(x, m)], recv_sem=c_recv.at[slot(x, m)],
                    device_id={"sp": z * nx + m}, device_id_type=MESH).wait_recv()
        upper = jnp.where(col >= row, 1.0, 0.0).astype(BF16)
        for h in range(first_head, last_head):
            state_in = jnp.concatenate([c_in[m, h] for m in range(nx)], axis=0)
            q_side = q_ref[:, hd(h)].astype(F32) * scale
            k_side = k_ref[:, hd(h)].astype(F32)
            q_grad = jnp.exp(c_buf[:, hd(h)]) * y_buf[:, hd(h)] + jnp.exp(span_buf[:, hd(h)]) * nn(
                o_ref[:, hv(h)], state_in.astype(BF16)
            )
            dq_ref[:, hd(h)] = (q_grad * scale).astype(BF16)
            terms = q_side * q_grad - k_side * kp_buf[:, hd(h)]
            far = jnp.exp(span_buf[tokens - 1 : tokens, hd(h)])
            span_end = st_buf[0, h] + far * state_in
            carry = jnp.sum(fr_buf[h] * span_end, axis=0, keepdims=True)
            dg_ref[:, hd(h)] = sum(nn(upper, part_) for part_ in pieces(terms, 3)) + carry

    def ring_step(step, carry):
        for d in range(2):
            for u in range(2):
                part[d, u] = share(d, u, owner_at(step, d))
        for u in range(2):
            for d in range(2):
                ring_copy(step - 1, d, u, first.at[d, u]).wait_recv()
                ring[step - 1, d, u] += part[d, u]
                ring_copy(step, d, u, ring.at[step - 1, d, u]).start()

        @pl.when(step == 2)
        def _():
            forward_spread()

        @pl.when(step == 4)
        def _():
            query_side()

        return carry

    if not cube:
        lax.fori_loop(1, n - 1, ring_step, 0)

        for d in range(2):
            for u in range(2):
                part[d, u] = share(d, u, me)
        for u in range(2):
            squares = 0.0
            for d in range(2):
                ring_copy(n - 2, d, u, first.at[d, u]).wait_recv()
                done = ring[n - 2, d, u] + part[d, u]
                dw_ref[u * half_r : (u + 1) * half_r, d * half_c : (d + 1) * half_c] = done
                for at in range(0, half_c, 128):
                    squares = squares + done[:, at : at + 128] * done[:, at : at + 128]
            norm_out[u : u + 1, :] = jnp.sum(squares.T, axis=0, keepdims=True)
    else:
        @pl.when(z >= nz - 2)
        def _():
            x_forward(0, 2)

        @pl.when((z > 0) & (z < nz - 2))
        def _():
            scatter_wait(0)
            forward_step()

        f0, f1, f2, f3 = [jnp.where(late_half, turns[i], turns[i ^ 1]) for i in range(chunks)]
        @pl.when(z > 0)
        def _():
            open_side()

        @pl.when(z < nz - 1)
        def _():
            keep(s0, 0)

            @pl.when(z > 0)
            def _():
                key_side()

            take_near(s1)
            side_send(s1, 0)
            keep(s1, 0)
            far_send(f0)

            @pl.when(z == 0)
            def _():
                other_slice(1)
                emit(1, 1 - x)
                keep_pieces()
                key_side()

            @pl.when(z == nz - 2)
            def _():
                x_forward(2, 4)

            take_near(s2)
            side_send(s2, 0)

            @pl.when(z == nz - 2)
            def _():
                scatter_wait(0)
                forward_step()

            take_near(s3)
            side_send(s3, 0)
            far_send(f1)
            x_take(1)
            side_send(s0, 1)
            side_send(s1, 1)
            keep(s2, 0)
            keep(s3, 0)
            far_send(f2)
            side_send(s2, 1)
            side_send(s3, 1)
            far_send(f3)
            for c in range(chunks):
                keep(c, 1)

        @pl.when(z == nz - 1)
        def _():
            for c in (s1, s2, s3):
                take_near(c)
                side_send(c, 0)
            x_forward(2, 4)
            key_side()
            x_take(1)
            for c in range(chunks):
                keep(c, 0)
                side_send(c, 1)
                keep(c, 1)
            far_send(0)
            far_take(1 - x)
            for c in range(1, chunks):
                far_send(c)
            scatter_wait(0)
            forward_step()

        query_side(0, heads)
        squares = [0.0, 0.0]
        pltpu.make_async_remote_copy(
            src_ref=sm_in, dst_ref=sm_in, send_sem=sx_send, recv_sem=sb_recv,
            device_id={"sp": z * nx + 1 - x}, device_id_type=MESH).wait_recv()
        for c in range(chunks):
            at = slice(c * wide, (c + 1) * wide)
            if c < nx:
                @pl.when((z < nz - 1) | (c != 1 - x))
                def _():
                    far_take(c)
            else:
                far_take(c)
            for u in range(2):
                done = acc_buf[c, 1, u] + sx_in[c, 1, u] + sm_in[c, u]
                dw_ref[u * half_r : (u + 1) * half_r, at] = done
                squares[u] = squares[u] + done * done
        for u in range(2):
            norm_out[u : u + 1, :] = jnp.sum(squares[u].T, axis=0, keepdims=True)

    def norm_copy(off):
        return pltpu.make_async_remote_copy(
            src_ref=norm_out, dst_ref=norm_in.at[off],
            send_sem=n_send, recv_sem=n_recv.at[off - 1],
            device_id={"tp": (mine + off) % ntp}, device_id_type=MESH)

    for off in range(1, ntp):
        norm_copy(off).start()

    for m in range(nx):
        @pl.when(m != x)
        def _():
            for d in range(2):
                pltpu.make_async_remote_copy(
                    src_ref=a_out.at[d, m], dst_ref=a_in.at[d, x],
                    send_sem=a_send.at[d, m], recv_sem=a_recv.at[slot(m, x)],
                    device_id={"sp": z * nx + m}, device_id_type=MESH).wait_send()
            pltpu.make_async_remote_copy(
                src_ref=b_out.at[m], dst_ref=b_in.at[x],
                send_sem=b_send.at[m], recv_sem=b_recv.at[slot(m, x), 0],
                device_id={"sp": z * nx + m}, device_id_type=MESH).wait_send()
            member_copy(m).wait_send()
    if cube:
        @pl.when(z < nz - 1)
        def _():
            step_copy().wait_send()
    else:
        for dz in range(1, nz):
            @pl.when(z + dz < nz)
            def _():
                plane_copy(dz).wait_send()

    @pl.when(z > 0)
    def _():
        pltpu.make_async_remote_copy(
            src_ref=h_out, dst_ref=h_in,
            send_sem=h_send, recv_sem=h_recv.at[0],
            device_id={"sp": (z - 1) * nx + x}, device_id_type=MESH).wait_send()

    if not cube:
        def sent(step, carry):
            for u in range(2):
                for d in range(2):
                    ring_copy(step, d, u, first.at[d, u]).wait_send()
            return carry

        lax.fori_loop(0, n - 1, sent, 0)
    else:
        def all_sent(ref, sem):
            pltpu.make_async_remote_copy(
                src_ref=ref, dst_ref=ref, send_sem=sem, recv_sem=v_recv.at[0],
                device_id={"sp": near * nx + x}, device_id_type=MESH).wait_send()

        all_sent(xs_out, xs_send.at[0])
        all_sent(xr_in.at[0], xs_send.at[1])
        all_sent(xr_in.at[0], xs_send.at[2])
        all_sent(xr_in.at[0], xs_send.at[3])
        all_sent(vx_out, v_send)
        all_sent(sx_out, sx_send)
        all_sent(sm_out, sm_send)

    norms = norm_out[...]
    for off in range(1, ntp):
        norm_copy(off).wait_recv()
        norms = norms + norm_in[off]
    for u in range(2):
        rn_ref[u] = norms[u : u + 1]
    pltpu.make_async_remote_copy(
        src_ref=norm_in.at[pl.ds(1, ntp - 1)], dst_ref=norm_in.at[pl.ds(1, ntp - 1)],
        send_sem=n_send, recv_sem=n_recv.at[0],
        device_id={"tp": (mine + 1) % ntp}, device_id_type=MESH).wait_send()


def finish(*refs):
    sems = refs[10]
    writes = [pltpu.make_async_copy(refs[i], refs[5 + i], sems.at[i]) for i in range(5)]
    for write in writes:
        write.start()
    for write in writes:
        write.wait()


def on_device(n, nx, ntp, block_input, queries, keys, w_value, log_decay, d_out):
    tokens, wide = queries.shape
    heads = wide // DK
    cols = w_value.shape[1]
    depth = block_input.shape[1]
    own = depth // n
    nz = n // nx
    dvx = DV // nx
    vm = pltpu.VMEM
    dma = pltpu.SemaphoreType.DMA
    wide_c = min(cols, 128)
    chunks, half = cols // wide_c, own // 2
    late = [
        vm((2, 2, half, cols // 2), F32),
        vm((2, 2, half, cols // 2), F32),
        vm((n - 1, 2, 2, half, cols // 2), F32),
        dma((n - 1, 2, 2)),
        dma((n - 1, 2, 2)),
    ]
    cube = is_cube(n, nx, ntp) and cols == 2 * DV
    if cube:
        late = [
            vm((4, own // 4, tokens), F32),
            vm((ntp, 4, own // 4, tokens), F32),
            vm((ntp, own, tokens), BF16),
            vm((chunks, tokens, wide_c), F32),
            vm((chunks, tokens, wide_c), F32),
            vm((chunks, tokens, wide_c), BF16),
            vm((chunks, 2, 2, half, wide_c), F32),
            vm((chunks, 2, 2, half, wide_c), F32),
            vm((chunks, 2, 2, half, wide_c), F32),
            vm((chunks, 2, half, wide_c), F32),
            vm((chunks, 2, half, wide_c), F32),
            dma((4,)),
            dma((8,)),
            dma((2, 2)),
            dma,
            dma((chunks,)),
            dma,
            dma((chunks, 2)),
            dma,
            dma,
            dma((chunks,)),
        ]
    out = pl.pallas_call(
        functools.partial(kernel, n, nx, ntp),
        out_shape=(
            vm((tokens, wide), BF16),
            vm((tokens, wide), BF16),
            vm((tokens, wide), F32),
            vm((own, cols), F32),
            vm((2, 1, own // 2), F32),
        ),
        in_specs=[pl.BlockSpec(memory_space=pltpu.HBM)] * 6,
        out_specs=(pl.BlockSpec(memory_space=vm),) * 5,
        scratch_shapes=[
            vm(block_input.shape, BF16),
            vm(queries.shape, BF16),
            vm(keys.shape, BF16),
            vm(w_value.shape, BF16),
            vm(log_decay.shape, F32),
            vm(d_out.shape, BF16),
            dma((6,)),
            vm((tokens, wide), F32),
            vm((tokens, wide), F32),
            vm((tokens, cols), BF16),
            vm((tokens, wide), BF16),
            vm((tokens, wide), BF16),
            vm((tokens, wide), BF16),
            vm((tokens, wide), F32),
            vm((tokens, wide), F32),
            vm((tokens, cols), F32),
            vm((2, heads, DV, DK), F32),
            vm((depth, tokens), BF16),
            vm((chunks, tokens, wide_c) if cube else (tokens, cols), BF16),
            vm((2, nx, heads, dvx + 8, DK), F32),
            vm((2, nx, heads, dvx + 8, DK), F32),
            vm((heads, dvx + 8, DK), F32),
            vm((nz, heads, dvx + 8, DK), F32),
            vm((heads, dvx, DK), F32),
            vm((nx, heads, dvx, DK), F32),
            vm((nx, heads, dvx, DK), F32),
            vm((4 * heads, dvx // 4, DK), F32),
            vm((4 * heads, dvx // 4, DK), F32),
            vm((nx, 4 * heads, dvx // 4, DK), F32),
            vm((nx, 4 * heads, dvx // 4, DK), F32),
            vm((heads, DV, DK), F32),
            vm((2, own // 2), F32),
            vm((ntp, 2, own // 2), F32),
            dma((2, nx)),
            dma((nx - 1,)),
            dma((nx - 1, 4 * heads)),
            dma((1 if cube else nz,)),
            dma((1 if cube else nz,)),
            dma((nx - 1,)),
            dma((nx - 1,)),
            dma,
            dma((4 * heads,)),
            dma((nx,)),
            dma((nx - 1, heads)),
            dma,
            dma((ntp - 1,)),
            vm((tokens, wide), F32),
            vm((tokens, wide), BF16),
            *late,
        ],
        compiler_params=pltpu.CompilerParams(
            collective_id=0, has_side_effects=True, vmem_limit_bytes=62 * 1024 * 1024
        ),
    )(block_input, queries, keys, w_value, log_decay, d_out)
    final = pl.pallas_call(
        finish,
        out_shape=tuple(jax.ShapeDtypeStruct(a.shape, a.dtype) for a in out[:4])
        + (jax.ShapeDtypeStruct((2, 1, own // 2), F32),),
        in_specs=[pl.BlockSpec(memory_space=vm)] * 5,
        out_specs=(pl.BlockSpec(memory_space=pltpu.HBM),) * 5,
        scratch_shapes=[dma((5,))],
        compiler_params=pltpu.CompilerParams(vmem_limit_bytes=1024 * 1024),
    )(*out)
    return (*final[:4], final[4].reshape(-1))


def solution(mesh):
    n, ntp = mesh.shape["sp"], mesh.shape["tp"]
    nx = 1 << ((n.bit_length() - 1) // 2)
    placed = (
        P("sp", None),
        P("sp", "tp"),
        P("sp", "tp"),
        P(None, "tp"),
        P("sp", "tp"),
        P("sp", "tp"),
    )
    return jax.shard_map(
        functools.partial(on_device, n, nx, ntp),
        mesh=mesh,
        in_specs=placed,
        out_specs=(P("sp", "tp"), P("sp", "tp"), P("sp", "tp"), P("sp", "tp"), P("sp")),
        check_vma=False,
    )
```
